32 devices in a mesh: ep: 8 (over z, core), tp: 4 (over y, x).
Axes of the slice: x: 2, y: 2, z: 4, core: 2. Of those that a mesh axis runs over, the one named last changes fastest.
Arguments:
- query_pairs: bfloat16 [3072, 2048], P('ep', 'tp'), may hold values from -64 to 64
- key_pairs: bfloat16 [3072, 2048], P('ep', 'tp'), may hold values from -64 to 64
- value_rows: bfloat16 [3072, 2048], P('ep', 'tp'), may hold values from -6 to 6
- head_lambda: float32 [16], P('tp'), may hold values from 0.3 to 0.8
- head_gain: float32 [128], replicated, may hold values from 0.1 to 1.9
- out_weight: bfloat16 [2048, 2048], P('tp'), may hold values from -0.1875 to 0.1875
- moe_input: bfloat16 [1280, 2048], P('ep'), may hold values from -6 to 6
- ffn_gain: float32 [2048], replicated, may hold values from 0.1 to 1.9
- routes: int32 [1280, 2], P('ep'), may hold values from 0 to 7, all different within a row; in each aligned block of 160 rows (0 to 159, 160 to 319, ...) at most 50 rows name the same one
- route_weight: float32 [1280, 2], P('ep'), may hold values from 0.25 to 2.5
- gate_weight: bfloat16 [8, 2048, 2048], P('ep', None, 'tp'), may hold values from -0.125 to 0.125
- up_weight: bfloat16 [8, 2048, 2048], P('ep', None, 'tp'), may hold values from -0.125 to 0.125
- down_weight: bfloat16 [8, 2048, 2048], P('ep', 'tp'), may hold values from -0.1875 to 0.1875
- shared_gate: bfloat16 [2048, 2048], P(None, 'tp'), may hold values from -0.125 to 0.125
- shared_up: bfloat16 [2048, 2048], P(None, 'tp'), may hold values from -0.125 to 0.125
- shared_down: bfloat16 [2048, 2048], P('tp'), may hold values from -0.1875 to 0.1875
Outputs:
- attn_out: bfloat16 [3072, 2048], P('ep', 'tp')
- moe_out: bfloat16 [1280, 2048], P('ep', 'tp')
The draws below stay inside these ranges and needn't reach their ends.
Inputs may be any that keep to these rules, and one draw needn't show every extreme that they name: `routes`: in each aligned block of 160 rows (the rows of one device along ep) no expert is named more than 50 times, a bound that some block reaches; a row names 2 different experts.
All inputs are finite; a program needn't handle non-finite values.
Results may differ from the reference program's by a relative error of at most 0.017.
The reference program's roundings to bfloat16 on the way count: a program that leaves them out, or rounds other values in their place, can miss the bound.
Values may be sent and summed in bfloat16 or wider, within the bound.
A program may use at most 64 MiB of HBM per device.

```python
import math
import jax
import jax.numpy as jnp
import numpy as np
from jax import lax

D = 2048
HEADS = 16
HEAD = 64
VHEAD = 128
FF = 2048
SFF = 2048
TOP_K = 2
KEY_BLOCK = 128
TOK_B = 160
TOKENS_A = 3072
TOKENS_B = 1280
EXPERTS = 8
CAP = 50
N_TP = 4


def paired_draw(key):
    draw_shape = (TOKENS_A, HEADS, 2, HEAD)
    queries = 1.3 * jax.random.truncated_normal(jax.random.fold_in(key, 101), -4.0, 4.0, draw_shape, jnp.float32)
    keyset = 1.3 * jax.random.truncated_normal(jax.random.fold_in(key, 102), -4.0, 4.0, draw_shape, jnp.float32)
    return (jnp.clip(queries, -64.0, 64.0), jnp.clip(keyset, -64.0, 64.0))


def draw_query_pairs(key, part):
    return paired_draw(key)[0].reshape(TOKENS_A, HEADS * 2 * HEAD).astype(jnp.bfloat16)


def draw_key_pairs(key, part):
    return paired_draw(key)[1].reshape(TOKENS_A, HEADS * 2 * HEAD).astype(jnp.bfloat16)


def with_spikes(entries, rng, source, target, blocks, factor):
    owner, partner = [(jnp.arange(entries.shape[axis_at]) // (entries.shape[axis_at] // blocks)).reshape([-1 if axis == axis_at else 1 for axis in range(entries.ndim)]) for axis_at in (source, target)]
    chosen = jax.random.permutation(rng, blocks)[partner]
    strong = (owner == chosen) | (owner == (partner + blocks // 2) % blocks)
    return jnp.where(strong, factor * entries, entries)


def level_of(key, dims, split, smallest, high):
    level, own = 1.0, jax.random.fold_in(key, 6)
    for dim, parts in split:
        draws = jnp.exp(jax.random.uniform(jax.random.fold_in(own, dim), (parts,), jnp.float32, smallest / len(split), high / len(split)))
        level = level * jnp.repeat(draws, dims[dim] // parts).reshape([-1 if axis == dim else 1 for axis in range(len(dims))])
    return level


def routed_block(own_key, own, number, rows, count, top, limit, lean):
    order = jax.random.permutation(own_key, count)
    heavy_load, usual = portions_of(count, rows * top, limit, lean, True), portions_of(count, rows * top, limit, lean, False)
    places = jnp.arange(count)

    def named(tallies, turn):
        used = int((tallies > 0).sum())
        fixed = max(1, used // 4)
        passed = fixed + (places - fixed + turn * (used - fixed)) % max(1, count - fixed)
        return jnp.zeros((count,), jnp.int32).at[order[jnp.where(places < fixed, places, passed)]].set(jnp.asarray(tallies, jnp.int32))

    tallies = jnp.where(number % 4 == 0, named(heavy_load, number // 4), named(usual, number - number // 4 - 1))
    mixed = jax.random.permutation(jax.random.fold_in(own, 3), count)
    source_of, taker = mixed[0:count // 2 * 2:2], mixed[1:count // 2 * 2:2]
    slack = jnp.minimum(tallies[source_of] - 1, limit - tallies[taker]) // 2
    slack = jnp.where((source_of == order[0]) | (taker == order[0]) | (tallies[taker] == 0), 0, jnp.maximum(slack, 0))
    passed = jax.random.randint(jax.random.fold_in(own, 4), (count // 2,), 0, 1 << 20) % (slack + 1)
    tallies = tallies.at[source_of].add(-passed).at[taker].add(passed)
    labels = jnp.searchsorted(jnp.cumsum(tallies), jnp.arange(rows * top), side="right").astype(jnp.int32)
    grid = labels.reshape(top, rows).T
    grid = grid[jax.random.permutation(jax.random.fold_in(own, 1), rows)]
    turn = jax.random.randint(jax.random.fold_in(own, 2), (rows, 1), 0, top)
    return jnp.take_along_axis(grid, (jnp.arange(top)[None, :] + turn) % top, axis=1)


def portions_of(number_of, total, limit, slope, full):
    weights = [(1 << 20) // math.isqrt(standing ** slope) + 1 for standing in range(1, number_of + 1)]
    largest = limit if full else min(limit, max(-(-total // number_of), total * weights[0] // sum(weights)))
    least = 1 if total - largest >= number_of - 1 else 0
    counts, spare = [largest] + [least] * (number_of - 1), total - largest - least * (number_of - 1)
    while spare > 0:
        free = [i for i in range(1, number_of) if counts[i] < largest] or [i for i in range(1, number_of) if counts[i] < limit]
        mass, remaining = sum([weights[i] for i in free]), spare
        for i in free:
            more = min(limit - counts[i], max(1, remaining * weights[i] // mass), spare)
            counts[i] = counts[i] + more
            spare = spare - more
    return np.array(counts)


def scatter_about(rng, dims, scale, bound, shards=(), held_as=jnp.bfloat16):
    loudness = level_of(rng, dims, shards, -0.22, 0.18) if shards else 1.0
    drawn = jax.random.normal(rng, dims, jnp.float32) * scale * loudness
    return jnp.minimum(jnp.maximum(drawn, -bound), bound).astype(held_as)


def bell_draw_with(stream_key, shape, width, limit, shards, heavy, kind=jnp.bfloat16):
    values = width * jax.random.normal(stream_key, shape, jnp.float32)
    if shards:
        values = values * level_of(stream_key, shape, shards, -0.22, 0.18)
    return jnp.clip(with_spikes(values, jax.random.fold_in(stream_key, 3), *heavy), -limit, limit).astype(kind)


def setup_inputs(seed: int = 0) -> dict:
    streams_of = jax.random.split(jax.random.key(seed), 17)
    query_pairs = draw_query_pairs(jax.random.fold_in(streams_of[16], 71), 0)
    key_pairs = draw_key_pairs(jax.random.fold_in(streams_of[16], 71), 0)
    value_rows = scatter_about(streams_of[2], (TOKENS_A, HEADS * VHEAD), 1.0, 6.0, ((0, 8), (1, 4)))
    head_lambda = jnp.clip(0.3 + 0.5 * jax.random.uniform(streams_of[3], (HEADS,), jnp.float32) ** level_of(streams_of[3], (HEADS,), ((0, 4),), -0.2, 0.2), 0.3, 0.8)
    head_gain = jnp.clip(1.0 + 0.18 * jax.random.normal(streams_of[4], (VHEAD,), jnp.float32), 0.1, 1.9)
    out_weight = bell_draw_with(streams_of[5], (HEADS * VHEAD, D), (HEADS * VHEAD) ** -0.5, 0.1875, ((0, 4),), (0, 1, 4, 2.0))
    moe_input = scatter_about(streams_of[6], (TOKENS_B, D), 1.0, 6.0, ((0, 8),))
    ffn_gain = jnp.clip(1.0 + 0.18 * jax.random.normal(streams_of[7], (D,), jnp.float32), 0.1, 1.9)
    routes_keys = jax.random.split(jax.random.fold_in(streams_of[8], 1), TOKENS_B // TOK_B)
    routes_turns = jax.random.permutation(jax.random.fold_in(streams_of[8], 3), TOKENS_B // TOK_B)
    routes = jax.vmap(lambda own, number: routed_block(jax.random.fold_in(streams_of[8], 2), own, number, TOK_B, EXPERTS, TOP_K, CAP, 1))(routes_keys, routes_turns).reshape((TOKENS_B, TOP_K))
    route_weight = jnp.clip(jnp.exp(math.log(2.5) - 2.3025851 * jax.random.uniform(streams_of[9], (TOKENS_B, TOP_K), jnp.float32) ** level_of(streams_of[9], (TOKENS_B, TOP_K), ((0, 8),), -0.2, 0.2)), 0.25, 2.5)
    gate_weight = scatter_about(streams_of[10], (EXPERTS, D, FF), D ** -0.5, 0.125, ((0, 8), (2, 4)))
    up_weight = scatter_about(streams_of[11], (EXPERTS, D, FF), D ** -0.5, 0.125, ((0, 8), (2, 4)))
    down_weight = bell_draw_with(streams_of[12], (EXPERTS, FF, D), FF ** -0.5, 0.1875, ((0, 8), (1, 4)), (1, 2, 4, 2.0))
    shared_gate = scatter_about(streams_of[13], (D, SFF), D ** -0.5, 0.125, ((1, 4),))
    shared_up = scatter_about(streams_of[14], (D, SFF), D ** -0.5, 0.125, ((1, 4),))
    shared_down = bell_draw_with(streams_of[15], (SFF, D), SFF ** -0.5, 0.1875, ((0, 4),), (0, 1, 4, 2.0))
    return {"query_pairs": query_pairs, "key_pairs": key_pairs, "value_rows": value_rows, "head_lambda": head_lambda, "head_gain": head_gain, "out_weight": out_weight, "moe_input": moe_input, "ffn_gain": ffn_gain, "routes": routes, "route_weight": route_weight, "gate_weight": gate_weight, "up_weight": up_weight, "down_weight": down_weight, "shared_gate": shared_gate, "shared_up": shared_up, "shared_down": shared_down}


theta_base = 500000.0
norm_eps = 1e-06
masked_low = -1e+30

def rotate(inputs, positions):
    half_size = inputs.shape[-1] // 2
    frequency = theta_base ** (-(jnp.arange(half_size, dtype=jnp.float32) * 2.0) / inputs.shape[-1])
    angles = positions.astype(jnp.float32)[:, None] * frequency[None, :]
    cosine = jnp.cos(angles)[:, None, None, :]
    sine_part = jnp.sin(angles)[:, None, None, :]
    front_half = inputs[..., :half_size]
    back_half = inputs[..., half_size:]
    return jnp.concatenate([front_half * cosine - back_half * sine_part, back_half * cosine + front_half * sine_part], axis=-1)

def attention(query_pairs, key_pairs, value_rows, head_lambda, head_gain, out_weight):
    total_rows = query_pairs.shape[0]
    head_count = head_lambda.shape[0]
    head_size = query_pairs.shape[1] // (2 * head_count)
    value_size = value_rows.shape[1] // head_count
    positions = jnp.arange(total_rows, dtype=jnp.int32)
    rot_queries = rotate(query_pairs.astype(jnp.float32).reshape(total_rows, head_count, 2, head_size), positions).astype(jnp.bfloat16)
    rot_keys = rotate(key_pairs.astype(jnp.float32).reshape(total_rows, head_count, 2, head_size), positions).astype(jnp.bfloat16)
    key_blocks = total_rows // KEY_BLOCK
    block_keys = rot_keys.reshape(key_blocks, KEY_BLOCK, head_count, 2, head_size).astype(jnp.float32)
    block_values = value_rows.reshape(key_blocks, KEY_BLOCK, head_count, value_size).astype(jnp.float32)
    key_positions = positions.reshape(key_blocks, KEY_BLOCK)
    query_block = math.gcd(total_rows, 256)
    query_count = total_rows // query_block

    def one_block(inputs):
        block_queries, query_positions = inputs
        scores = jnp.einsum('qhmd,bkhmd->hmqbk', block_queries.astype(jnp.float32), block_keys) * head_size ** (-0.5)
        allowed = key_positions[None, :, :] <= query_positions[:, None, None]
        scores = jnp.where(allowed, scores, masked_low)
        block_max = lax.optimization_barrier(jnp.max(scores, axis=-1))
        weights = jnp.where(allowed, jnp.exp(scores - block_max[..., None]), 0.0)
        block_sum = lax.optimization_barrier(jnp.sum(weights, axis=-1))
        rounded = lax.optimization_barrier(weights.astype(jnp.bfloat16)).astype(jnp.float32)
        block_out = jnp.einsum('hmqbk,bkhc->hmqbc', rounded, block_values)
        row_max = lax.optimization_barrier(jnp.max(block_max, axis=-1, keepdims=True))
        rescale = jnp.exp(block_max - row_max)
        summed = lax.optimization_barrier(jnp.sum(rescale * block_sum, axis=-1))
        combined = lax.optimization_barrier(jnp.sum(rescale[..., None] * block_out, axis=-2))
        return combined / summed[..., None]
    outputs = lax.map(one_block, (rot_queries.reshape(query_count, query_block, head_count, 2, head_size), positions.reshape(query_count, query_block)))
    difference = outputs[:, :, 0] - head_lambda[None, :, None, None] * outputs[:, :, 1]
    inverse_rms = lax.rsqrt(lax.optimization_barrier(jnp.mean(difference * difference, axis=-1, keepdims=True)) + norm_eps)
    normed = (difference * inverse_rms * head_gain.astype(jnp.float32)).astype(jnp.bfloat16)
    normed = normed.transpose(0, 2, 1, 3).reshape(total_rows, head_count * value_size)
    group_cols = head_count * value_size // N_TP
    grouped = normed.reshape(total_rows, N_TP, group_cols).transpose(1, 0, 2)
    weight_groups = out_weight.reshape(N_TP, group_cols, out_weight.shape[1])

    def add_group(running, block_parts):
        partial_out = jnp.dot(block_parts[0], block_parts[1], preferred_element_type=jnp.float32)
        return (running + lax.optimization_barrier(partial_out.astype(jnp.bfloat16)).astype(jnp.float32), None)
    result, _ = lax.scan(add_group, jnp.zeros((total_rows, out_weight.shape[1]), jnp.float32), (grouped, weight_groups))
    return result.astype(jnp.bfloat16)

def swiglu_blocks(inputs, gate_w, up_w, down_w):
    model_width = gate_w.shape[0]
    block_width = gate_w.shape[1] // N_TP
    gate_blocks = gate_w.reshape(model_width, N_TP, block_width).transpose(1, 0, 2)
    up_blocks = up_w.reshape(model_width, N_TP, block_width).transpose(1, 0, 2)
    down_blocks = down_w.reshape(N_TP, block_width, down_w.shape[1])

    def add_block(running, block_parts):
        gate_part = jnp.dot(inputs, block_parts[0], preferred_element_type=jnp.float32)
        up_part = jnp.dot(inputs, block_parts[1], preferred_element_type=jnp.float32)
        hidden = (jax.nn.silu(gate_part) * up_part).astype(jnp.bfloat16)
        partial_out = jnp.dot(hidden, block_parts[2], preferred_element_type=jnp.float32)
        return (running + lax.optimization_barrier(partial_out.astype(jnp.bfloat16)).astype(jnp.float32), None)
    result, _ = lax.scan(add_block, jnp.zeros((inputs.shape[0], down_w.shape[1]), jnp.float32), (gate_blocks, up_blocks, down_blocks))
    return result

def mixture(moe_input, ffn_gain, routes, route_weight, gate_weight, up_weight, down_weight, shared_gate, shared_up, shared_down):
    row_values = moe_input.astype(jnp.float32)
    inverse_rms = lax.rsqrt(lax.optimization_barrier(jnp.mean(row_values * row_values, axis=-1, keepdims=True)) + norm_eps)
    normed = (row_values * inverse_rms * ffn_gain.astype(jnp.float32)).astype(jnp.bfloat16)
    total_rows = normed.shape[0]
    experts = gate_weight.shape[0]
    blocks = total_rows // TOK_B
    flat_routes = routes.reshape(blocks, TOK_B * TOP_K)
    onehot = (flat_routes[..., None] == jnp.arange(experts, dtype=jnp.int32)).astype(jnp.int32)
    slot_rank = lax.optimization_barrier(jnp.sum((jnp.cumsum(onehot, axis=1) - 1) * onehot, axis=-1)).astype(jnp.int32)
    token_ids = jnp.arange(blocks, dtype=jnp.int32)[:, None] * TOK_B + jnp.arange(TOK_B * TOP_K, dtype=jnp.int32)[None, :] // TOP_K
    source_ids = jnp.broadcast_to(jnp.arange(blocks, dtype=jnp.int32)[:, None], flat_routes.shape)
    slot_table = jnp.full((experts, blocks, CAP), total_rows, jnp.int32).at[flat_routes, source_ids, slot_rank].set(token_ids)
    padded = jnp.concatenate([normed, jnp.zeros((1, normed.shape[1]), jnp.bfloat16)], axis=0)

    def one_expert(inputs):
        chosen = padded[inputs[0].reshape(-1)]
        return swiglu_blocks(chosen, inputs[1], inputs[2], inputs[3]).astype(jnp.bfloat16)
    expert_out = lax.map(one_expert, (slot_table, gate_weight, up_weight, down_weight))
    expert_out = expert_out.reshape(experts, blocks, CAP, normed.shape[1])
    block_index = (jnp.arange(total_rows, dtype=jnp.int32) // TOK_B)[:, None]
    picked = expert_out[routes, block_index, slot_rank.reshape(total_rows, TOP_K)]
    shared_sum = swiglu_blocks(normed, shared_gate, shared_up, shared_down)
    combined = lax.optimization_barrier(jnp.sum(route_weight[..., None] * picked.astype(jnp.float32), axis=1)) + shared_sum
    return combined.astype(jnp.bfloat16)

def reference(query_pairs, key_pairs, value_rows, head_lambda, head_gain, out_weight, moe_input, ffn_gain, routes, route_weight, gate_weight, up_weight, down_weight, shared_gate, shared_up, shared_down):
    attn_out = attention(query_pairs, key_pairs, value_rows, head_lambda, head_gain, out_weight)
    moe_out = mixture(moe_input, ffn_gain, routes, route_weight, gate_weight, up_weight, down_weight, shared_gate, shared_up, shared_down)
    return (attn_out, moe_out)
```

```python
import functools

import jax
import jax.numpy as jnp
import numpy as np
from jax import lax
from jax.experimental import pallas as pl
from jax.experimental.pallas import tpu as pltpu
from jax.sharding import PartitionSpec as P

TOP_K = 2
KEY_BLOCK = 128


theta_base = 500000.0
norm_eps = 1e-06
masked_low = -1e30


def rotate(inputs, positions):
    half_size = inputs.shape[-1] // 2
    frequency = theta_base ** (-(jnp.arange(half_size, dtype=jnp.float32) * 2.0) / inputs.shape[-1])
    angles = positions.astype(jnp.float32)[:, None] * frequency[None, :]
    cosine = jnp.cos(angles)[:, None, None, :]
    sine_part = jnp.sin(angles)[:, None, None, :]
    front_half = inputs[..., :half_size]
    back_half = inputs[..., half_size:]
    return jnp.concatenate(
        [front_half * cosine - back_half * sine_part, back_half * cosine + front_half * sine_part],
        axis=-1,
    )


def generic_attention(query_pairs, key_pairs, value_rows, head_lambda, head_gain, out_weight):
    local_rows = query_pairs.shape[0]
    local_heads = head_lambda.shape[0]
    head_size = query_pairs.shape[1] // (2 * local_heads)
    value_size = value_rows.shape[1] // local_heads
    positions = lax.axis_index("ep") * local_rows + jnp.arange(local_rows, dtype=jnp.int32)
    rot_queries = rotate(
        query_pairs.astype(jnp.float32).reshape(local_rows, local_heads, 2, head_size), positions
    ).astype(jnp.bfloat16)
    rot_keys = rotate(
        key_pairs.astype(jnp.float32).reshape(local_rows, local_heads, 2, head_size), positions
    ).astype(jnp.bfloat16)
    rot_keys = rot_keys.reshape(local_rows, local_heads * 2 * head_size)
    zero_init = (
        jnp.full((local_heads, 2, local_rows), masked_low, jnp.float32),
        jnp.zeros((local_heads, 2, local_rows), jnp.float32),
        jnp.zeros((local_heads, 2, local_rows, value_size), jnp.float32),
    )
    piece_keys = lax.all_gather(rot_keys, "ep", axis=0, tiled=True)
    piece_values = lax.all_gather(value_rows, "ep", axis=0, tiled=True)
    block_count = piece_keys.shape[0] // KEY_BLOCK
    group_size = 4
    group_count = block_count // group_size
    grouped_keys = piece_keys.reshape(group_count, group_size, KEY_BLOCK, local_heads, 2, head_size)
    grouped_values = piece_values.reshape(
        group_count, group_size, KEY_BLOCK, local_heads, value_size
    )

    def one_group(current, inputs):
        block_keys, block_values, group_index = inputs
        key_positions = group_index * group_size * KEY_BLOCK + jnp.arange(
            group_size * KEY_BLOCK, dtype=jnp.int32
        ).reshape(group_size, KEY_BLOCK)
        scores = jnp.einsum(
            "qhmd,gkhmd->hmqgk", rot_queries, block_keys, preferred_element_type=jnp.float32
        ) * head_size ** (-0.5)
        allowed = key_positions[None, :, :] <= positions[:, None, None]
        scores = jnp.where(allowed, scores, masked_low)
        block_max = jnp.max(scores, axis=-1)
        weights = jnp.where(allowed, jnp.exp(scores - block_max[..., None]), 0.0)
        block_sum = jnp.sum(weights, axis=-1)
        block_out = jnp.einsum(
            "hmqgk,gkhc->hmqgc",
            weights.astype(jnp.bfloat16),
            block_values,
            preferred_element_type=jnp.float32,
        )
        run_max, run_sum, run_out = current
        new_max = jnp.maximum(run_max, jnp.max(block_max, axis=-1))
        old_scale = jnp.exp(run_max - new_max)
        new_scale = jnp.exp(block_max - new_max[..., None])
        run_sum = run_sum * old_scale + jnp.sum(new_scale * block_sum, axis=-1)
        run_out = run_out * old_scale[..., None] + jnp.sum(
            new_scale[..., None] * block_out, axis=-2
        )
        return ((new_max, run_sum, run_out), None)

    result, _ = lax.scan(
        one_group,
        zero_init,
        (grouped_keys, grouped_values, jnp.arange(group_count, dtype=jnp.int32)),
    )
    run_max, run_sum, run_out = result
    map_outputs = run_out / run_sum[..., None]
    difference = map_outputs[:, 0] - head_lambda[:, None, None] * map_outputs[:, 1]
    inverse_rms = lax.rsqrt(jnp.mean(difference * difference, axis=-1, keepdims=True) + norm_eps)
    normed_heads = (difference * inverse_rms * head_gain).astype(jnp.bfloat16)
    head_rows = normed_heads.transpose(1, 0, 2).reshape(local_rows, local_heads * value_size)
    mixer_terms = jnp.dot(head_rows, out_weight, preferred_element_type=jnp.float32)
    attn_out = lax.psum_scatter(
        mixer_terms.astype(jnp.bfloat16), "tp", scatter_dimension=1, tiled=True
    )
    return attn_out


MESH = pl.DeviceIdType.MESH
f32, bf16 = jnp.float32, jnp.bfloat16


def mega_kernel(
    n, heads, n_tp, head_size, lam_ref, gain_ref, routes_ref, rw_ref, ffn_ref, turn_ref, base_ref,
    q_ref, k_ref, v_ref, x_ref, w_ref, wg_ref, wu_ref, wd_ref, sg_ref, su_ref, sd_ref,
    attn_ref, moe_ref,
    q_in, k_in, v_in, turn, x_in, xn, place, rq, rk, q_buf, k_buf, v_buf, vt_buf, st_buf, acc, m_buf,
    hn_send, hn_buf, w_buf, out_buf, own_buf, arr, wg, wu, wd, sg, su, sd,
    sh_send, sh_in, ex_send, ex_in, mix_send, mix_in, y_buf, ret, rw_pad,
    load, load_v, barrier_free, q_ss, q_rs, k_ss, k_rs, v_ss, v_rs, fk_ss, fk_rs, fv_ss, fv_rs, h_ss, h_rs,
    t_ss, t_rs, o_ss, o_rs, x_ss, x_rs, m_ss, m_rs, s_ss, s_rs, e_ss, e_rs, y_ss, y_rs,
):
    me, my_tp = lax.axis_index("ep"), lax.axis_index("tp")
    g = n // heads
    chip, core = me // g, me % g
    rows, width = k_buf.shape[1:]
    vw = v_buf.shape[2]
    sub = rows // g
    cap, piece = out_buf.shape[1:]
    tokens = xn.shape[0]
    top_k = rw_ref.shape[0]
    half = head_size // 2
    side = chip // (heads // 2)

    def mirrored(p):
        return p + side * (heads - 1 - 2 * p)

    near = mirrored(chip)

    def nearest(s):
        return mirrored(jnp.where(s <= near, near - s, s))

    barrier = pltpu.get_barrier_semaphore()
    for step in range(1, n):
        pl.semaphore_signal(barrier, inc=1, device_id={"ep": lax.rem(me + step, n)}, device_id_type=MESH)
    for step in range(1, n_tp):
        pl.semaphore_signal(barrier, inc=1, device_id={"tp": lax.rem(my_tp + step, n_tp)}, device_id_type=MESH)
    loads = [
        pltpu.make_async_copy(source, target, load.at[i])
        for i, (source, target) in enumerate((
            (x_ref, x_in), (turn_ref, turn), (k_ref, k_in), (q_ref, q_in),
            (sg_ref, sg), (su_ref, su), (sd_ref, sd),
            (wg_ref.at[0], wg), (wu_ref.at[0], wu), (wd_ref.at[0], wd), (w_ref, w_buf)))
    ]
    values = [
        pltpu.make_async_copy(v_ref.at[:, h * vw : (h + 1) * vw], v_in.at[h], load_v.at[h]) for h in range(heads)
    ]
    for copy in loads[:4]:
        copy.start()
    for copy in values:
        copy.start()
    for copy in loads[4:]:
        copy.start()

    def to_ep(source, target, send_sem, recv_sem, dest):
        return pltpu.make_async_remote_copy(
            source, target, send_sem, recv_sem, device_id={"ep": dest}, device_id_type=MESH)

    def to_tp(source, target, send_sem, recv_sem, dest):
        return pltpu.make_async_remote_copy(
            source, target, send_sem, recv_sem, device_id={"tp": dest}, device_id_type=MESH)

    def arrived(ref, sem):
        to_ep(ref, ref, sem, sem, lax.rem(me + 1, n)).wait_recv()

    peers = [lax.rem(my_tp + step, n_tp) for step in (*range(1, n_tp), 0)]

    def columns(t):
        return pl.ds(pl.multiple_of(t * piece, piece), piece)

    expert = lax.broadcasted_iota(jnp.int32, (n, tokens), 0)
    chosen = [(routes_ref[k : k + 1, :] == expert).astype(f32) for k in range(top_k)]
    earlier = lax.broadcasted_iota(jnp.int32, (tokens, tokens), 0) <= lax.broadcasted_iota(jnp.int32, (tokens, tokens), 1)
    ranks = jnp.dot(sum(chosen).astype(bf16), earlier.astype(bf16), preferred_element_type=f32) - 1.0
    slot = ranks + (expert * cap).astype(f32)
    slots = [jnp.sum(c * slot, axis=0, keepdims=True) for c in chosen]
    slot_row = lax.broadcasted_iota(jnp.int32, (n * cap, tokens), 0).astype(f32)
    marks = [(slot_row == s).astype(f32) for s in slots]
    for k in range(top_k):
        place[k] = marks[k].astype(bf16).reshape(n, cap, tokens)
    loads[0].wait()
    x = x_in[...].astype(f32)
    inverse = lax.rsqrt(jnp.mean(x * x, axis=-1, keepdims=True) + norm_eps)
    xn[...] = (x * inverse * ffn_ref[...]).astype(bf16)
    out_buf[...] = jnp.dot(
        sum(marks).astype(bf16), xn[:, columns(my_tp)], preferred_element_type=f32).astype(bf16).reshape(n, cap, piece)

    def own_rows(dest):
        mark = place[0, dest]
        for k in range(1, top_k):
            mark = mark + place[k, dest]
        return jnp.dot(mark, xn[...], preferred_element_type=f32).astype(bf16)

    pl.semaphore_wait(barrier, n - 1 + n_tp - 1)

    def tok_copy(dest):
        return to_ep(out_buf.at[dest], arr.at[my_tp, me], t_ss.at[dest], t_rs.at[me], dest)

    def own_copy(step):
        dest = chip * g + lax.rem(core + step, g)
        return to_ep(own_buf.at[step - 1], arr.at[:, me], o_ss.at[step - 1], o_rs.at[me], dest)

    for s in range(1, heads):
        for c in range(g):
            tok_copy(nearest(s) * g + c).start()
    for step in range(g):
        full = own_rows(chip * g + lax.rem(core + step, g))
        for t in range(n_tp):
            part = full[:, t * piece : (t + 1) * piece]
            if step == 0:
                arr[t, me] = part
            else:
                own_buf[step - 1, t] = part
        if step:
            own_copy(step).start()

    base_cos, base_sin = base_ref[0, pl.ds(me, 1)], base_ref[1, pl.ds(me, 1)]
    lane = lax.broadcasted_iota(jnp.int32, (1, width), 1)
    front = lane % head_size < half
    loads[1].wait()
    cosine = turn[0] * base_cos - turn[1] * base_sin
    sine = turn[1] * base_cos + turn[0] * base_sin
    sine = jnp.where(front, -sine, sine)

    def turned(source, h):
        x = source[:, h * width : (h + 1) * width].astype(f32)
        partner = jnp.where(front, pltpu.roll(x, width - half, 1), pltpu.roll(x, half, 1))
        return (x * cosine + partner * sine).astype(bf16)

    loads[2].wait()
    for h in range(heads):
        rk[h] = turned(k_in, h)
    loads[3].wait()
    for h in range(heads):
        rq[h] = turned(q_in, h) * jnp.asarray(head_size ** -0.5, bf16)
    for copy in values:
        copy.wait()

    def q_rows(dest):
        return pl.ds(pl.multiple_of(((dest % g + me) % g) * sub, sub), sub)

    def q_copy(dest):
        return to_ep(rq.at[dest // g, q_rows(dest)], q_buf.at[me], q_ss.at[dest], q_rs.at[me], dest)

    def k_copy(dest):
        return to_ep(rk.at[dest // g], k_buf.at[me], k_ss.at[dest], k_rs.at[me], dest)

    def v_copy(dest):
        return to_ep(v_in.at[dest // g], v_buf.at[me], v_ss.at[dest], v_rs.at[me], dest)

    for s in range(1, heads):
        dest = nearest(s) * g + core
        k_copy(dest).start()
        for c in range(g):
            q_copy(nearest(s) * g + c).start()
        v_copy(dest).start()
    for step in range(1, g):
        q_copy(chip * g + lax.rem(core + step, g)).start()
    q_buf[me] = rq[chip, q_rows(me)]
    k_buf[me] = rk[chip]
    v_buf[me] = v_in[chip]

    def gated(gate, up):
        return (gate / (1.0 + jnp.exp(-gate)) * up).astype(bf16)

    for i in (4, 5, 6):
        loads[i].wait()
    hidden = gated(
        jnp.dot(xn[...], sg[...], preferred_element_type=f32), jnp.dot(xn[...], su[...], preferred_element_type=f32))

    def sh_copy(dest):
        return to_tp(sh_send.at[dest], sh_in.at[my_tp], s_ss.at[dest], s_rs.at[my_tp], dest)

    for dest in peers:
        sh_send[dest] = jnp.dot(hidden, sd[:, columns(dest)], preferred_element_type=f32).astype(bf16)
        if dest is not peers[-1]:
            sh_copy(dest).start()

    lam = lam_ref[chip]
    gain = gain_ref[...]
    vt_rows = vt_buf.shape[1]
    keys = g * rows
    lane_row = lax.broadcasted_iota(jnp.int32, (sub, width), 1)

    def forward(source, step):
        to = chip * g + lax.rem(core + step, g)
        return (
            to_ep(k_buf.at[source], k_buf.at[source], fk_ss.at[source, step], fk_rs.at[source], to),
            to_ep(v_buf.at[source], v_buf.at[source], fv_ss.at[source, step], fv_rs.at[source], to),
        )

    def receive(p):
        direct = p * g + core

        @pl.when(direct != me)
        def _():
            arrived(k_buf.at[direct], k_rs.at[direct])
            arrived(v_buf.at[direct], v_rs.at[direct])

        for step in range(1, g):
            for copy in forward(direct, step):
                copy.start()
        for c in range(g):
            e = p * g + c

            @pl.when(e != me)
            def _():
                arrived(q_buf.at[e], q_rs.at[e])

            q = q_buf[e]
            zero = jnp.zeros_like(q)
            st_buf[p, 2 * c * sub : (2 * c + 1) * sub] = jnp.where(lane_row < width // 2, q, zero)
            st_buf[p, (2 * c + 1) * sub : (2 * c + 2) * sub] = jnp.where(lane_row < width // 2, zero, q)
        for step in range(1, g):
            other = p * g + lax.rem(core + step, g)
            arrived(k_buf.at[other], fk_rs.at[other])
            arrived(v_buf.at[other], fv_rs.at[other])
        for c in range(g):
            vt_buf[p, :vw, c * rows : (c + 1) * rows] = v_buf[p * g + c].astype(f32).T.astype(bf16)
        vt_buf[p, vw:] = jnp.ones((vt_rows - vw, keys), bf16)
        m_buf[p] = jnp.full((1, keys), masked_low, f32)
        acc[p] = jnp.zeros((vt_rows, keys), f32)

    def tile(p, j, diagonal):
        for c in range(g):
            first = c * rows if diagonal else 0
            span = slice(first, keys)
            size = keys - first
            s = lax.dot_general(
                k_buf[j * g + c], st_buf[p, span], (((1,), (1,)), ((), ())), preferred_element_type=f32)
            if diagonal:
                key = lax.broadcasted_iota(jnp.int32, (rows, size), 0) + c * rows
                column = lax.broadcasted_iota(jnp.int32, (rows, size), 1) + first
                block = column // rows
                query = block * rows + column % sub + (core + block) % g * sub
                s = jnp.where(key <= query, s, masked_low)
            old = m_buf[p, :, span]
            m = jnp.maximum(old, jnp.max(s, axis=0, keepdims=True))
            weights = jnp.exp(s - m).astype(bf16)
            m_buf[p, :, span] = m
            acc[p, :, span] = acc[p, :, span] * jnp.exp(old - m) + jnp.dot(
                vt_buf[j, :, c * rows : (c + 1) * rows], weights, preferred_element_type=f32)

    def hn_copy(dest):
        return to_ep(hn_send.at[dest], hn_buf.at[me], h_ss.at[dest], h_rs.at[me], dest)

    def finish(p):
        a = (acc[p, :vw] / acc[p, vw : vw + 1]).T
        for c in range(g):
            e = p * g + c
            diff = a[2 * c * sub : (2 * c + 1) * sub] - lam * a[(2 * c + 1) * sub : (2 * c + 2) * sub]
            inverse = lax.rsqrt(jnp.mean(diff * diff, axis=-1, keepdims=True) + norm_eps)
            hn_send[e] = (diff * inverse * gain).astype(bf16)

            @pl.when(e != me)
            def _():
                hn_copy(e).start()

    def turn_of(p):
        p = mirrored(p)
        return jnp.where(p <= near, near - p, p)

    def attend(s):
        receive(nearest(s))

        def queries(p, _):
            def blocks(j, _):
                @pl.when(jnp.maximum(turn_of(p), turn_of(j)) == s)
                def _():
                    tile(p, j, False)

                return 0

            @pl.when(turn_of(p) == s)
            def _():
                tile(p, p, True)

            @pl.when(turn_of(p) <= s)
            def _():
                lax.fori_loop(0, p, blocks, 0)

            last = 0
            for j in range(heads):
                last = jnp.maximum(last, jnp.where(j <= p, turn_of(j), 0))

            @pl.when(last == s)
            def _():
                finish(p)

            return 0

        lax.fori_loop(0, heads, queries, 0)
        return 0

    def spread_copy(p, dest):
        part = arr.at[my_tp, pl.ds(p * g, g)]
        return to_tp(part, part, x_ss.at[p, dest], x_rs.at[my_tp, p], dest)

    def spread(s):
        p = nearest(s)
        for c in range(g):
            arrived(arr.at[my_tp, p * g + c], t_rs.at[p * g + c])
        for dest in peers[:-1]:
            spread_copy(p, dest).start()

    def ex_copy(dest):
        return to_tp(ex_send.at[dest], ex_in.at[my_tp], e_ss.at[dest], e_rs.at[my_tp], dest)

    def routed():
        for step in range(1, g):
            other = chip * g + lax.rem(core + step, g)
            arrived(arr.at[:, other], o_rs.at[other])
        for s in range(1, heads):
            for t in peers[:-1]:
                arrived(arr.at[t, pl.ds(nearest(s) * g, g)], x_rs.at[t, nearest(s)])
        for i in (7, 8, 9):
            loads[i].wait()
        gate = up = None
        for t in range(n_tp):
            block = arr[t].reshape(n * cap, piece)
            span = slice(t * piece, (t + 1) * piece)
            gate_part = jnp.dot(block, wg[span, :], preferred_element_type=f32)
            up_part = jnp.dot(block, wu[span, :], preferred_element_type=f32)
            gate = gate_part if gate is None else gate + gate_part
            up = up_part if up is None else up + up_part
        hidden = gated(gate, up)
        for dest in peers:
            ex_send[dest] = jnp.dot(hidden, wd[:, columns(dest)], preferred_element_type=f32).astype(bf16)
            if dest is not peers[-1]:
                ex_copy(dest).start()

    def phase(s, _):
        attend(s)

        @pl.when(s == 0)
        def _():
            for step in range(1, heads):
                spread(step)

        @pl.when(s == 1)
        def _():
            routed()

        return 0

    lax.fori_loop(0, heads, phase, 0)

    hn_buf[me] = hn_send[me]
    for step in range(1, n):
        source = lax.rem(me + step, n)
        arrived(hn_buf.at[source], h_rs.at[source])
    loads[10].wait()

    def mix_copy(dest):
        return to_tp(mix_send.at[dest], mix_in.at[my_tp], m_ss.at[dest], m_rs.at[my_tp], dest)

    normed = [
        jnp.concatenate([hn_buf[h * g + (part + n - me) % g] for h in range(heads)], axis=1) for part in range(g)]
    for dest in peers:
        for part in range(g):
            mix_send[dest, part * sub : (part + 1) * sub] = jnp.dot(
                normed[part], w_buf[:, columns(dest)], preferred_element_type=f32).astype(bf16)
        if dest is not peers[-1]:
            mix_copy(dest).start()

    def y_copy(dest):
        return to_ep(y_buf.at[dest], ret.at[me], y_ss.at[dest], y_rs.at[me], dest)

    y = ex_send[my_tp].astype(f32)
    for source in peers[:-1]:
        arrived(ex_in.at[source], e_rs.at[source])
        y = y + ex_in[source].astype(f32)
    y_buf[...] = y.astype(bf16).reshape(n, cap, piece)
    for s in range(1, heads):
        for c in range(g):
            y_copy(nearest(s) * g + c).start()
    for step in range(1, g):
        y_copy(chip * g + lax.rem(core + step, g)).start()
    ret[me] = y_buf[me]
    out = sh_send[my_tp].astype(f32)
    for source in peers[:-1]:
        arrived(sh_in.at[source], s_rs.at[source])
        out = out + sh_in[source].astype(f32)
    rw_pad[...] = jnp.zeros_like(rw_pad)
    rw_pad[:top_k, :tokens] = rw_ref[...]
    scale = rw_pad[...].T
    for step in range(1, n):
        source = lax.rem(me + step, n)
        arrived(ret.at[source], y_rs.at[source])
    returned = ret[...].reshape(n * cap, piece)
    for k in range(top_k):
        out = out + scale[:tokens, k : k + 1] * lax.dot_general(
            place[k].reshape(n * cap, tokens), returned, (((0,), (0,)), ((), ())), preferred_element_type=f32)
    moe_ref[...] = out.astype(bf16)

    total = mix_send[my_tp].astype(f32)
    for source in peers[:-1]:
        arrived(mix_in.at[source], m_rs.at[source])
        total = total + mix_in[source].astype(f32)
    attn_ref[...] = total.astype(bf16)

    for s in range(1, heads):
        p = nearest(s)
        k_copy(p * g + core).wait_send()
        v_copy(p * g + core).wait_send()
        for c in range(g):
            tok_copy(p * g + c).wait_send()
        for dest in peers[:-1]:
            spread_copy(p, dest).wait_send()
    for step in range(1, n):
        dest = lax.rem(me + step, n)
        q_copy(dest).wait_send()
        hn_copy(dest).wait_send()
        y_copy(dest).wait_send()
    for step in range(1, g):
        own_copy(step).wait_send()
    for p in range(heads):
        for step in range(1, g):
            for copy in forward(p * g + core, step):
                copy.wait_send()
    for dest in peers[:-1]:
        sh_copy(dest).wait_send()
        ex_copy(dest).wait_send()
        mix_copy(dest).wait_send()


def turn_tables(rows, n, head_size):
    half = head_size // 2
    frequency = theta_base ** (-(np.arange(half) * 2.0) / head_size)

    def waves(positions):
        angles = np.tile(positions[:, None] * frequency[None, :], (1, 4))
        return np.stack([np.cos(angles), np.sin(angles)]).astype(np.float32)

    return waves(np.arange(rows)), waves(np.arange(n) * rows)


def exchange_all(
    query_pairs, key_pairs, value_rows, head_lambda, head_gain, out_weight, moe_input, ffn_gain, routes, route_weight,
    gate_weight, up_weight, down_weight, shared_gate, shared_up, shared_down,
):
    n, n_tp = lax.axis_size("ep"), lax.axis_size("tp")
    tokens, model = moe_input.shape
    piece = model // n_tp
    rows = query_pairs.shape[0]
    heads = head_lambda.shape[0]
    width = query_pairs.shape[1] // heads
    head_size = width // 2
    vw = value_rows.shape[1] // heads
    g = n // heads
    sub = rows // g
    keys = g * rows
    cap = -(-(tokens * TOP_K * 5 // (4 * n)) // 8) * 8
    hidden, shared = gate_weight.shape[2], shared_gate.shape[1]
    turns, bases = turn_tables(rows, n, head_size)
    any_spec = pl.BlockSpec(memory_space=pl.ANY)
    vmem = pl.BlockSpec(memory_space=pltpu.VMEM)
    dma = pltpu.SemaphoreType.DMA
    buffers = [
        (rows, heads * width), (rows, heads * width), (heads, rows, vw), ((2, rows, width), f32),
        (tokens, model), (tokens, model), (TOP_K, n, cap, tokens), (heads, rows, width), (heads, rows, width),
        (n, sub, width), (n, rows, width), (n, rows, vw), (heads, vw + 8, keys), (heads, 2 * rows, width),
        ((heads, vw + 8, keys), f32), ((heads, 1, keys), f32), (n, sub, vw), (n, sub, vw), out_weight.shape,
        (n, cap, piece), (g - 1, n_tp, cap, piece), (n_tp, n, cap, piece),
        (model, hidden), (model, hidden), (hidden, model), (model, shared), (model, shared), (shared, model),
        (n_tp, tokens, piece), (n_tp, tokens, piece), (n_tp, n * cap, piece), (n_tp, n * cap, piece),
        (n_tp, rows, piece), (n_tp, rows, piece), (n, cap, piece), (n, cap, piece),
        ((8, -(-tokens // 128) * 128), f32),
    ]
    semaphores = [
        (11,), (heads,), (1,), (n,), (n,), (n,), (n,), (n,), (n,), (n, g), (n,), (n, g), (n,), (n,), (n,),
        (n,), (n,), (g - 1,), (n,), (heads, n_tp), (n_tp, heads), (n_tp,), (n_tp,), (n_tp,), (n_tp,), (n_tp,), (n_tp,),
        (n,), (n,),
    ]
    return pl.pallas_call(
        functools.partial(mega_kernel, n, heads, n_tp, head_size),
        out_shape=(
            jax.ShapeDtypeStruct((rows, piece), bf16),
            jax.ShapeDtypeStruct((tokens, piece), bf16),
        ),
        in_specs=[pl.BlockSpec(memory_space=pltpu.SMEM)] + [vmem] * 4 + [any_spec, vmem] + [any_spec] * 11,
        out_specs=(vmem, vmem),
        scratch_shapes=[
            pltpu.VMEM(shape[0], shape[1]) if isinstance(shape[0], tuple) else pltpu.VMEM(shape, bf16)
            for shape in buffers
        ] + [dma(shape) for shape in semaphores],
        compiler_params=pltpu.CompilerParams(
            collective_id=0, has_side_effects=True, vmem_limit_bytes=60 * 2**20),
        cost_estimate=pl.CostEstimate(flops=30 * 10**9, bytes_accessed=24 * 2**20, transcendentals=6 * 10**6),
        name="exchange",
    )(
        head_lambda, head_gain.reshape(1, vw), routes.T, route_weight.T, ffn_gain.reshape(1, model),
        jnp.asarray(turns), jnp.asarray(bases), query_pairs, key_pairs, value_rows, moe_input, out_weight,
        gate_weight, up_weight, down_weight, shared_gate, shared_up, shared_down)


def local(
    query_pairs,
    key_pairs,
    value_rows,
    head_lambda,
    head_gain,
    out_weight,
    moe_input,
    ffn_gain,
    routes,
    route_weight,
    gate_weight,
    up_weight,
    down_weight,
    shared_gate,
    shared_up,
    shared_down,
):
    n = lax.axis_size("ep")
    heads = head_lambda.shape[0]
    rows = query_pairs.shape[0]
    fits = n == 2 * heads and heads % 2 == 0 and (rows * heads) % (n * 64) == 0
    if fits:
        return exchange_all(
            query_pairs, key_pairs, value_rows, head_lambda, head_gain, out_weight, moe_input, ffn_gain, routes,
            route_weight, gate_weight, up_weight, down_weight, shared_gate, shared_up, shared_down,
        )
    row_values = moe_input.astype(jnp.float32)
    inverse_norm = lax.rsqrt(jnp.mean(row_values * row_values, axis=-1, keepdims=True) + norm_eps)
    normed = (row_values * inverse_norm * ffn_gain).astype(jnp.bfloat16)
    attn_out = generic_attention(query_pairs, key_pairs, value_rows, head_lambda, head_gain, out_weight)
    token_rows = normed.shape[0]
    experts = lax.axis_size("ep")
    capacity = token_rows * TOP_K * 5 // (4 * experts)
    flat_routes = routes.reshape(-1)
    onehot = (flat_routes[:, None] == jnp.arange(experts, dtype=jnp.int32)).astype(jnp.int32)
    slot_rank = jnp.sum((jnp.cumsum(onehot, axis=0) - 1) * onehot, axis=-1)
    slot_index = flat_routes * capacity + slot_rank
    token_index = jnp.arange(token_rows * TOP_K, dtype=jnp.int32) // TOP_K
    slot_rows = (
        jnp.full((experts * capacity,), token_rows, jnp.int32).at[slot_index].set(token_index)
    )
    padded = jnp.concatenate([normed, jnp.zeros((1, normed.shape[1]), jnp.bfloat16)], axis=0)
    outgoing = padded[slot_rows]
    arrived = lax.all_to_all(outgoing, "ep", split_axis=0, concat_axis=0, tiled=True)
    gate_part = jnp.dot(arrived, gate_weight[0], preferred_element_type=jnp.float32)
    up_part = jnp.dot(arrived, up_weight[0], preferred_element_type=jnp.float32)
    hidden = (jax.nn.silu(gate_part) * up_part).astype(jnp.bfloat16)
    expert_terms = jnp.dot(hidden, down_weight[0], preferred_element_type=jnp.float32)
    shared_gated = jnp.dot(normed, shared_gate, preferred_element_type=jnp.float32)
    shared_lifted = jnp.dot(normed, shared_up, preferred_element_type=jnp.float32)
    shared_hidden = (jax.nn.silu(shared_gated) * shared_lifted).astype(jnp.bfloat16)
    shared_terms = jnp.dot(shared_hidden, shared_down, preferred_element_type=jnp.float32)
    expert_sum, shared_sum = (
        lax.psum_scatter(
            expert_terms.astype(jnp.bfloat16), "tp", scatter_dimension=1, tiled=True
        ).astype(jnp.float32),
        lax.psum_scatter(
            shared_terms.astype(jnp.bfloat16), "tp", scatter_dimension=1, tiled=True
        ).astype(jnp.float32),
    )
    returned = lax.all_to_all(
        expert_sum.astype(jnp.bfloat16), "ep", split_axis=0, concat_axis=0, tiled=True
    )
    picked = returned[slot_index.reshape(token_rows, TOP_K)]
    moe_out = (
        jnp.sum(route_weight[..., None] * picked.astype(jnp.float32), axis=1) + shared_sum
    ).astype(jnp.bfloat16)
    return (attn_out, moe_out)


def solution(mesh):
    return jax.shard_map(
        local,
        mesh=mesh,
        in_specs=(
            P("ep", "tp"),
            P("ep", "tp"),
            P("ep", "tp"),
            P("tp"),
            P(),
            P("tp", None),
            P("ep", None),
            P(),
            P("ep", None),
            P("ep", None),
            P("ep", None, "tp"),
            P("ep", None, "tp"),
            P("ep", "tp", None),
            P(None, "tp"),
            P(None, "tp"),
            P("tp", None),
        ),
        out_specs=(P("ep", "tp"), P("ep", "tp")),
        check_vma=False,
    )
```

```python
import functools

import jax
import jax.numpy as jnp
import numpy as np
from jax import lax
from jax.experimental import pallas as pl
from jax.experimental.pallas import tpu as pltpu
from jax.sharding import PartitionSpec as P

TOP_K = 2
KEY_BLOCK = 128


theta_base = 500000.0
norm_eps = 1e-06
masked_low = -1e30


def rotate(inputs, positions):
    half_size = inputs.shape[-1] // 2
    frequency = theta_base ** (-(jnp.arange(half_size, dtype=jnp.float32) * 2.0) / inputs.shape[-1])
    angles = positions.astype(jnp.float32)[:, None] * frequency[None, :]
    cosine = jnp.cos(angles)[:, None, None, :]
    sine_part = jnp.sin(angles)[:, None, None, :]
    front_half = inputs[..., :half_size]
    back_half = inputs[..., half_size:]
    return jnp.concatenate(
        [front_half * cosine - back_half * sine_part, back_half * cosine + front_half * sine_part],
        axis=-1,
    )


def generic_attention(query_pairs, key_pairs, value_rows, head_lambda, head_gain, out_weight):
    local_rows = query_pairs.shape[0]
    local_heads = head_lambda.shape[0]
    head_size = query_pairs.shape[1] // (2 * local_heads)
    value_size = value_rows.shape[1] // local_heads
    positions = lax.axis_index("ep") * local_rows + jnp.arange(local_rows, dtype=jnp.int32)
    rot_queries = rotate(
        query_pairs.astype(jnp.float32).reshape(local_rows, local_heads, 2, head_size), positions
    ).astype(jnp.bfloat16)
    rot_keys = rotate(
        key_pairs.astype(jnp.float32).reshape(local_rows, local_heads, 2, head_size), positions
    ).astype(jnp.bfloat16)
    rot_keys = rot_keys.reshape(local_rows, local_heads * 2 * head_size)
    zero_init = (
        jnp.full((local_heads, 2, local_rows), masked_low, jnp.float32),
        jnp.zeros((local_heads, 2, local_rows), jnp.float32),
        jnp.zeros((local_heads, 2, local_rows, value_size), jnp.float32),
    )
    piece_keys = lax.all_gather(rot_keys, "ep", axis=0, tiled=True)
    piece_values = lax.all_gather(value_rows, "ep", axis=0, tiled=True)
    block_count = piece_keys.shape[0] // KEY_BLOCK
    group_size = 4
    group_count = block_count // group_size
    grouped_keys = piece_keys.reshape(group_count, group_size, KEY_BLOCK, local_heads, 2, head_size)
    grouped_values = piece_values.reshape(
        group_count, group_size, KEY_BLOCK, local_heads, value_size
    )

    def one_group(current, inputs):
        block_keys, block_values, group_index = inputs
        key_positions = group_index * group_size * KEY_BLOCK + jnp.arange(
            group_size * KEY_BLOCK, dtype=jnp.int32
        ).reshape(group_size, KEY_BLOCK)
        scores = jnp.einsum(
            "qhmd,gkhmd->hmqgk", rot_queries, block_keys, preferred_element_type=jnp.float32
        ) * head_size ** (-0.5)
        allowed = key_positions[None, :, :] <= positions[:, None, None]
        scores = jnp.where(allowed, scores, masked_low)
        block_max = jnp.max(scores, axis=-1)
        weights = jnp.where(allowed, jnp.exp(scores - block_max[..., None]), 0.0)
        block_sum = jnp.sum(weights, axis=-1)
        block_out = jnp.einsum(
            "hmqgk,gkhc->hmqgc",
            weights.astype(jnp.bfloat16),
            block_values,
            preferred_element_type=jnp.float32,
        )
        run_max, run_sum, run_out = current
        new_max = jnp.maximum(run_max, jnp.max(block_max, axis=-1))
        old_scale = jnp.exp(run_max - new_max)
        new_scale = jnp.exp(block_max - new_max[..., None])
        run_sum = run_sum * old_scale + jnp.sum(new_scale * block_sum, axis=-1)
        run_out = run_out * old_scale[..., None] + jnp.sum(
            new_scale[..., None] * block_out, axis=-2
        )
        return ((new_max, run_sum, run_out), None)

    result, _ = lax.scan(
        one_group,
        zero_init,
        (grouped_keys, grouped_values, jnp.arange(group_count, dtype=jnp.int32)),
    )
    run_max, run_sum, run_out = result
    map_outputs = run_out / run_sum[..., None]
    difference = map_outputs[:, 0] - head_lambda[:, None, None] * map_outputs[:, 1]
    inverse_rms = lax.rsqrt(jnp.mean(difference * difference, axis=-1, keepdims=True) + norm_eps)
    normed_heads = (difference * inverse_rms * head_gain).astype(jnp.bfloat16)
    head_rows = normed_heads.transpose(1, 0, 2).reshape(local_rows, local_heads * value_size)
    mixer_terms = jnp.dot(head_rows, out_weight, preferred_element_type=jnp.float32)
    attn_out = lax.psum_scatter(
        mixer_terms.astype(jnp.bfloat16), "tp", scatter_dimension=1, tiled=True
    )
    return attn_out


MESH = pl.DeviceIdType.MESH
f32, bf16 = jnp.float32, jnp.bfloat16


def mega_kernel(
    n, heads, n_tp, head_size, lam_ref, gain_ref, routes_ref, rw_ref, ffn_ref, turn_ref, base_ref,
    q_ref, k_ref, v_ref, x_ref, w_ref, wg_ref, wu_ref, wd_ref, sg_ref, su_ref, sd_ref,
    attn_ref, moe_ref,
    q_in, k_in, v_in, turn, x_in, xn, place, rq, rk, q_buf, k_buf, v_buf, vt_buf, st_buf, acc, m_buf,
    hn_send, hn_buf, w_buf, out_buf, own_buf, arr, wg, wu, wd, sg, su, sd,
    sh_send, sh_in, ex_send, ex_first, ex_held, ex_second, mix_send, mix_first, mix_held, mix_second, y_buf, ret, rw_pad,
    load, load_v, q_ss, q_rs, k_ss, k_rs, v_ss, v_rs, fk_ss, fk_rs, fv_ss, fv_rs, h_ss, h_rs,
    t_ss, t_rs, o_ss, o_rs, x_ss, x_rs, d_ss, d_rs, m_ss, m_rs, m2_ss, m2_rs, s_ss, s_rs, e_ss, e_rs, e2_ss, e2_rs, y_ss, y_rs,
):
    me, my_tp = lax.axis_index("ep"), lax.axis_index("tp")
    g = n // heads
    chip, core = me // g, me % g
    rows, width = k_buf.shape[1:]
    vw = v_buf.shape[2]
    sub = rows // g
    cap, piece = out_buf.shape[1:]
    tokens = xn.shape[0]
    top_k = rw_ref.shape[0]
    half = head_size // 2
    side = chip // (heads // 2)

    def mirrored(p):
        return p + side * (heads - 1 - 2 * p)

    near = mirrored(chip)

    def nearest(s):
        return mirrored(jnp.where(s <= near, near - s, s))

    barrier = pltpu.get_barrier_semaphore()
    for step in range(1, n):
        pl.semaphore_signal(barrier, inc=1, device_id={"ep": lax.rem(me + step, n)}, device_id_type=MESH)
    for step in range(1, n_tp):
        pl.semaphore_signal(barrier, inc=1, device_id={"tp": lax.rem(my_tp + step, n_tp)}, device_id_type=MESH)
    loads = [
        pltpu.make_async_copy(source, target, load.at[i])
        for i, (source, target) in enumerate((
            (x_ref, x_in), (turn_ref, turn), (k_ref, k_in), (q_ref, q_in),
            (sg_ref, sg), (su_ref, su), (sd_ref, sd),
            (wg_ref.at[0], wg), (wu_ref.at[0], wu), (wd_ref.at[0], wd), (w_ref, w_buf)))
    ]
    values = [
        pltpu.make_async_copy(v_ref.at[:, h * vw : (h + 1) * vw], v_in.at[h], load_v.at[h]) for h in range(heads)
    ]
    for copy in loads[:4]:
        copy.start()
    for copy in values:
        copy.start()

    def to_ep(source, target, send_sem, recv_sem, dest):
        return pltpu.make_async_remote_copy(
            source, target, send_sem, recv_sem, device_id={"ep": dest}, device_id_type=MESH)

    def to_tp(source, target, send_sem, recv_sem, dest):
        return pltpu.make_async_remote_copy(
            source, target, send_sem, recv_sem, device_id={"tp": dest}, device_id_type=MESH)

    def arrived(ref, sem):
        to_ep(ref, ref, sem, sem, lax.rem(me + 1, n)).wait_recv()

    peers = [lax.rem(my_tp + step, n_tp) for step in (*range(1, n_tp), 0)]
    across = (my_tp + 1 - 2 * (my_tp % 2), (my_tp + 2) % n_tp)
    corner = (across[0] + 2) % n_tp

    def reduction(send, first_in, held, second_in, ss, rs, ss2, rs2):
        def first_copies(h):
            return [
                to_tp(send.at[dest, h], first_in.at[h, i], ss.at[h, i], rs.at[h, i], across[h])
                for i, dest in enumerate((corner, across[h]))]

        def second_copy(h):
            return to_tp(held.at[h], second_in.at[h], ss2.at[h], rs2.at[h], across[1 - h])

        def pass_on(h):
            arrived(first_in.at[h, 0], rs.at[h, 0])
            held[h] = (send[across[1 - h], h].astype(f32) + first_in[h, 0].astype(f32)).astype(bf16)
            second_copy(h).start()

        def total(h):
            arrived(first_in.at[h, 1], rs.at[h, 1])
            arrived(second_in.at[h], rs2.at[h])
            return send[my_tp, h].astype(f32) + first_in[h, 1].astype(f32) + second_in[h].astype(f32)

        def sent():
            for h in range(2):
                for copy in (*first_copies(h), second_copy(h)):
                    copy.wait_send()

        return first_copies, pass_on, total, sent

    def columns(t):
        return pl.ds(pl.multiple_of(t * piece, piece), piece)

    expert = lax.broadcasted_iota(jnp.int32, (n, tokens), 0)
    chosen = [(routes_ref[k : k + 1, :] == expert).astype(f32) for k in range(top_k)]
    earlier = lax.broadcasted_iota(jnp.int32, (tokens, tokens), 0) <= lax.broadcasted_iota(jnp.int32, (tokens, tokens), 1)
    ranks = jnp.dot(sum(chosen).astype(bf16), earlier.astype(bf16), preferred_element_type=f32) - 1.0
    slot = ranks + (expert * cap).astype(f32)
    slots = [jnp.sum(c * slot, axis=0, keepdims=True) for c in chosen]
    slot_row = lax.broadcasted_iota(jnp.int32, (n * cap, tokens), 0).astype(f32)
    marks = [(slot_row == s).astype(f32) for s in slots]
    for k in range(top_k):
        place[k] = marks[k].astype(bf16).reshape(n, cap, tokens)
    loads[0].wait()
    x = x_in[...].astype(f32)
    inverse = lax.rsqrt(jnp.mean(x * x, axis=-1, keepdims=True) + norm_eps)
    xn[...] = (x * inverse * ffn_ref[...]).astype(bf16)
    out_buf[...] = jnp.dot(
        sum(marks).astype(bf16), xn[:, columns(my_tp)], preferred_element_type=f32).astype(bf16).reshape(n, cap, piece)

    def own_rows(dest):
        mark = place[0, dest]
        for k in range(1, top_k):
            mark = mark + place[k, dest]
        return jnp.dot(mark, xn[...], preferred_element_type=f32).astype(bf16)

    pl.semaphore_wait(barrier, n - 1 + n_tp - 1)
    for copy in loads[4:]:
        copy.start()

    def tok_copy(dest):
        return to_ep(out_buf.at[dest], arr.at[my_tp, me], t_ss.at[dest], t_rs.at[me], dest)

    def own_copy(step):
        dest = chip * g + lax.rem(core + step, g)
        return to_ep(own_buf.at[step - 1], arr.at[:, me], o_ss.at[step - 1], o_rs.at[me], dest)

    mate_chip = chip + 1 - 2 * (chip % 2)
    inner = (chip + side) % 2

    def send_tokens(first, last):
        for s in range(first, last):
            for c in range(g):
                tok_copy(nearest(s) * g + c).start()

    send_tokens(1, 2)

    @pl.when(inner == 1)
    def _():
        send_tokens(2, heads)

    for step in range(g):
        full = own_rows(chip * g + lax.rem(core + step, g))
        for t in range(n_tp):
            part = full[:, t * piece : (t + 1) * piece]
            if step == 0:
                arr[t, me] = part
            else:
                own_buf[step - 1, t] = part
        if step:
            own_copy(step).start()

    base_cos, base_sin = base_ref[0, pl.ds(me, 1)], base_ref[1, pl.ds(me, 1)]
    lane = lax.broadcasted_iota(jnp.int32, (1, width), 1)
    front = lane % head_size < half
    loads[1].wait()
    cosine = turn[0] * base_cos - turn[1] * base_sin
    sine = turn[1] * base_cos + turn[0] * base_sin
    sine = jnp.where(front, -sine, sine)

    def turned(source, h):
        x = source[:, h * width : (h + 1) * width].astype(f32)
        partner = jnp.where(front, pltpu.roll(x, width - half, 1), pltpu.roll(x, half, 1))
        return (x * cosine + partner * sine).astype(bf16)

    loads[2].wait()
    for h in range(heads):
        rk[h] = turned(k_in, h)
    loads[3].wait()
    for h in range(heads):
        rq[h] = turned(q_in, h) * jnp.asarray(head_size ** -0.5, bf16)
    for copy in values:
        copy.wait()

    def q_rows(dest):
        return pl.ds(pl.multiple_of(((dest % g + me) % g) * sub, sub), sub)

    def q_copy(dest):
        return to_ep(rq.at[dest // g, q_rows(dest)], q_buf.at[me], q_ss.at[dest], q_rs.at[me], dest)

    def k_copy(dest):
        return to_ep(rk.at[dest // g], k_buf.at[me], k_ss.at[dest], k_rs.at[me], dest)

    def v_copy(dest):
        return to_ep(v_in.at[dest // g], v_buf.at[me], v_ss.at[dest], v_rs.at[me], dest)

    def send_kv(p):
        k_copy(p * g + core).start()
        v_copy(p * g + core).start()

    def send_q(p):
        for c in range(g):
            q_copy(p * g + c).start()

    for step in range(1, g):
        q_copy(chip * g + lax.rem(core + step, g)).start()
    send_kv(mate_chip)
    send_q(mate_chip)

    @pl.when(inner == 0)
    def _():
        send_tokens(2, heads)

    @pl.when(side == 0)
    def _():
        for i in (0, 1):
            send_kv(2 + (inner + i) % 2)
            send_q(2 + (inner + i) % 2)

    @pl.when(side == 1)
    def _():
        for s in range(2, heads):
            send_q(nearest(s))
        for i in (1, 0):
            send_kv((inner + i) % 2)

    q_buf[me] = rq[chip, q_rows(me)]
    k_buf[me] = rk[chip]
    v_buf[me] = v_in[chip]

    def gated(gate, up):
        return (gate / (1.0 + jnp.exp(-gate)) * up).astype(bf16)

    for i in (4, 5, 6):
        loads[i].wait()
    hidden = gated(
        jnp.dot(xn[...], sg[...], preferred_element_type=f32), jnp.dot(xn[...], su[...], preferred_element_type=f32))

    def sh_copy(dest):
        return to_tp(sh_send.at[dest], sh_in.at[my_tp], s_ss.at[dest], s_rs.at[my_tp], dest)

    for dest in peers:
        sh_send[dest] = jnp.dot(hidden, sd[:, columns(dest)], preferred_element_type=f32).astype(bf16)
        if dest is not peers[-1]:
            sh_copy(dest).start()

    lam = lam_ref[chip]
    gain = gain_ref[...]
    vt_rows = vt_buf.shape[1]
    keys = g * rows
    lane_row = lax.broadcasted_iota(jnp.int32, (sub, width), 1)

    def forward(source, step):
        to = chip * g + lax.rem(core + step, g)
        return (
            to_ep(k_buf.at[source], k_buf.at[source], fk_ss.at[source, step], fk_rs.at[source], to),
            to_ep(v_buf.at[source], v_buf.at[source], fv_ss.at[source, step], fv_rs.at[source], to),
        )

    def prepare_kv(e):
        vt_buf[e, :vw] = v_buf[e].astype(f32).T.astype(bf16)
        vt_buf[e, vw:] = jnp.ones((vt_rows - vw, rows), bf16)

    def receive_kv(p):
        direct = p * g + core

        @pl.when(direct != me)
        def _():
            arrived(k_buf.at[direct], k_rs.at[direct])
            arrived(v_buf.at[direct], v_rs.at[direct])

        for step in range(1, g):
            for copy in forward(direct, step):
                copy.start()
        prepare_kv(direct)

    def complete_kv(p):
        for step in range(1, g):
            other = p * g + lax.rem(core + step, g)
            arrived(k_buf.at[other], fk_rs.at[other])
            arrived(v_buf.at[other], fv_rs.at[other])
            prepare_kv(other)

    def receive_q(p):
        for c in range(g):
            e = p * g + c

            @pl.when(e != me)
            def _():
                arrived(q_buf.at[e], q_rs.at[e])

            q = q_buf[e]
            zero = jnp.zeros_like(q)
            st_buf[p, 2 * c * sub : (2 * c + 1) * sub] = jnp.where(lane_row < width // 2, q, zero)
            st_buf[p, (2 * c + 1) * sub : (2 * c + 2) * sub] = jnp.where(lane_row < width // 2, zero, q)
        m_buf[p] = jnp.full((1, keys), masked_low, f32)
        acc[p] = jnp.zeros((vt_rows, keys), f32)

    def tile(p, e, first=0, diagonal=False):
        span = slice(first, keys)
        size = keys - first
        s = lax.dot_general(k_buf[e], st_buf[p, span], (((1,), (1,)), ((), ())), preferred_element_type=f32)
        if diagonal:
            key = lax.broadcasted_iota(jnp.int32, (rows, size), 0) + first
            column = lax.broadcasted_iota(jnp.int32, (rows, size), 1) + first
            block = column // rows
            query = block * rows + column % sub + (core + block) % g * sub
            s = jnp.where(key <= query, s, masked_low)
        old = m_buf[p, :, span]
        m = jnp.maximum(old, jnp.max(s, axis=0, keepdims=True))
        weights = jnp.exp(s - m).astype(bf16)
        m_buf[p, :, span] = m
        acc[p, :, span] = acc[p, :, span] * jnp.exp(old - m) + jnp.dot(
            vt_buf[e], weights, preferred_element_type=f32)

    def hn_copy(dest):
        return to_ep(hn_send.at[dest], hn_buf.at[me], h_ss.at[dest], h_rs.at[me], dest)

    def finish(p):
        a = (acc[p, :vw] / acc[p, vw : vw + 1]).T
        for c in range(g):
            e = p * g + c
            diff = a[2 * c * sub : (2 * c + 1) * sub] - lam * a[(2 * c + 1) * sub : (2 * c + 2) * sub]
            inverse = lax.rsqrt(jnp.mean(diff * diff, axis=-1, keepdims=True) + norm_eps)
            hn_send[e] = (diff * inverse * gain).astype(bf16)

            @pl.when(e != me)
            def _():
                hn_copy(e).start()

    def spread_copy(p, i):
        part = arr.at[my_tp, pl.ds(p * g, g)]
        return to_tp(part, part, x_ss.at[p, i], x_rs.at[my_tp, p], across[i])

    def relay_copy(p, c):
        part = arr.at[across[c], p * g + c]
        return to_tp(part, part, d_ss.at[p, c], d_rs.at[p, c], across[1 - c])

    def spread(s):
        p = nearest(s)
        for c in range(g):
            arrived(arr.at[my_tp, p * g + c], t_rs.at[p * g + c])
        for i in range(2):
            spread_copy(p, i).start()

    def relay(s):
        p = nearest(s)
        for c in range(2):
            arrived(arr.at[across[c], pl.ds(p * g, g)], x_rs.at[across[c], p])
            relay_copy(p, c).start()

    ex_copies, ex_pass, ex_total, ex_sent = reduction(
        ex_send, ex_first, ex_held, ex_second, e_ss, e_rs, e2_ss, e2_rs)
    mix_copies, mix_pass, mix_total, mix_sent = reduction(
        mix_send, mix_first, mix_held, mix_second, m_ss, m_rs, m2_ss, m2_rs)
    half_rows = n // 2 * cap

    def routed():
        for step in range(1, g):
            other = chip * g + lax.rem(core + step, g)
            arrived(arr.at[:, other], o_rs.at[other])
        for s in range(1, heads):
            for c in range(2):
                arrived(arr.at[corner, nearest(s) * g + c], d_rs.at[nearest(s), c])
        for i in (7, 8, 9):
            loads[i].wait()
        gate = up = None
        for t in range(n_tp):
            block = arr[t].reshape(n * cap, piece)
            span = slice(t * piece, (t + 1) * piece)
            gate_part = jnp.dot(block, wg[span, :], preferred_element_type=f32)
            up_part = jnp.dot(block, wu[span, :], preferred_element_type=f32)
            gate = gate_part if gate is None else gate + gate_part
            up = up_part if up is None else up + up_part
        hidden = gated(gate, up)

        def down(dest, h):
            ex_send[dest, h] = jnp.dot(
                hidden[h * half_rows : (h + 1) * half_rows], wd[:, columns(dest)],
                preferred_element_type=f32).astype(bf16)

        for i in range(2):
            for h in range(2):
                down((corner, across[h])[i], h)
                ex_copies(h)[i].start()
        for h in range(2):
            down(across[1 - h], h)
            down(my_tp, h)

    low, pair = 1 - side, 2 * side

    def phase(s, _):
        early = (4 - s) // 3
        second = (s // 2) * (1 - s // 3)
        third = (s // 3) * (1 - s // 4)
        fourth = s // 4
        newest = early * (chip + s * (mate_chip - chip)) + (1 - early) * (
            low * (third * (2 + inner) + fourth * (3 - inner)) + side * (second * (1 - inner) + third * inner))
        with_q = early + side * (second + third)
        with_kv = with_q + low * (third + fourth)
        split = third * (1 - inner) + fourth * inner

        @pl.when(low * second == 1)
        def _():
            for p in (2, 3):
                receive_q(p)

        @pl.when(with_kv == 1)
        def _():
            receive_kv(newest)

        @pl.when(with_q == 1)
        def _():
            receive_q(newest)

        def diagonal(step, _):
            c = (core + step) % g

            @pl.when(step == 1)
            def _():
                complete_kv(newest)

            for first in range(g):
                @pl.when(c == first)
                def _():
                    tile(newest, newest * g + first, first * rows, True)

            return 0

        @pl.when(with_kv == 1)
        def _():
            lax.fori_loop(0, g, diagonal, 0)

        @pl.when(low * (third * (1 - inner) + fourth) + side * (second * inner + third * (1 - inner)) == 1)
        def _():
            finish(newest)

        def full(i, _):
            p = early * (pair + 1) + second * (2 + low * (i // 2) + side * i) + low * split * 3 + side * third * (1 + i)
            j = early * pair + second * (low * (i % 2) + side * newest) + low * split * 2 + side * third * newest * ((i + 1) // 2)
            for c in range(g):
                tile(p, j * g + c)

            @pl.when(third * side + low * fourth * inner == 1)
            def _():
                finish(p)

            return 0

        lax.fori_loop(0, early * s + second * (4 * low + 2 * side) + low * split + side * third * 3, full, 0)

        def done(p, _):
            finish(p)
            return 0

        @pl.when(early * s * low == 1)
        def _():
            lax.fori_loop(pair, pair + 2, done, 0)

        @pl.when(s == 0)
        def _():
            spread(1)

        first = 1 - inner

        @pl.when(s == 1 - first)
        def _():
            for step in range(2, heads):
                spread(step)
            for step in range(1, heads):
                relay(step)

        @pl.when(s == 1)
        def _():
            routed()

        @pl.when(s == 2)
        def _():
            for h in range(2):
                ex_pass(h)

        return 0

    lax.fori_loop(0, heads + 1, phase, 0)

    hn_buf[me] = hn_send[me]
    for step in range(1, n):
        source = lax.rem(me + step, n)
        arrived(hn_buf.at[source], h_rs.at[source])
    loads[10].wait()
    normed = [
        jnp.concatenate([hn_buf[h * g + (part + n - me) % g] for h in range(heads)], axis=1) for part in range(g)]

    def project(dest, h):
        mix_send[dest, h] = jnp.dot(normed[h], w_buf[:, columns(dest)], preferred_element_type=f32).astype(bf16)

    for i in range(2):
        for h in range(2):
            project((corner, across[h])[i], h)
            mix_copies(h)[i].start()
    for h in range(2):
        project(across[1 - h], h)
        project(my_tp, h)
    def y_copy(dest):
        return to_ep(y_buf.at[dest], ret.at[me], y_ss.at[dest], y_rs.at[me], dest)

    for h in range(2):
        y_buf[h * n // 2 : (h + 1) * n // 2] = ex_total(h).astype(bf16).reshape(n // 2, cap, piece)
    for step in range(1, n):
        hn_copy(lax.rem(me + step, n)).wait_send()
    for s in range(heads - 1, 0, -1):
        for c in range(g):
            y_copy(nearest(s) * g + c).start()
    for step in range(1, g):
        y_copy(chip * g + lax.rem(core + step, g)).start()
    ret[me] = y_buf[me]
    out = sh_send[my_tp].astype(f32)
    for source in peers[:-1]:
        arrived(sh_in.at[source], s_rs.at[source])
        out = out + sh_in[source].astype(f32)
    rw_pad[...] = jnp.zeros_like(rw_pad)
    rw_pad[:top_k, :tokens] = rw_ref[...]
    scale = rw_pad[...].T
    for h in range(2):
        mix_pass(h)
    for step in range(1, n):
        source = lax.rem(me + step, n)
        arrived(ret.at[source], y_rs.at[source])
    returned = ret[...].reshape(n * cap, piece)
    for k in range(top_k):
        out = out + scale[:tokens, k : k + 1] * lax.dot_general(
            place[k].reshape(n * cap, tokens), returned, (((0,), (0,)), ((), ())), preferred_element_type=f32)
    moe_ref[...] = out.astype(bf16)
    for h in range(2):
        attn_ref[h * sub : (h + 1) * sub] = mix_total(h).astype(bf16)
    for s in range(1, heads):
        p = nearest(s)
        k_copy(p * g + core).wait_send()
        v_copy(p * g + core).wait_send()
        for c in range(g):
            tok_copy(p * g + c).wait_send()
        for i in range(2):
            spread_copy(p, i).wait_send()
            relay_copy(p, i).wait_send()
    for step in range(1, n):
        dest = lax.rem(me + step, n)
        q_copy(dest).wait_send()
        y_copy(dest).wait_send()
    for step in range(1, g):
        own_copy(step).wait_send()
    for p in range(heads):
        for step in range(1, g):
            for copy in forward(p * g + core, step):
                copy.wait_send()
    for dest in peers[:-1]:
        sh_copy(dest).wait_send()
    ex_sent()
    mix_sent()


def turn_tables(rows, n, head_size):
    half = head_size // 2
    frequency = theta_base ** (-(np.arange(half) * 2.0) / head_size)

    def waves(positions):
        angles = np.tile(positions[:, None] * frequency[None, :], (1, 4))
        return np.stack([np.cos(angles), np.sin(angles)]).astype(np.float32)

    return waves(np.arange(rows)), waves(np.arange(n) * rows)


def exchange_all(
    query_pairs, key_pairs, value_rows, head_lambda, head_gain, out_weight, moe_input, ffn_gain, routes, route_weight,
    gate_weight, up_weight, down_weight, shared_gate, shared_up, shared_down,
):
    n, n_tp = lax.axis_size("ep"), lax.axis_size("tp")
    tokens, model = moe_input.shape
    piece = model // n_tp
    rows = query_pairs.shape[0]
    heads = head_lambda.shape[0]
    width = query_pairs.shape[1] // heads
    head_size = width // 2
    vw = value_rows.shape[1] // heads
    g = n // heads
    sub = rows // g
    keys = g * rows
    cap = -(-(tokens * TOP_K * 5 // (4 * n)) // 8) * 8
    hidden, shared = gate_weight.shape[2], shared_gate.shape[1]
    turns, bases = turn_tables(rows, n, head_size)
    any_spec = pl.BlockSpec(memory_space=pl.ANY)
    vmem = pl.BlockSpec(memory_space=pltpu.VMEM)
    dma = pltpu.SemaphoreType.DMA
    buffers = [
        (rows, heads * width), (rows, heads * width), (heads, rows, vw), ((2, rows, width), f32),
        (tokens, model), (tokens, model), (TOP_K, n, cap, tokens), (heads, rows, width), (heads, rows, width),
        (n, sub, width), (n, rows, width), (n, rows, vw), (n, vw + 8, rows), (heads, 2 * rows, width),
        ((heads, vw + 8, keys), f32), ((heads, 1, keys), f32), (n, sub, vw), (n, sub, vw), out_weight.shape,
        (n, cap, piece), (g - 1, n_tp, cap, piece), (n_tp, n, cap, piece),
        (model, hidden), (model, hidden), (hidden, model), (model, shared), (model, shared), (shared, model),
        (n_tp, tokens, piece), (n_tp, tokens, piece),
        (n_tp, 2, n // 2 * cap, piece), (2, 2, n // 2 * cap, piece), (2, n // 2 * cap, piece), (2, n // 2 * cap, piece),
        (n_tp, 2, sub, piece), (2, 2, sub, piece), (2, sub, piece), (2, sub, piece), (n, cap, piece), (n, cap, piece),
        ((8, -(-tokens // 128) * 128), f32),
    ]
    semaphores = [
        (11,), (heads,), (n,), (n,), (n,), (n,), (n,), (n,), (n, g), (n,), (n, g), (n,), (n,), (n,),
        (n,), (n,), (g - 1,), (n,), (heads, 2), (n_tp, heads), (heads, 2), (heads, 2),
        (2, 2), (2, 2), (2,), (2,), (n_tp,), (n_tp,), (2, 2), (2, 2), (2,), (2,), (n,), (n,),
    ]
    results = pl.pallas_call(
        functools.partial(mega_kernel, n, heads, n_tp, head_size),
        out_shape=(
            jax.ShapeDtypeStruct((rows, piece), bf16),
            jax.ShapeDtypeStruct((tokens, piece), bf16),
        ),
        in_specs=[pl.BlockSpec(memory_space=pltpu.SMEM)] + [vmem] * 4 + [any_spec, vmem] + [any_spec] * 11,
        out_specs=(vmem, vmem),
        scratch_shapes=[
            pltpu.VMEM(shape[0], shape[1]) if isinstance(shape[0], tuple) else pltpu.VMEM(shape, bf16)
            for shape in buffers
        ] + [dma(shape) for shape in semaphores],
        compiler_params=pltpu.CompilerParams(
            collective_id=0, has_side_effects=True, vmem_limit_bytes=60 * 2**20),
        cost_estimate=pl.CostEstimate(flops=30 * 10**9, bytes_accessed=24 * 2**20, transcendentals=6 * 10**6),
        name="exchange",
    )(
        head_lambda, head_gain.reshape(1, vw), routes.T, route_weight.T, ffn_gain.reshape(1, model),
        jnp.asarray(turns), jnp.asarray(bases), query_pairs, key_pairs, value_rows, moe_input, out_weight,
        gate_weight, up_weight, down_weight, shared_gate, shared_up, shared_down)
    return pl.pallas_call(
        store_kernel,
        out_shape=tuple(jax.ShapeDtypeStruct(r.shape, r.dtype) for r in results),
        in_specs=[any_spec] * 2,
        out_specs=(any_spec, any_spec),
        scratch_shapes=[pltpu.VMEM(r.shape, r.dtype) for r in results] + [dma((2,)), dma((2,))],
        name="store",
    )(*results)


def store_kernel(attn_ref, moe_ref, attn_out, moe_out, attn_buf, moe_buf, in_sems, out_sems):
    refs = ((attn_ref, attn_buf, attn_out), (moe_ref, moe_buf, moe_out))
    ins = [pltpu.make_async_copy(source, buf, in_sems.at[i]) for i, (source, buf, _) in enumerate(refs)]
    outs = [pltpu.make_async_copy(buf, target, out_sems.at[i]) for i, (_, buf, target) in enumerate(refs)]
    for copy in ins:
        copy.start()
    for i in (1, 0):
        ins[i].wait()
        outs[i].start()
    for copy in outs:
        copy.wait()


def local(
    query_pairs,
    key_pairs,
    value_rows,
    head_lambda,
    head_gain,
    out_weight,
    moe_input,
    ffn_gain,
    routes,
    route_weight,
    gate_weight,
    up_weight,
    down_weight,
    shared_gate,
    shared_up,
    shared_down,
):
    n = lax.axis_size("ep")
    heads = head_lambda.shape[0]
    rows = query_pairs.shape[0]
    fits = n == 2 * heads and heads == 4 and lax.axis_size("tp") == 4 and (rows * heads) % (n * 64) == 0
    if fits:
        return exchange_all(
            query_pairs, key_pairs, value_rows, head_lambda, head_gain, out_weight, moe_input, ffn_gain, routes,
            route_weight, gate_weight, up_weight, down_weight, shared_gate, shared_up, shared_down,
        )
    row_values = moe_input.astype(jnp.float32)
    inverse_norm = lax.rsqrt(jnp.mean(row_values * row_values, axis=-1, keepdims=True) + norm_eps)
    normed = (row_values * inverse_norm * ffn_gain).astype(jnp.bfloat16)
    attn_out = generic_attention(query_pairs, key_pairs, value_rows, head_lambda, head_gain, out_weight)
    token_rows = normed.shape[0]
    experts = lax.axis_size("ep")
    capacity = token_rows * TOP_K * 5 // (4 * experts)
    flat_routes = routes.reshape(-1)
    onehot = (flat_routes[:, None] == jnp.arange(experts, dtype=jnp.int32)).astype(jnp.int32)
    slot_rank = jnp.sum((jnp.cumsum(onehot, axis=0) - 1) * onehot, axis=-1)
    slot_index = flat_routes * capacity + slot_rank
    token_index = jnp.arange(token_rows * TOP_K, dtype=jnp.int32) // TOP_K
    slot_rows = (
        jnp.full((experts * capacity,), token_rows, jnp.int32).at[slot_index].set(token_index)
    )
    padded = jnp.concatenate([normed, jnp.zeros((1, normed.shape[1]), jnp.bfloat16)], axis=0)
    outgoing = padded[slot_rows]
    arrived = lax.all_to_all(outgoing, "ep", split_axis=0, concat_axis=0, tiled=True)
    gate_part = jnp.dot(arrived, gate_weight[0], preferred_element_type=jnp.float32)
    up_part = jnp.dot(arrived, up_weight[0], preferred_element_type=jnp.float32)
    hidden = (jax.nn.silu(gate_part) * up_part).astype(jnp.bfloat16)
    expert_terms = jnp.dot(hidden, down_weight[0], preferred_element_type=jnp.float32)
    shared_gated = jnp.dot(normed, shared_gate, preferred_element_type=jnp.float32)
    shared_lifted = jnp.dot(normed, shared_up, preferred_element_type=jnp.float32)
    shared_hidden = (jax.nn.silu(shared_gated) * shared_lifted).astype(jnp.bfloat16)
    shared_terms = jnp.dot(shared_hidden, shared_down, preferred_element_type=jnp.float32)
    expert_sum, shared_sum = (
        lax.psum_scatter(
            expert_terms.astype(jnp.bfloat16), "tp", scatter_dimension=1, tiled=True
        ).astype(jnp.float32),
        lax.psum_scatter(
            shared_terms.astype(jnp.bfloat16), "tp", scatter_dimension=1, tiled=True
        ).astype(jnp.float32),
    )
    returned = lax.all_to_all(
        expert_sum.astype(jnp.bfloat16), "ep", split_axis=0, concat_axis=0, tiled=True
    )
    picked = returned[slot_index.reshape(token_rows, TOP_K)]
    moe_out = (
        jnp.sum(route_weight[..., None] * picked.astype(jnp.float32), axis=1) + shared_sum
    ).astype(jnp.bfloat16)
    return (attn_out, moe_out)


def solution(mesh):
    return jax.shard_map(
        local,
        mesh=mesh,
        in_specs=(
            P("ep", "tp"),
            P("ep", "tp"),
            P("ep", "tp"),
            P("tp"),
            P(),
            P("tp", None),
            P("ep", None),
            P(),
            P("ep", None),
            P("ep", None),
            P("ep", None, "tp"),
            P("ep", None, "tp"),
            P("ep", "tp", None),
            P(None, "tp"),
            P(None, "tp"),
            P("tp", None),
        ),
        out_specs=(P("ep", "tp"), P("ep", "tp")),
        check_vma=False,
    )
```

```python
import functools

import jax
import jax.numpy as jnp
import numpy as np
from jax import lax
from jax.experimental import pallas as pl
from jax.experimental.pallas import tpu as pltpu
from jax.sharding import PartitionSpec as P

TOP_K = 2
KEY_BLOCK = 128


theta_base = 500000.0
norm_eps = 1e-06
masked_low = -1e30


def rotate(inputs, positions):
    half_size = inputs.shape[-1] // 2
    frequency = theta_base ** (-(jnp.arange(half_size, dtype=jnp.float32) * 2.0) / inputs.shape[-1])
    angles = positions.astype(jnp.float32)[:, None] * frequency[None, :]
    cosine = jnp.cos(angles)[:, None, None, :]
    sine_part = jnp.sin(angles)[:, None, None, :]
    front_half = inputs[..., :half_size]
    back_half = inputs[..., half_size:]
    return jnp.concatenate(
        [front_half * cosine - back_half * sine_part, back_half * cosine + front_half * sine_part],
        axis=-1,
    )


def generic_attention(query_pairs, key_pairs, value_rows, head_lambda, head_gain, out_weight):
    local_rows = query_pairs.shape[0]
    local_heads = head_lambda.shape[0]
    head_size = query_pairs.shape[1] // (2 * local_heads)
    value_size = value_rows.shape[1] // local_heads
    positions = lax.axis_index("ep") * local_rows + jnp.arange(local_rows, dtype=jnp.int32)
    rot_queries = rotate(
        query_pairs.astype(jnp.float32).reshape(local_rows, local_heads, 2, head_size), positions
    ).astype(jnp.bfloat16)
    rot_keys = rotate(
        key_pairs.astype(jnp.float32).reshape(local_rows, local_heads, 2, head_size), positions
    ).astype(jnp.bfloat16)
    rot_keys = rot_keys.reshape(local_rows, local_heads * 2 * head_size)
    zero_init = (
        jnp.full((local_heads, 2, local_rows), masked_low, jnp.float32),
        jnp.zeros((local_heads, 2, local_rows), jnp.float32),
        jnp.zeros((local_heads, 2, local_rows, value_size), jnp.float32),
    )
    piece_keys = lax.all_gather(rot_keys, "ep", axis=0, tiled=True)
    piece_values = lax.all_gather(value_rows, "ep", axis=0, tiled=True)
    block_count = piece_keys.shape[0] // KEY_BLOCK
    group_size = 4
    group_count = block_count // group_size
    grouped_keys = piece_keys.reshape(group_count, group_size, KEY_BLOCK, local_heads, 2, head_size)
    grouped_values = piece_values.reshape(
        group_count, group_size, KEY_BLOCK, local_heads, value_size
    )

    def one_group(current, inputs):
        block_keys, block_values, group_index = inputs
        key_positions = group_index * group_size * KEY_BLOCK + jnp.arange(
            group_size * KEY_BLOCK, dtype=jnp.int32
        ).reshape(group_size, KEY_BLOCK)
        scores = jnp.einsum(
            "qhmd,gkhmd->hmqgk", rot_queries, block_keys, preferred_element_type=jnp.float32
        ) * head_size ** (-0.5)
        allowed = key_positions[None, :, :] <= positions[:, None, None]
        scores = jnp.where(allowed, scores, masked_low)
        block_max = jnp.max(scores, axis=-1)
        weights = jnp.where(allowed, jnp.exp(scores - block_max[..., None]), 0.0)
        block_sum = jnp.sum(weights, axis=-1)
        block_out = jnp.einsum(
            "hmqgk,gkhc->hmqgc",
            weights.astype(jnp.bfloat16),
            block_values,
            preferred_element_type=jnp.float32,
        )
        run_max, run_sum, run_out = current
        new_max = jnp.maximum(run_max, jnp.max(block_max, axis=-1))
        old_scale = jnp.exp(run_max - new_max)
        new_scale = jnp.exp(block_max - new_max[..., None])
        run_sum = run_sum * old_scale + jnp.sum(new_scale * block_sum, axis=-1)
        run_out = run_out * old_scale[..., None] + jnp.sum(
            new_scale[..., None] * block_out, axis=-2
        )
        return ((new_max, run_sum, run_out), None)

    result, _ = lax.scan(
        one_group,
        zero_init,
        (grouped_keys, grouped_values, jnp.arange(group_count, dtype=jnp.int32)),
    )
    run_max, run_sum, run_out = result
    map_outputs = run_out / run_sum[..., None]
    difference = map_outputs[:, 0] - head_lambda[:, None, None] * map_outputs[:, 1]
    inverse_rms = lax.rsqrt(jnp.mean(difference * difference, axis=-1, keepdims=True) + norm_eps)
    normed_heads = (difference * inverse_rms * head_gain).astype(jnp.bfloat16)
    head_rows = normed_heads.transpose(1, 0, 2).reshape(local_rows, local_heads * value_size)
    mixer_terms = jnp.dot(head_rows, out_weight, preferred_element_type=jnp.float32)
    attn_out = lax.psum_scatter(
        mixer_terms.astype(jnp.bfloat16), "tp", scatter_dimension=1, tiled=True
    )
    return attn_out


MESH = pl.DeviceIdType.MESH
f32, bf16 = jnp.float32, jnp.bfloat16


def mega_kernel(
    n, heads, n_tp, head_size, lam_ref, gain_ref, routes_ref, rw_ref, ffn_ref, turn_ref, base_ref,
    q_ref, k_ref, v_ref, x_ref, w_ref, wg_ref, wu_ref, wd_ref, sg_ref, su_ref, sd_ref,
    attn_ref, moe_ref,
    q_in, k_in, v_in, turn, x_in, xn, place, rq, rk, q_buf, k_buf, v_buf, vt_buf, st_buf, acc, m_buf,
    hn_send, hn_buf, w_buf, out_buf, own_buf, arr, wg, wu, wd, sg, su, sd,
    sh_send, sh_first, sh_held, sh_second, ex_send, ex_first, ex_held, ex_second, mix_send, mix_first, mix_held, mix_second, y_buf, ret, rw_pad,
    load, load_v, q_ss, q_rs, k_ss, k_rs, v_ss, v_rs, fk_ss, fk_rs, fv_ss, fv_rs, h_ss, h_rs,
    t_ss, t_rs, o_ss, o_rs, x_ss, x_rs, d_ss, d_rs, m_ss, m_rs, m2_ss, m2_rs, s_ss, s_rs, s2_ss, s2_rs, e_ss, e_rs, e2_ss, e2_rs, y_ss, y_rs,
):
    me, my_tp = lax.axis_index("ep"), lax.axis_index("tp")
    g = n // heads
    chip, core = me // g, me % g
    rows, width = k_buf.shape[1:]
    vw = v_buf.shape[2]
    sub = rows // g
    cap, piece = out_buf.shape[1:]
    tokens = xn.shape[0]
    top_k = rw_ref.shape[0]
    half = head_size // 2
    side = chip // (heads // 2)

    def mirrored(p):
        return p + side * (heads - 1 - 2 * p)

    near = mirrored(chip)

    def nearest(s):
        return mirrored(jnp.where(s <= near, near - s, s))

    barrier = pltpu.get_barrier_semaphore()
    for step in range(1, n):
        pl.semaphore_signal(barrier, inc=1, device_id={"ep": lax.rem(me + step, n)}, device_id_type=MESH)
    for step in range(1, n_tp):
        pl.semaphore_signal(barrier, inc=1, device_id={"tp": lax.rem(my_tp + step, n_tp)}, device_id_type=MESH)
    loads = [
        pltpu.make_async_copy(source, target, load.at[i])
        for i, (source, target) in enumerate((
            (x_ref, x_in), (turn_ref, turn), (k_ref, k_in), (q_ref, q_in),
            (sg_ref, sg), (su_ref, su), (sd_ref, sd),
            (wg_ref.at[0], wg), (wu_ref.at[0], wu), (wd_ref.at[0], wd), (w_ref, w_buf)))
    ]
    values = [
        pltpu.make_async_copy(v_ref.at[:, h * vw : (h + 1) * vw], v_in.at[h], load_v.at[h]) for h in range(heads)
    ]
    for copy in loads[:4]:
        copy.start()
    for copy in values:
        copy.start()

    def to_ep(source, target, send_sem, recv_sem, dest):
        return pltpu.make_async_remote_copy(
            source, target, send_sem, recv_sem, device_id={"ep": dest}, device_id_type=MESH)

    def to_tp(source, target, send_sem, recv_sem, dest):
        return pltpu.make_async_remote_copy(
            source, target, send_sem, recv_sem, device_id={"tp": dest}, device_id_type=MESH)

    def arrived(ref, sem):
        to_ep(ref, ref, sem, sem, lax.rem(me + 1, n)).wait_recv()

    across = (my_tp + 1 - 2 * (my_tp % 2), (my_tp + 2) % n_tp)
    corner = (across[0] + 2) % n_tp

    def reduction(send, first_in, held, second_in, ss, rs, ss2, rs2, pre=()):
        at = lambda ref, *index: ref.at[(*pre, *index)]

        def first_copies(h):
            return [
                to_tp(at(send, dest, h), at(first_in, h, i), at(ss, h, i), at(rs, h, i), across[h])
                for i, dest in enumerate((corner, across[h]))]

        def second_copy(h):
            return to_tp(at(held, h), at(second_in, h), at(ss2, h), at(rs2, h), across[1 - h])

        def pass_on(h):
            arrived(at(first_in, h, 0), at(rs, h, 0))
            own = send[(*pre, across[1 - h], h)].astype(f32)
            held[(*pre, h)] = (own + first_in[(*pre, h, 0)].astype(f32)).astype(bf16)
            second_copy(h).start()

        def total(h):
            arrived(at(first_in, h, 1), at(rs, h, 1))
            arrived(at(second_in, h), at(rs2, h))
            own = send[(*pre, my_tp, h)].astype(f32)
            return own + first_in[(*pre, h, 1)].astype(f32) + second_in[(*pre, h)].astype(f32)

        def sent():
            for h in range(2):
                for copy in (*first_copies(h), second_copy(h)):
                    copy.wait_send()

        return first_copies, pass_on, total, sent

    def columns(t):
        return pl.ds(pl.multiple_of(t * piece, piece), piece)

    expert = lax.broadcasted_iota(jnp.int32, (n, tokens), 0)
    chosen = [(routes_ref[k : k + 1, :] == expert).astype(f32) for k in range(top_k)]
    earlier = lax.broadcasted_iota(jnp.int32, (tokens, tokens), 0) <= lax.broadcasted_iota(jnp.int32, (tokens, tokens), 1)
    ranks = jnp.dot(sum(chosen).astype(bf16), earlier.astype(bf16), preferred_element_type=f32) - 1.0
    slot = ranks + (expert * cap).astype(f32)
    slots = [jnp.sum(c * slot, axis=0, keepdims=True) for c in chosen]
    slot_row = lax.broadcasted_iota(jnp.int32, (n * cap, tokens), 0).astype(f32)
    marks = [(slot_row == s).astype(f32) for s in slots]
    for k in range(top_k):
        place[k] = marks[k].astype(bf16).reshape(n, cap, tokens)
    loads[0].wait()
    x = x_in[...].astype(f32)
    inverse = lax.rsqrt(jnp.mean(x * x, axis=-1, keepdims=True) + norm_eps)
    xn[...] = (x * inverse * ffn_ref[...]).astype(bf16)
    out_buf[...] = jnp.dot(
        sum(marks).astype(bf16), xn[:, columns(my_tp)], preferred_element_type=f32).astype(bf16).reshape(n, cap, piece)

    def own_rows(dest):
        mark = place[0, dest]
        for k in range(1, top_k):
            mark = mark + place[k, dest]
        return jnp.dot(mark, xn[...], preferred_element_type=f32).astype(bf16)

    pl.semaphore_wait(barrier, n - 1 + n_tp - 1)
    for copy in loads[4:]:
        copy.start()

    def tok_copy(dest):
        return to_ep(out_buf.at[dest], arr.at[my_tp, me], t_ss.at[dest], t_rs.at[me], dest)

    def own_copy(step):
        dest = chip * g + lax.rem(core + step, g)
        return to_ep(own_buf.at[step - 1], arr.at[:, me], o_ss.at[step - 1], o_rs.at[me], dest)

    mate_chip = chip + 1 - 2 * (chip % 2)
    inner = (chip + side) % 2

    def send_tokens(first, last):
        for s in range(first, last):
            for c in range(g):
                tok_copy(nearest(s) * g + c).start()

    send_tokens(1, 2)

    @pl.when(inner == 1)
    def _():
        send_tokens(2, heads)

    for step in range(g):
        full = own_rows(chip * g + lax.rem(core + step, g))
        for t in range(n_tp):
            part = full[:, t * piece : (t + 1) * piece]
            if step == 0:
                arr[t, me] = part
            else:
                own_buf[step - 1, t] = part
        if step:
            own_copy(step).start()

    base_cos, base_sin = base_ref[0, pl.ds(me, 1)], base_ref[1, pl.ds(me, 1)]
    lane = lax.broadcasted_iota(jnp.int32, (1, width), 1)
    front = lane % head_size < half
    loads[1].wait()
    cosine = turn[0] * base_cos - turn[1] * base_sin
    sine = turn[1] * base_cos + turn[0] * base_sin
    sine = jnp.where(front, -sine, sine)

    def turned(source, h):
        x = source[:, h * width : (h + 1) * width].astype(f32)
        partner = jnp.where(front, pltpu.roll(x, width - half, 1), pltpu.roll(x, half, 1))
        return (x * cosine + partner * sine).astype(bf16)

    loads[2].wait()
    for h in range(heads):
        rk[h] = turned(k_in, h)
    loads[3].wait()
    for h in range(heads):
        rq[h] = turned(q_in, h) * jnp.asarray(head_size ** -0.5, bf16)
    for copy in values:
        copy.wait()

    def q_rows(dest):
        return pl.ds(pl.multiple_of(((dest % g + me) % g) * sub, sub), sub)

    def q_copy(dest):
        return to_ep(rq.at[dest // g, q_rows(dest)], q_buf.at[me], q_ss.at[dest], q_rs.at[me], dest)

    def k_copy(dest):
        return to_ep(rk.at[dest // g], k_buf.at[me], k_ss.at[dest], k_rs.at[me], dest)

    def v_copy(dest):
        return to_ep(v_in.at[dest // g], v_buf.at[me], v_ss.at[dest], v_rs.at[me], dest)

    def send_kv(p):
        k_copy(p * g + core).start()
        v_copy(p * g + core).start()

    def send_q(p):
        for c in range(g):
            q_copy(p * g + c).start()

    for step in range(1, g):
        q_copy(chip * g + lax.rem(core + step, g)).start()
    send_kv(mate_chip)
    send_q(mate_chip)

    @pl.when(inner == 0)
    def _():
        send_tokens(2, heads)

    @pl.when(side == 0)
    def _():
        for i in (0, 1):
            send_kv(2 + (inner + i) % 2)
            send_q(2 + (inner + i) % 2)

    @pl.when(side == 1)
    def _():
        for s in range(2, heads):
            send_q(nearest(s))
        for i in (1, 0):
            send_kv((inner + i) % 2)

    q_buf[me] = rq[chip, q_rows(me)]
    k_buf[me] = rk[chip]
    v_buf[me] = v_in[chip]

    def gated(gate, up):
        return (gate / (1.0 + jnp.exp(-gate)) * up).astype(bf16)

    for i in (4, 5, 6):
        loads[i].wait()
    hidden = gated(
        jnp.dot(xn[...], sg[...], preferred_element_type=f32), jnp.dot(xn[...], su[...], preferred_element_type=f32))

    sh_copies, sh_pass, sh_total, sh_sent = reduction(
        sh_send, sh_first, sh_held, sh_second, s_ss, s_rs, s2_ss, s2_rs)
    half_tokens = tokens // 2

    def shared_down(dest, h):
        sh_send[dest, h] = jnp.dot(
            hidden[h * half_tokens : (h + 1) * half_tokens], sd[:, columns(dest)],
            preferred_element_type=f32).astype(bf16)

    for i in range(2):
        for h in range(2):
            shared_down((corner, across[h])[i], h)
            sh_copies(h)[i].start()
    for h in range(2):
        shared_down(across[1 - h], h)
        shared_down(my_tp, h)

    lam = lam_ref[chip]
    gain = gain_ref[...]
    vt_rows = vt_buf.shape[1]
    keys = g * rows
    lane_row = lax.broadcasted_iota(jnp.int32, (sub, width), 1)

    def forward(source, step):
        to = chip * g + lax.rem(core + step, g)
        return (
            to_ep(k_buf.at[source], k_buf.at[source], fk_ss.at[source, step], fk_rs.at[source], to),
            to_ep(v_buf.at[source], v_buf.at[source], fv_ss.at[source, step], fv_rs.at[source], to),
        )

    def prepare_kv(e):
        vt_buf[e, :vw] = v_buf[e].astype(f32).T.astype(bf16)
        vt_buf[e, vw:] = jnp.ones((vt_rows - vw, rows), bf16)

    def receive_kv(p):
        direct = p * g + core

        @pl.when(direct != me)
        def _():
            arrived(k_buf.at[direct], k_rs.at[direct])
            arrived(v_buf.at[direct], v_rs.at[direct])

        for step in range(1, g):
            for copy in forward(direct, step):
                copy.start()
        prepare_kv(direct)

    def complete_kv(p):
        for step in range(1, g):
            other = p * g + lax.rem(core + step, g)
            arrived(k_buf.at[other], fk_rs.at[other])
            arrived(v_buf.at[other], fv_rs.at[other])
            prepare_kv(other)

    def receive_q(p):
        for c in range(g):
            e = p * g + c

            @pl.when(e != me)
            def _():
                arrived(q_buf.at[e], q_rs.at[e])

            q = q_buf[e]
            zero = jnp.zeros_like(q)
            st_buf[p, 2 * c * sub : (2 * c + 1) * sub] = jnp.where(lane_row < width // 2, q, zero)
            st_buf[p, (2 * c + 1) * sub : (2 * c + 2) * sub] = jnp.where(lane_row < width // 2, zero, q)
        m_buf[p] = jnp.full((1, keys), masked_low, f32)
        acc[p] = jnp.zeros((vt_rows, keys), f32)

    def tile(p, e, first=0, diagonal=False):
        span = slice(first, keys)
        size = keys - first
        s = lax.dot_general(k_buf[e], st_buf[p, span], (((1,), (1,)), ((), ())), preferred_element_type=f32)
        if diagonal:
            key = lax.broadcasted_iota(jnp.int32, (rows, size), 0) + first
            column = lax.broadcasted_iota(jnp.int32, (rows, size), 1) + first
            block = column // rows
            query = block * rows + column % sub + (core + block) % g * sub
            s = jnp.where(key <= query, s, masked_low)
        old = m_buf[p, :, span]
        m = jnp.maximum(old, jnp.max(s, axis=0, keepdims=True))
        weights = jnp.exp(s - m).astype(bf16)
        m_buf[p, :, span] = m
        acc[p, :, span] = acc[p, :, span] * jnp.exp(old - m) + jnp.dot(
            vt_buf[e], weights, preferred_element_type=f32)

    def hn_copy(dest):
        return to_ep(hn_send.at[dest], hn_buf.at[me], h_ss.at[dest], h_rs.at[me], dest)

    def finish(p):
        a = (acc[p, :vw] / acc[p, vw : vw + 1]).T
        for c in range(g):
            e = p * g + c
            diff = a[2 * c * sub : (2 * c + 1) * sub] - lam * a[(2 * c + 1) * sub : (2 * c + 2) * sub]
            inverse = lax.rsqrt(jnp.mean(diff * diff, axis=-1, keepdims=True) + norm_eps)
            hn_send[e] = (diff * inverse * gain).astype(bf16)

            @pl.when(e != me)
            def _():
                hn_copy(e).start()

    def spread_copy(p, i):
        part = arr.at[my_tp, pl.ds(p * g, g)]
        return to_tp(part, part, x_ss.at[p, i], x_rs.at[my_tp, p], across[i])

    def relay_copy(p, c):
        part = arr.at[across[c], p * g + c]
        return to_tp(part, part, d_ss.at[p, c], d_rs.at[p, c], across[1 - c])

    def spread(s):
        p = nearest(s)
        for c in range(g):
            arrived(arr.at[my_tp, p * g + c], t_rs.at[p * g + c])
        for i in range(2):
            spread_copy(p, i).start()

    def relay(s):
        p = nearest(s)
        for c in range(2):
            arrived(arr.at[across[c], pl.ds(p * g, g)], x_rs.at[across[c], p])
            relay_copy(p, c).start()

    expert_sums = [
        reduction(ex_send, ex_first, ex_held, ex_second, e_ss, e_rs, e2_ss, e2_rs, (part,)) for part in range(2)]
    mix_copies, mix_pass, mix_total, mix_sent = reduction(
        mix_send, mix_first, mix_held, mix_second, m_ss, m_rs, m2_ss, m2_rs)
    def routed(part):
        half = n // 2
        start = half * (side if part == 0 else 1 - side)
        if part == 0:
            for step in range(1, g):
                other = chip * g + lax.rem(core + step, g)
                arrived(arr.at[:, other], o_rs.at[other])
        for s in range(1, 2) if part == 0 else range(2, heads):
            for c in range(2):
                arrived(arr.at[corner, nearest(s) * g + c], d_rs.at[nearest(s), c])
        if part == 0:
            for i in (7, 8, 9):
                loads[i].wait()
        gate = up = None
        for t in range(n_tp):
            block = arr[t, pl.ds(start, half)].reshape(half * cap, piece)
            span = slice(t * piece, (t + 1) * piece)
            gate_part = jnp.dot(block, wg[span, :], preferred_element_type=f32)
            up_part = jnp.dot(block, wu[span, :], preferred_element_type=f32)
            gate = gate_part if gate is None else gate + gate_part
            up = up_part if up is None else up + up_part
        hidden = gated(gate, up)
        quarter = half // 2 * cap

        def down(dest, h):
            ex_send[part, dest, h] = jnp.dot(
                hidden[h * quarter : (h + 1) * quarter], wd[:, columns(dest)], preferred_element_type=f32).astype(bf16)

        copies = expert_sums[part][0]
        for i in range(2):
            for h in range(2):
                down((corner, across[h])[i], h)
                copies(h)[i].start()
        for h in range(2):
            down(across[1 - h], h)
            down(my_tp, h)

    low, pair = 1 - side, 2 * side

    def phase(s, _):
        early = (4 - s) // 3
        second = (s // 2) * (1 - s // 3)
        third = (s // 3) * (1 - s // 4)
        fourth = s // 4
        newest = early * (chip + s * (mate_chip - chip)) + (1 - early) * (
            low * (third * 3 + fourth * 2) + side * (second * (1 - inner) + third * inner))
        with_q = early + side * (second + third)
        with_kv = with_q + low * (third + fourth)

        @pl.when(low * second == 1)
        def _():
            for p in (2, 3):
                receive_q(p)

        @pl.when(with_kv == 1)
        def _():
            receive_kv(newest)

        @pl.when(with_q == 1)
        def _():
            receive_q(newest)

        def diagonal(step, _):
            c = (core + step) % g

            @pl.when(step == 1)
            def _():
                complete_kv(newest)

            for first in range(g):
                @pl.when(c == first)
                def _():
                    tile(newest, newest * g + first, first * rows, True)

            return 0

        @pl.when(with_kv == 1)
        def _():
            lax.fori_loop(0, g, diagonal, 0)

        @pl.when(side * (second * inner + third * (1 - inner)) == 1)
        def _():
            finish(newest)

        def full(i, _):
            p = early * (pair + 1) + second * (2 + low * (i // 2) + side * i) + low * fourth * 3 + side * third * (1 + i)
            j = early * pair + second * (low * (i % 2) + side * newest) + low * fourth * 2 + side * third * newest * ((i + 1) // 2)
            for c in range(g):
                tile(p, j * g + c)

            @pl.when(third * side + low * fourth == 1)
            def _():
                finish(p)

            return 0

        lax.fori_loop(0, early * s + second * (4 * low + 2 * side) + low * fourth + side * third * 3, full, 0)

        def done(p, _):
            finish(p)
            return 0

        @pl.when((early * s + fourth) * low == 1)
        def _():
            lax.fori_loop(early * pair + fourth * 2, early * (pair + 2) + fourth * 3, done, 0)

        @pl.when(s == 0)
        def _():
            spread(1)
            relay(1)

        @pl.when(s == inner)
        def _():
            for step in range(2, heads):
                spread(step)

        @pl.when(s == 1)
        def _():
            for step in range(2, heads):
                relay(step)
            routed(0)
            routed(1)
            for h in range(2):
                expert_sums[0][1](h)
                sh_pass(h)

        @pl.when(s == 2)
        def _():
            for h in range(2):
                expert_sums[1][1](h)

        return 0

    lax.fori_loop(0, heads + 1, phase, 0)

    def y_copy(dest):
        return to_ep(y_buf.at[dest], ret.at[me], y_ss.at[dest], y_rs.at[me], dest)

    def send_back():
        for part in (1, 0):
            for h in range(2):
                p = (side if part == 0 else 1 - side) * 2 + h
                y_buf[pl.ds(p * g, g)] = expert_sums[part][2](h).astype(bf16).reshape(g, cap, piece)
        for s in range(heads - 1, 0, -1):
            for c in range(g):
                y_copy(nearest(s) * g + c).start()
        for step in range(1, g):
            y_copy(chip * g + lax.rem(core + step, g)).start()
        ret[me] = y_buf[me]

    @pl.when(side == 1)
    def _():
        send_back()

    hn_buf[me] = hn_send[me]
    for step in range(1, n):
        source = lax.rem(me + step, n)
        arrived(hn_buf.at[source], h_rs.at[source])
    loads[10].wait()
    normed = [
        jnp.concatenate([hn_buf[h * g + (part + n - me) % g] for h in range(heads)], axis=1) for part in range(g)]

    def project(dest, h):
        mix_send[dest, h] = jnp.dot(normed[h], w_buf[:, columns(dest)], preferred_element_type=f32).astype(bf16)

    for i in range(2):
        for h in range(2):
            project((corner, across[h])[i], h)
            mix_copies(h)[i].start()
    for h in range(2):
        project(across[1 - h], h)
        project(my_tp, h)
    for h in range(2):
        mix_pass(h)

    @pl.when(side == 0)
    def _():
        send_back()

    out = jnp.concatenate([sh_total(h) for h in range(2)], axis=0)
    rw_pad[...] = jnp.zeros_like(rw_pad)
    rw_pad[:top_k, :tokens] = rw_ref[...]
    scale = rw_pad[...].T
    for step in range(1, n):
        source = lax.rem(me + step, n)
        arrived(ret.at[source], y_rs.at[source])
    returned = ret[...].reshape(n * cap, piece)
    for k in range(top_k):
        out = out + scale[:tokens, k : k + 1] * lax.dot_general(
            place[k].reshape(n * cap, tokens), returned, (((0,), (0,)), ((), ())), preferred_element_type=f32)
    moe_ref[...] = out.astype(bf16)
    for h in range(2):
        attn_ref[h * sub : (h + 1) * sub] = mix_total(h).astype(bf16)
    for s in range(1, heads):
        p = nearest(s)
        k_copy(p * g + core).wait_send()
        v_copy(p * g + core).wait_send()
        for c in range(g):
            tok_copy(p * g + c).wait_send()
        for i in range(2):
            spread_copy(p, i).wait_send()
            relay_copy(p, i).wait_send()
    for step in range(1, n):
        dest = lax.rem(me + step, n)
        q_copy(dest).wait_send()
        hn_copy(dest).wait_send()
        y_copy(dest).wait_send()
    for step in range(1, g):
        own_copy(step).wait_send()
    for p in range(heads):
        for step in range(1, g):
            for copy in forward(p * g + core, step):
                copy.wait_send()
    sh_sent()
    for part in range(2):
        expert_sums[part][3]()
    mix_sent()


def turn_tables(rows, n, head_size):
    half = head_size // 2
    frequency = theta_base ** (-(np.arange(half) * 2.0) / head_size)

    def waves(positions):
        angles = np.tile(positions[:, None] * frequency[None, :], (1, 4))
        return np.stack([np.cos(angles), np.sin(angles)]).astype(np.float32)

    return waves(np.arange(rows)), waves(np.arange(n) * rows)


def exchange_all(
    query_pairs, key_pairs, value_rows, head_lambda, head_gain, out_weight, moe_input, ffn_gain, routes, route_weight,
    gate_weight, up_weight, down_weight, shared_gate, shared_up, shared_down,
):
    n, n_tp = lax.axis_size("ep"), lax.axis_size("tp")
    tokens, model = moe_input.shape
    piece = model // n_tp
    rows = query_pairs.shape[0]
    heads = head_lambda.shape[0]
    width = query_pairs.shape[1] // heads
    head_size = width // 2
    vw = value_rows.shape[1] // heads
    g = n // heads
    sub = rows // g
    keys = g * rows
    cap = -(-(tokens * TOP_K * 5 // (4 * n)) // 8) * 8
    hidden, shared = gate_weight.shape[2], shared_gate.shape[1]
    turns, bases = turn_tables(rows, n, head_size)
    any_spec = pl.BlockSpec(memory_space=pl.ANY)
    vmem = pl.BlockSpec(memory_space=pltpu.VMEM)
    dma = pltpu.SemaphoreType.DMA
    buffers = [
        (rows, heads * width), (rows, heads * width), (heads, rows, vw), ((2, rows, width), f32),
        (tokens, model), (tokens, model), (TOP_K, n, cap, tokens), (heads, rows, width), (heads, rows, width),
        (n, sub, width), (n, rows, width), (n, rows, vw), (n, vw + 8, rows), (heads, 2 * rows, width),
        ((heads, vw + 8, keys), f32), ((heads, 1, keys), f32), (n, sub, vw), (n, sub, vw), out_weight.shape,
        (n, cap, piece), (g - 1, n_tp, cap, piece), (n_tp, n, cap, piece),
        (model, hidden), (model, hidden), (hidden, model), (model, shared), (model, shared), (shared, model),
        (n_tp, 2, tokens // 2, piece), (2, 2, tokens // 2, piece), (2, tokens // 2, piece), (2, tokens // 2, piece),
        (2, n_tp, 2, g * cap, piece), (2, 2, 2, g * cap, piece), (2, 2, g * cap, piece), (2, 2, g * cap, piece),
        (n_tp, 2, sub, piece), (2, 2, sub, piece), (2, sub, piece), (2, sub, piece), (n, cap, piece), (n, cap, piece),
        ((8, -(-tokens // 128) * 128), f32),
    ]
    semaphores = [
        (11,), (heads,), (n,), (n,), (n,), (n,), (n,), (n,), (n, g), (n,), (n, g), (n,), (n,), (n,),
        (n,), (n,), (g - 1,), (n,), (heads, 2), (n_tp, heads), (heads, 2), (heads, 2),
        (2, 2), (2, 2), (2,), (2,), (2, 2), (2, 2), (2,), (2,), (2, 2, 2), (2, 2, 2), (2, 2), (2, 2), (n,), (n,),
    ]
    results = pl.pallas_call(
        functools.partial(mega_kernel, n, heads, n_tp, head_size),
        out_shape=(
            jax.ShapeDtypeStruct((rows, piece), bf16),
            jax.ShapeDtypeStruct((tokens, piece), bf16),
        ),
        in_specs=[pl.BlockSpec(memory_space=pltpu.SMEM)] + [vmem] * 4 + [any_spec, vmem] + [any_spec] * 11,
        out_specs=(vmem, vmem),
        scratch_shapes=[
            pltpu.VMEM(shape[0], shape[1]) if isinstance(shape[0], tuple) else pltpu.VMEM(shape, bf16)
            for shape in buffers
        ] + [dma(shape) for shape in semaphores],
        compiler_params=pltpu.CompilerParams(
            collective_id=0, has_side_effects=True, vmem_limit_bytes=60 * 2**20),
        cost_estimate=pl.CostEstimate(flops=30 * 10**9, bytes_accessed=24 * 2**20, transcendentals=6 * 10**6),
        name="exchange",
    )(
        head_lambda, head_gain.reshape(1, vw), routes.T, route_weight.T, ffn_gain.reshape(1, model),
        jnp.asarray(turns), jnp.asarray(bases), query_pairs, key_pairs, value_rows, moe_input, out_weight,
        gate_weight, up_weight, down_weight, shared_gate, shared_up, shared_down)
    return pl.pallas_call(
        store_kernel,
        out_shape=tuple(jax.ShapeDtypeStruct(r.shape, r.dtype) for r in results),
        in_specs=[any_spec] * 2,
        out_specs=(any_spec, any_spec),
        scratch_shapes=[pltpu.VMEM(r.shape, r.dtype) for r in results] + [dma((2,)), dma((2,))],
        name="store",
    )(*results)


def store_kernel(attn_ref, moe_ref, attn_out, moe_out, attn_buf, moe_buf, in_sems, out_sems):
    refs = ((attn_ref, attn_buf, attn_out), (moe_ref, moe_buf, moe_out))
    ins = [pltpu.make_async_copy(source, buf, in_sems.at[i]) for i, (source, buf, _) in enumerate(refs)]
    outs = [pltpu.make_async_copy(buf, target, out_sems.at[i]) for i, (_, buf, target) in enumerate(refs)]
    for copy in ins:
        copy.start()
    for i in (1, 0):
        ins[i].wait()
        outs[i].start()
    for copy in outs:
        copy.wait()


def local(
    query_pairs,
    key_pairs,
    value_rows,
    head_lambda,
    head_gain,
    out_weight,
    moe_input,
    ffn_gain,
    routes,
    route_weight,
    gate_weight,
    up_weight,
    down_weight,
    shared_gate,
    shared_up,
    shared_down,
):
    n = lax.axis_size("ep")
    heads = head_lambda.shape[0]
    rows = query_pairs.shape[0]
    fits = n == 2 * heads and heads == 4 and lax.axis_size("tp") == 4 and (rows * heads) % (n * 64) == 0 and routes.shape[0] % 32 == 0
    if fits:
        return exchange_all(
            query_pairs, key_pairs, value_rows, head_lambda, head_gain, out_weight, moe_input, ffn_gain, routes,
            route_weight, gate_weight, up_weight, down_weight, shared_gate, shared_up, shared_down,
        )
    row_values = moe_input.astype(jnp.float32)
    inverse_norm = lax.rsqrt(jnp.mean(row_values * row_values, axis=-1, keepdims=True) + norm_eps)
    normed = (row_values * inverse_norm * ffn_gain).astype(jnp.bfloat16)
    attn_out = generic_attention(query_pairs, key_pairs, value_rows, head_lambda, head_gain, out_weight)
    token_rows = normed.shape[0]
    experts = lax.axis_size("ep")
    capacity = token_rows * TOP_K * 5 // (4 * experts)
    flat_routes = routes.reshape(-1)
    onehot = (flat_routes[:, None] == jnp.arange(experts, dtype=jnp.int32)).astype(jnp.int32)
    slot_rank = jnp.sum((jnp.cumsum(onehot, axis=0) - 1) * onehot, axis=-1)
    slot_index = flat_routes * capacity + slot_rank
    token_index = jnp.arange(token_rows * TOP_K, dtype=jnp.int32) // TOP_K
    slot_rows = (
        jnp.full((experts * capacity,), token_rows, jnp.int32).at[slot_index].set(token_index)
    )
    padded = jnp.concatenate([normed, jnp.zeros((1, normed.shape[1]), jnp.bfloat16)], axis=0)
    outgoing = padded[slot_rows]
    arrived = lax.all_to_all(outgoing, "ep", split_axis=0, concat_axis=0, tiled=True)
    gate_part = jnp.dot(arrived, gate_weight[0], preferred_element_type=jnp.float32)
    up_part = jnp.dot(arrived, up_weight[0], preferred_element_type=jnp.float32)
    hidden = (jax.nn.silu(gate_part) * up_part).astype(jnp.bfloat16)
    expert_terms = jnp.dot(hidden, down_weight[0], preferred_element_type=jnp.float32)
    shared_gated = jnp.dot(normed, shared_gate, preferred_element_type=jnp.float32)
    shared_lifted = jnp.dot(normed, shared_up, preferred_element_type=jnp.float32)
    shared_hidden = (jax.nn.silu(shared_gated) * shared_lifted).astype(jnp.bfloat16)
    shared_terms = jnp.dot(shared_hidden, shared_down, preferred_element_type=jnp.float32)
    expert_sum, shared_sum = (
        lax.psum_scatter(
            expert_terms.astype(jnp.bfloat16), "tp", scatter_dimension=1, tiled=True
        ).astype(jnp.float32),
        lax.psum_scatter(
            shared_terms.astype(jnp.bfloat16), "tp", scatter_dimension=1, tiled=True
        ).astype(jnp.float32),
    )
    returned = lax.all_to_all(
        expert_sum.astype(jnp.bfloat16), "ep", split_axis=0, concat_axis=0, tiled=True
    )
    picked = returned[slot_index.reshape(token_rows, TOP_K)]
    moe_out = (
        jnp.sum(route_weight[..., None] * picked.astype(jnp.float32), axis=1) + shared_sum
    ).astype(jnp.bfloat16)
    return (attn_out, moe_out)


def solution(mesh):
    return jax.shard_map(
        local,
        mesh=mesh,
        in_specs=(
            P("ep", "tp"),
            P("ep", "tp"),
            P("ep", "tp"),
            P("tp"),
            P(),
            P("tp", None),
            P("ep", None),
            P(),
            P("ep", None),
            P("ep", None),
            P("ep", None, "tp"),
            P("ep", None, "tp"),
            P("ep", "tp", None),
            P(None, "tp"),
            P(None, "tp"),
            P("tp", None),
        ),
        out_specs=(P("ep", "tp"), P("ep", "tp")),
        check_vma=False,
    )
```

```python
import functools

import jax
import jax.numpy as jnp
import numpy as np
from jax import lax
from jax.experimental import pallas as pl
from jax.experimental.pallas import tpu as pltpu
from jax.sharding import PartitionSpec as P

TOP_K = 2
KEY_BLOCK = 128


theta_base = 500000.0
norm_eps = 1e-06
masked_low = -1e30


def rotate(inputs, positions):
    half_size = inputs.shape[-1] // 2
    frequency = theta_base ** (-(jnp.arange(half_size, dtype=jnp.float32) * 2.0) / inputs.shape[-1])
    angles = positions.astype(jnp.float32)[:, None] * frequency[None, :]
    cosine = jnp.cos(angles)[:, None, None, :]
    sine_part = jnp.sin(angles)[:, None, None, :]
    front_half = inputs[..., :half_size]
    back_half = inputs[..., half_size:]
    return jnp.concatenate(
        [front_half * cosine - back_half * sine_part, back_half * cosine + front_half * sine_part],
        axis=-1,
    )


def generic_attention(query_pairs, key_pairs, value_rows, head_lambda, head_gain, out_weight):
    local_rows = query_pairs.shape[0]
    local_heads = head_lambda.shape[0]
    head_size = query_pairs.shape[1] // (2 * local_heads)
    value_size = value_rows.shape[1] // local_heads
    positions = lax.axis_index("ep") * local_rows + jnp.arange(local_rows, dtype=jnp.int32)
    rot_queries = rotate(
        query_pairs.astype(jnp.float32).reshape(local_rows, local_heads, 2, head_size), positions
    ).astype(jnp.bfloat16)
    rot_keys = rotate(
        key_pairs.astype(jnp.float32).reshape(local_rows, local_heads, 2, head_size), positions
    ).astype(jnp.bfloat16)
    rot_keys = rot_keys.reshape(local_rows, local_heads * 2 * head_size)
    zero_init = (
        jnp.full((local_heads, 2, local_rows), masked_low, jnp.float32),
        jnp.zeros((local_heads, 2, local_rows), jnp.float32),
        jnp.zeros((local_heads, 2, local_rows, value_size), jnp.float32),
    )
    piece_keys = lax.all_gather(rot_keys, "ep", axis=0, tiled=True)
    piece_values = lax.all_gather(value_rows, "ep", axis=0, tiled=True)
    block_count = piece_keys.shape[0] // KEY_BLOCK
    group_size = 4
    group_count = block_count // group_size
    grouped_keys = piece_keys.reshape(group_count, group_size, KEY_BLOCK, local_heads, 2, head_size)
    grouped_values = piece_values.reshape(
        group_count, group_size, KEY_BLOCK, local_heads, value_size
    )

    def one_group(current, inputs):
        block_keys, block_values, group_index = inputs
        key_positions = group_index * group_size * KEY_BLOCK + jnp.arange(
            group_size * KEY_BLOCK, dtype=jnp.int32
        ).reshape(group_size, KEY_BLOCK)
        scores = jnp.einsum(
            "qhmd,gkhmd->hmqgk", rot_queries, block_keys, preferred_element_type=jnp.float32
        ) * head_size ** (-0.5)
        allowed = key_positions[None, :, :] <= positions[:, None, None]
        scores = jnp.where(allowed, scores, masked_low)
        block_max = jnp.max(scores, axis=-1)
        weights = jnp.where(allowed, jnp.exp(scores - block_max[..., None]), 0.0)
        block_sum = jnp.sum(weights, axis=-1)
        block_out = jnp.einsum(
            "hmqgk,gkhc->hmqgc",
            weights.astype(jnp.bfloat16),
            block_values,
            preferred_element_type=jnp.float32,
        )
        run_max, run_sum, run_out = current
        new_max = jnp.maximum(run_max, jnp.max(block_max, axis=-1))
        old_scale = jnp.exp(run_max - new_max)
        new_scale = jnp.exp(block_max - new_max[..., None])
        run_sum = run_sum * old_scale + jnp.sum(new_scale * block_sum, axis=-1)
        run_out = run_out * old_scale[..., None] + jnp.sum(
            new_scale[..., None] * block_out, axis=-2
        )
        return ((new_max, run_sum, run_out), None)

    result, _ = lax.scan(
        one_group,
        zero_init,
        (grouped_keys, grouped_values, jnp.arange(group_count, dtype=jnp.int32)),
    )
    run_max, run_sum, run_out = result
    map_outputs = run_out / run_sum[..., None]
    difference = map_outputs[:, 0] - head_lambda[:, None, None] * map_outputs[:, 1]
    inverse_rms = lax.rsqrt(jnp.mean(difference * difference, axis=-1, keepdims=True) + norm_eps)
    normed_heads = (difference * inverse_rms * head_gain).astype(jnp.bfloat16)
    head_rows = normed_heads.transpose(1, 0, 2).reshape(local_rows, local_heads * value_size)
    mixer_terms = jnp.dot(head_rows, out_weight, preferred_element_type=jnp.float32)
    attn_out = lax.psum_scatter(
        mixer_terms.astype(jnp.bfloat16), "tp", scatter_dimension=1, tiled=True
    )
    return attn_out


MESH = pl.DeviceIdType.MESH
f32, bf16 = jnp.float32, jnp.bfloat16


def mega_kernel(
    n, heads, n_tp, head_size, lam_hbm, gain_hbm, routes_hbm, rw_hbm, ffn_hbm, turn_ref, base_hbm,
    q_ref, k_ref, v_ref, x_ref, w_ref, wg_ref, wu_ref, wd_ref, sg_ref, su_ref, sd_ref,
    attn_hbm, moe_hbm,
    lam_ref, gain_ref, routes_ref, rw_ref, ffn_ref, base_ref, attn_ref, moe_ref, small, out_sem,
    q_in, k_in, v_in, turn, x_in, xn, place, rq, rk, q_buf, k_buf, v_buf, vt_buf, st_buf, acc, m_buf,
    hn_send, hn_buf, w_buf, out_buf, own_buf, arr, wg, wu, wd, sg, su, sd,
    sh_send, sh_first, sh_held, sh_second, ex_send, ex_first, ex_held, ex_second, mix_send, mix_first, mix_held, mix_second, y_buf, ret, rw_pad,
    load, load_v, q_ss, q_rs, k_ss, k_rs, v_ss, v_rs, fk_ss, fk_rs, fv_ss, fv_rs, h_ss, h_rs,
    t_ss, t_rs, o_ss, o_rs, x_ss, x_rs, d_ss, d_rs, m_ss, m_rs, m2_ss, m2_rs, s_ss, s_rs, s2_ss, s2_rs, e_ss, e_rs, e2_ss, e2_rs, y_ss, y_rs,
):
    me, my_tp = lax.axis_index("ep"), lax.axis_index("tp")
    g = n // heads
    chip, core = me // g, me % g
    rows, width = k_buf.shape[1:]
    vw = v_buf.shape[2]
    sub = rows // g
    cap, piece = out_buf.shape[1:]
    tokens = xn.shape[0]
    top_k = rw_ref.shape[0]
    half = head_size // 2
    side = chip // (heads // 2)

    def mirrored(p):
        return p + side * (heads - 1 - 2 * p)

    near = mirrored(chip)

    def nearest(s):
        return mirrored(jnp.where(s <= near, near - s, s))

    barrier = pltpu.get_barrier_semaphore()
    for step in range(1, n):
        pl.semaphore_signal(barrier, inc=1, device_id={"ep": lax.rem(me + step, n)}, device_id_type=MESH)
    for step in range(1, n_tp):
        pl.semaphore_signal(barrier, inc=1, device_id={"tp": lax.rem(my_tp + step, n_tp)}, device_id_type=MESH)
    loads = [
        pltpu.make_async_copy(source, target, load.at[i])
        for i, (source, target) in enumerate((
            (x_ref, x_in), (turn_ref, turn), (k_ref, k_in), (q_ref, q_in),
            (sg_ref, sg), (su_ref, su), (sd_ref, sd),
            (wg_ref.at[0], wg), (wu_ref.at[0], wu), (wd_ref.at[0], wd), (w_ref, w_buf)))
    ]
    values = [
        pltpu.make_async_copy(v_ref.at[:, h * vw : (h + 1) * vw], v_in.at[h], load_v.at[h]) for h in range(heads)
    ]
    smalls = [
        pltpu.make_async_copy(source, target, small.at[i])
        for i, (source, target) in enumerate((
            (routes_hbm, routes_ref), (ffn_hbm, ffn_ref), (base_hbm, base_ref),
            (lam_hbm, lam_ref), (gain_hbm, gain_ref), (rw_hbm, rw_ref)))]
    for copy in (smalls[0], loads[0], *smalls[1:3], *loads[1:4], *values, *smalls[3:]):
        copy.start()

    def to_ep(source, target, send_sem, recv_sem, dest):
        return pltpu.make_async_remote_copy(
            source, target, send_sem, recv_sem, device_id={"ep": dest}, device_id_type=MESH)

    def to_tp(source, target, send_sem, recv_sem, dest):
        return pltpu.make_async_remote_copy(
            source, target, send_sem, recv_sem, device_id={"tp": dest}, device_id_type=MESH)

    def arrived(ref, sem):
        to_ep(ref, ref, sem, sem, lax.rem(me + 1, n)).wait_recv()

    across = (my_tp + 1 - 2 * (my_tp % 2), (my_tp + 2) % n_tp)
    corner = (across[0] + 2) % n_tp

    def reduction(send, first_in, held, second_in, ss, rs, ss2, rs2, pre=()):
        at = lambda ref, *index: ref.at[(*pre, *index)]

        def first_copies(h):
            return [
                to_tp(at(send, dest, h), at(first_in, h, i), at(ss, h, i), at(rs, h, i), across[h])
                for i, dest in enumerate((corner, across[h]))]

        def second_copy(h):
            return to_tp(at(held, h), at(second_in, h), at(ss2, h), at(rs2, h), across[1 - h])

        def pass_on(h):
            arrived(at(first_in, h, 0), at(rs, h, 0))
            own = send[(*pre, across[1 - h], h)].astype(f32)
            held[(*pre, h)] = (own + first_in[(*pre, h, 0)].astype(f32)).astype(bf16)
            second_copy(h).start()

        def total(h):
            arrived(at(first_in, h, 1), at(rs, h, 1))
            arrived(at(second_in, h), at(rs2, h))
            own = send[(*pre, my_tp, h)].astype(f32)
            return own + first_in[(*pre, h, 1)].astype(f32) + second_in[(*pre, h)].astype(f32)

        def sent():
            for h in range(2):
                for copy in (*first_copies(h), second_copy(h)):
                    copy.wait_send()

        return first_copies, pass_on, total, sent

    def columns(t):
        return pl.ds(pl.multiple_of(t * piece, piece), piece)

    smalls[0].wait()
    expert = lax.broadcasted_iota(jnp.int32, (n, tokens), 0)
    chosen = [(routes_ref[k : k + 1, :] == expert).astype(f32) for k in range(top_k)]
    earlier = lax.broadcasted_iota(jnp.int32, (tokens, tokens), 0) <= lax.broadcasted_iota(jnp.int32, (tokens, tokens), 1)
    ranks = jnp.dot(sum(chosen).astype(bf16), earlier.astype(bf16), preferred_element_type=f32) - 1.0
    slot = ranks + (expert * cap).astype(f32)
    slots = [jnp.sum(c * slot, axis=0, keepdims=True) for c in chosen]
    slot_row = lax.broadcasted_iota(jnp.int32, (n * cap, tokens), 0).astype(f32)
    marks = [(slot_row == s).astype(f32) for s in slots]
    for k in range(top_k):
        place[k] = marks[k].astype(bf16).reshape(n, cap, tokens)
    loads[0].wait()
    smalls[1].wait()
    x = x_in[...].astype(f32)
    inverse = lax.rsqrt(jnp.mean(x * x, axis=-1, keepdims=True) + norm_eps)
    xn[...] = (x * inverse * ffn_ref[...]).astype(bf16)
    out_buf[...] = jnp.dot(
        sum(marks).astype(bf16), xn[:, columns(my_tp)], preferred_element_type=f32).astype(bf16).reshape(n, cap, piece)

    def own_rows(dest):
        mark = place[0, dest]
        for k in range(1, top_k):
            mark = mark + place[k, dest]
        return jnp.dot(mark, xn[...], preferred_element_type=f32).astype(bf16)

    pl.semaphore_wait(barrier, n - 1 + n_tp - 1)
    for copy in loads[4:]:
        copy.start()

    def tok_copy(dest):
        return to_ep(out_buf.at[dest], arr.at[my_tp, me], t_ss.at[dest], t_rs.at[me], dest)

    def own_copy(step):
        dest = chip * g + lax.rem(core + step, g)
        return to_ep(own_buf.at[step - 1], arr.at[:, me], o_ss.at[step - 1], o_rs.at[me], dest)

    mate_chip = chip + 1 - 2 * (chip % 2)
    inner = (chip + side) % 2

    def send_tokens(first, last):
        for s in range(first, last):
            for c in range(g):
                tok_copy(nearest(s) * g + c).start()

    send_tokens(1, 2)

    @pl.when(inner == 1)
    def _():
        send_tokens(2, heads)

    for step in range(g):
        full = own_rows(chip * g + lax.rem(core + step, g))
        for t in range(n_tp):
            part = full[:, t * piece : (t + 1) * piece]
            if step == 0:
                arr[t, me] = part
            else:
                own_buf[step - 1, t] = part
        if step:
            own_copy(step).start()

    smalls[2].wait()
    base_cos, base_sin = base_ref[0, pl.ds(me, 1)], base_ref[1, pl.ds(me, 1)]
    lane = lax.broadcasted_iota(jnp.int32, (1, width), 1)
    front = lane % head_size < half
    loads[1].wait()
    cosine = turn[0] * base_cos - turn[1] * base_sin
    sine = turn[1] * base_cos + turn[0] * base_sin
    sine = jnp.where(front, -sine, sine)

    def turned(source, h):
        x = source[:, h * width : (h + 1) * width].astype(f32)
        partner = jnp.where(front, pltpu.roll(x, width - half, 1), pltpu.roll(x, half, 1))
        return (x * cosine + partner * sine).astype(bf16)

    loads[2].wait()
    for h in range(heads):
        rk[h] = turned(k_in, h)
    loads[3].wait()
    for h in range(heads):
        rq[h] = turned(q_in, h) * jnp.asarray(head_size ** -0.5, bf16)
    for copy in values:
        copy.wait()

    def q_rows(dest):
        return pl.ds(pl.multiple_of(((dest % g + me) % g) * sub, sub), sub)

    def q_copy(dest):
        return to_ep(rq.at[dest // g, q_rows(dest)], q_buf.at[me], q_ss.at[dest], q_rs.at[me], dest)

    def k_copy(dest):
        return to_ep(rk.at[dest // g], k_buf.at[me], k_ss.at[dest], k_rs.at[me], dest)

    def v_copy(dest):
        return to_ep(v_in.at[dest // g], v_buf.at[me], v_ss.at[dest], v_rs.at[me], dest)

    def send_kv(p):
        k_copy(p * g + core).start()
        v_copy(p * g + core).start()

    def send_q(p):
        for c in range(g):
            q_copy(p * g + c).start()

    for step in range(1, g):
        q_copy(chip * g + lax.rem(core + step, g)).start()
    send_kv(mate_chip)
    send_q(mate_chip)

    @pl.when(inner == 0)
    def _():
        send_tokens(2, heads)

    @pl.when(side == 0)
    def _():
        for i in (0, 1):
            send_kv(2 + (inner + i) % 2)
            send_q(2 + (inner + i) % 2)

    @pl.when(side == 1)
    def _():
        for s in range(2, heads):
            send_q(nearest(s))
        for i in (1, 0):
            send_kv((inner + i) % 2)

    q_buf[me] = rq[chip, q_rows(me)]
    k_buf[me] = rk[chip]
    v_buf[me] = v_in[chip]

    def gated(gate, up):
        return (gate / (1.0 + jnp.exp(-gate)) * up).astype(bf16)

    for i in (4, 5, 6):
        loads[i].wait()
    hidden = gated(
        jnp.dot(xn[...], sg[...], preferred_element_type=f32), jnp.dot(xn[...], su[...], preferred_element_type=f32))

    sh_copies, sh_pass, sh_total, sh_sent = reduction(
        sh_send, sh_first, sh_held, sh_second, s_ss, s_rs, s2_ss, s2_rs)
    half_tokens = tokens // 2

    def shared_down(dest, h):
        sh_send[dest, h] = jnp.dot(
            hidden[h * half_tokens : (h + 1) * half_tokens], sd[:, columns(dest)],
            preferred_element_type=f32).astype(bf16)

    for i in range(2):
        for h in range(2):
            shared_down((corner, across[h])[i], h)
            sh_copies(h)[i].start()
    for h in range(2):
        shared_down(across[1 - h], h)
        shared_down(my_tp, h)

    for copy in smalls[3:]:
        copy.wait()
    lam = lam_ref[chip]
    gain = gain_ref[...]
    vt_rows = vt_buf.shape[1]
    keys = g * rows
    lane_row = lax.broadcasted_iota(jnp.int32, (sub, width), 1)

    def forward(source, step):
        to = chip * g + lax.rem(core + step, g)
        return (
            to_ep(k_buf.at[source], k_buf.at[source], fk_ss.at[source, step], fk_rs.at[source], to),
            to_ep(v_buf.at[source], v_buf.at[source], fv_ss.at[source, step], fv_rs.at[source], to),
        )

    def prepare_kv(e):
        vt_buf[e, :vw] = v_buf[e].astype(f32).T.astype(bf16)
        vt_buf[e, vw:] = jnp.ones((vt_rows - vw, rows), bf16)

    def receive_kv(p):
        direct = p * g + core

        @pl.when(direct != me)
        def _():
            arrived(k_buf.at[direct], k_rs.at[direct])
            arrived(v_buf.at[direct], v_rs.at[direct])

        for step in range(1, g):
            for copy in forward(direct, step):
                copy.start()
        prepare_kv(direct)

    def complete_kv(p):
        for step in range(1, g):
            other = p * g + lax.rem(core + step, g)
            arrived(k_buf.at[other], fk_rs.at[other])
            arrived(v_buf.at[other], fv_rs.at[other])
            prepare_kv(other)

    def receive_q(p):
        for c in range(g):
            e = p * g + c

            @pl.when(e != me)
            def _():
                arrived(q_buf.at[e], q_rs.at[e])

            q = q_buf[e]
            zero = jnp.zeros_like(q)
            st_buf[p, 2 * c * sub : (2 * c + 1) * sub] = jnp.where(lane_row < width // 2, q, zero)
            st_buf[p, (2 * c + 1) * sub : (2 * c + 2) * sub] = jnp.where(lane_row < width // 2, zero, q)
        m_buf[p] = jnp.full((1, keys), masked_low, f32)
        acc[p] = jnp.zeros((vt_rows, keys), f32)

    def tile(p, e, first=0, diagonal=False):
        span = slice(first, keys)
        size = keys - first
        s = lax.dot_general(k_buf[e], st_buf[p, span], (((1,), (1,)), ((), ())), preferred_element_type=f32)
        if diagonal:
            key = lax.broadcasted_iota(jnp.int32, (rows, size), 0) + first
            column = lax.broadcasted_iota(jnp.int32, (rows, size), 1) + first
            block = column // rows
            query = block * rows + column % sub + (core + block) % g * sub
            s = jnp.where(key <= query, s, masked_low)
        old = m_buf[p, :, span]
        m = jnp.maximum(old, jnp.max(s, axis=0, keepdims=True))
        weights = jnp.exp(s - m).astype(bf16)
        m_buf[p, :, span] = m
        acc[p, :, span] = acc[p, :, span] * jnp.exp(old - m) + jnp.dot(
            vt_buf[e], weights, preferred_element_type=f32)

    def hn_copy(dest):
        return to_ep(hn_send.at[dest], hn_buf.at[me], h_ss.at[dest], h_rs.at[me], dest)

    def finish(p):
        a = (acc[p, :vw] / acc[p, vw : vw + 1]).T
        for c in range(g):
            e = p * g + c
            diff = a[2 * c * sub : (2 * c + 1) * sub] - lam * a[(2 * c + 1) * sub : (2 * c + 2) * sub]
            inverse = lax.rsqrt(jnp.mean(diff * diff, axis=-1, keepdims=True) + norm_eps)
            hn_send[e] = (diff * inverse * gain).astype(bf16)

            @pl.when(e != me)
            def _():
                hn_copy(e).start()

    def spread_copy(p, i):
        part = arr.at[my_tp, pl.ds(p * g, g)]
        return to_tp(part, part, x_ss.at[p, i], x_rs.at[my_tp, p], across[i])

    def relay_copy(p, c):
        part = arr.at[across[c], p * g + c]
        return to_tp(part, part, d_ss.at[p, c], d_rs.at[p, c], across[1 - c])

    def spread(s):
        p = nearest(s)
        for c in range(g):
            arrived(arr.at[my_tp, p * g + c], t_rs.at[p * g + c])
        for i in range(2):
            spread_copy(p, i).start()

    def relay(s):
        p = nearest(s)
        for c in range(2):
            arrived(arr.at[across[c], pl.ds(p * g, g)], x_rs.at[across[c], p])
            relay_copy(p, c).start()

    expert_sums = [
        reduction(ex_send, ex_first, ex_held, ex_second, e_ss, e_rs, e2_ss, e2_rs, (part,)) for part in range(2)]
    mix_copies, mix_pass, mix_total, mix_sent = reduction(
        mix_send, mix_first, mix_held, mix_second, m_ss, m_rs, m2_ss, m2_rs)
    def routed(part):
        half = n // 2
        start = half * (side if part == 0 else 1 - side)
        if part == 0:
            for step in range(1, g):
                other = chip * g + lax.rem(core + step, g)
                arrived(arr.at[:, other], o_rs.at[other])
        for s in range(1, 2) if part == 0 else range(2, heads):
            for c in range(2):
                arrived(arr.at[corner, nearest(s) * g + c], d_rs.at[nearest(s), c])
        if part == 0:
            for i in (7, 8, 9):
                loads[i].wait()
        gate = up = None
        for t in range(n_tp):
            block = arr[t, pl.ds(start, half)].reshape(half * cap, piece)
            span = slice(t * piece, (t + 1) * piece)
            gate_part = jnp.dot(block, wg[span, :], preferred_element_type=f32)
            up_part = jnp.dot(block, wu[span, :], preferred_element_type=f32)
            gate = gate_part if gate is None else gate + gate_part
            up = up_part if up is None else up + up_part
        hidden = gated(gate, up)
        quarter = half // 2 * cap

        def down(dest, h):
            ex_send[part, dest, h] = jnp.dot(
                hidden[h * quarter : (h + 1) * quarter], wd[:, columns(dest)], preferred_element_type=f32).astype(bf16)

        copies = expert_sums[part][0]
        for i in range(2):
            for h in range(2):
                down((corner, across[h])[i], h)
                copies(h)[i].start()
        for h in range(2):
            down(across[1 - h], h)
            down(my_tp, h)

    low, pair = 1 - side, 2 * side

    def phase(s, _):
        early = (5 - s) // 4
        second = (s // 2) * (1 - s // 3)
        third = (s // 3) * (1 - s // 4)
        fourth = (s // 4) * (1 - s // 5)
        fifth = s // 5
        newest = early * (chip + s * (mate_chip - chip)) + (1 - early) * (
            low * (third * 3 + (fourth + fifth) * 2) + side * (second * (1 - inner) + third * inner))
        with_q = early + side * (second + third)
        with_kv = with_q + low * (third + fifth)

        @pl.when(low * second == 1)
        def _():
            for p in (2, 3):
                receive_q(p)

        @pl.when(with_kv - low * fifth == 1)
        def _():
            receive_kv(newest)

        @pl.when(low * fourth == 1)
        def _():
            receive_kv(2)
            complete_kv(2)

        @pl.when(with_q == 1)
        def _():
            receive_q(newest)

        def diagonal(step, _):
            c = (core + step) % g

            @pl.when(step * (1 - fifth) == 1)
            def _():
                complete_kv(newest)

            for first in range(g):
                @pl.when(c == first)
                def _():
                    tile(newest, newest * g + first, first * rows, True)

            return 0

        @pl.when(with_kv == 1)
        def _():
            lax.fori_loop(0, g, diagonal, 0)

        @pl.when(side * (second * inner + third * (1 - inner)) == 1)
        def _():
            finish(newest)

        def full(i, _):
            p = early * (pair + 1) + second * (2 + low * (i // 2) + side * i) + low * fourth * 3 + side * third * (1 + i)
            j = early * pair + second * (low * (i % 2) + side * newest) + low * fourth * 2 + side * third * newest * ((i + 1) // 2)
            for c in range(g):
                tile(p, j * g + c)

            @pl.when(third * side + low * fourth == 1)
            def _():
                finish(p)

            return 0

        lax.fori_loop(0, early * s + second * (4 * low + 2 * side) + low * fourth + side * third * 3, full, 0)

        def done(p, _):
            finish(p)
            return 0

        @pl.when((early * s + fifth) * low == 1)
        def _():
            lax.fori_loop(early * pair + fifth * 2, early * (pair + 2) + fifth * 3, done, 0)

        @pl.when(s == 0)
        def _():
            spread(1)
            relay(1)

        @pl.when(s == inner)
        def _():
            for step in range(2, heads):
                spread(step)

        @pl.when(s == 1)
        def _():
            for step in range(2, heads):
                relay(step)
            routed(0)
            routed(1)
            for h in range(2):
                expert_sums[0][1](h)
                sh_pass(h)

        @pl.when(s == 2)
        def _():
            for h in range(2):
                expert_sums[1][1](h)

        return 0

    lax.fori_loop(0, heads + 2, phase, 0)

    def y_copy(dest):
        return to_ep(y_buf.at[dest], ret.at[me], y_ss.at[dest], y_rs.at[me], dest)

    def send_back():
        for part in (1, 0):
            for h in range(2):
                p = (side if part == 0 else 1 - side) * 2 + h
                y_buf[pl.ds(p * g, g)] = expert_sums[part][2](h).astype(bf16).reshape(g, cap, piece)
        for s in range(heads - 1, 0, -1):
            for c in range(g):
                y_copy(nearest(s) * g + c).start()
        for step in range(1, g):
            y_copy(chip * g + lax.rem(core + step, g)).start()
        ret[me] = y_buf[me]

    @pl.when(side == 1)
    def _():
        send_back()

    hn_buf[me] = hn_send[me]
    for step in range(1, n):
        source = lax.rem(me + step, n)
        arrived(hn_buf.at[source], h_rs.at[source])
    loads[10].wait()
    normed = [
        jnp.concatenate([hn_buf[h * g + (part + n - me) % g] for h in range(heads)], axis=1) for part in range(g)]

    def project(dest, h):
        mix_send[dest, h] = jnp.dot(normed[h], w_buf[:, columns(dest)], preferred_element_type=f32).astype(bf16)

    for i in range(2):
        for h in range(2):
            project((corner, across[h])[i], h)
            mix_copies(h)[i].start()
    for h in range(2):
        project(across[1 - h], h)
        project(my_tp, h)
    for h in range(2):
        mix_pass(h)

    @pl.when(side == 0)
    def _():
        send_back()

    out = jnp.concatenate([sh_total(h) for h in range(2)], axis=0)
    rw_pad[...] = jnp.zeros_like(rw_pad)
    rw_pad[:top_k, :tokens] = rw_ref[...]
    scale = rw_pad[...].T
    for step in range(1, n):
        source = lax.rem(me + step, n)
        arrived(ret.at[source], y_rs.at[source])
    returned = ret[...].reshape(n * cap, piece)
    for k in range(top_k):
        out = out + scale[:tokens, k : k + 1] * lax.dot_general(
            place[k].reshape(n * cap, tokens), returned, (((0,), (0,)), ((), ())), preferred_element_type=f32)
    moe_ref[...] = out.astype(bf16)
    moe_store = pltpu.make_async_copy(moe_ref, moe_hbm, out_sem.at[2])
    moe_store.start()
    for h in range(2):
        attn_ref[h] = mix_total(h).astype(bf16)
        pltpu.make_async_copy(attn_ref.at[h], attn_hbm.at[h * sub : (h + 1) * sub], out_sem.at[h]).start()
    for s in range(1, heads):
        p = nearest(s)
        k_copy(p * g + core).wait_send()
        v_copy(p * g + core).wait_send()
        for c in range(g):
            tok_copy(p * g + c).wait_send()
        for i in range(2):
            spread_copy(p, i).wait_send()
            relay_copy(p, i).wait_send()
    for step in range(1, n):
        dest = lax.rem(me + step, n)
        q_copy(dest).wait_send()
        hn_copy(dest).wait_send()
        y_copy(dest).wait_send()
    for step in range(1, g):
        own_copy(step).wait_send()
    for p in range(heads):
        for step in range(1, g):
            for copy in forward(p * g + core, step):
                copy.wait_send()
    sh_sent()
    for part in range(2):
        expert_sums[part][3]()
    mix_sent()
    moe_store.wait()
    for h in range(2):
        pltpu.make_async_copy(attn_ref.at[h], attn_hbm.at[h * sub : (h + 1) * sub], out_sem.at[h]).wait()


def turn_tables(rows, n, head_size):
    half = head_size // 2
    frequency = theta_base ** (-(np.arange(half) * 2.0) / head_size)

    def waves(positions):
        angles = np.tile(positions[:, None] * frequency[None, :], (1, 4))
        return np.stack([np.cos(angles), np.sin(angles)]).astype(np.float32)

    return waves(np.arange(rows)), waves(np.arange(n) * rows)


def exchange_all(
    query_pairs, key_pairs, value_rows, head_lambda, head_gain, out_weight, moe_input, ffn_gain, routes, route_weight,
    gate_weight, up_weight, down_weight, shared_gate, shared_up, shared_down,
):
    n, n_tp = lax.axis_size("ep"), lax.axis_size("tp")
    tokens, model = moe_input.shape
    piece = model // n_tp
    rows = query_pairs.shape[0]
    heads = head_lambda.shape[0]
    width = query_pairs.shape[1] // heads
    head_size = width // 2
    vw = value_rows.shape[1] // heads
    g = n // heads
    sub = rows // g
    keys = g * rows
    cap = -(-(tokens * TOP_K * 5 // (4 * n)) // 8) * 8
    hidden, shared = gate_weight.shape[2], shared_gate.shape[1]
    turns, bases = turn_tables(rows, n, head_size)
    any_spec = pl.BlockSpec(memory_space=pl.ANY)
    dma = pltpu.SemaphoreType.DMA
    buffers = [
        (rows, heads * width), (rows, heads * width), (heads, rows, vw), ((2, rows, width), f32),
        (tokens, model), (tokens, model), (TOP_K, n, cap, tokens), (heads, rows, width), (heads, rows, width),
        (n, sub, width), (n, rows, width), (n, rows, vw), (n, vw + 8, rows), (heads, 2 * rows, width),
        ((heads, vw + 8, keys), f32), ((heads, 1, keys), f32), (n, sub, vw), (n, sub, vw), out_weight.shape,
        (n, cap, piece), (g - 1, n_tp, cap, piece), (n_tp, n, cap, piece),
        (model, hidden), (model, hidden), (hidden, model), (model, shared), (model, shared), (shared, model),
        (n_tp, 2, tokens // 2, piece), (2, 2, tokens // 2, piece), (2, tokens // 2, piece), (2, tokens // 2, piece),
        (2, n_tp, 2, g * cap, piece), (2, 2, 2, g * cap, piece), (2, 2, g * cap, piece), (2, 2, g * cap, piece),
        (n_tp, 2, sub, piece), (2, 2, sub, piece), (2, sub, piece), (2, sub, piece), (n, cap, piece), (n, cap, piece),
        ((8, -(-tokens // 128) * 128), f32),
    ]
    semaphores = [
        (11,), (heads,), (n,), (n,), (n,), (n,), (n,), (n,), (n, g), (n,), (n, g), (n,), (n,), (n,),
        (n,), (n,), (g - 1,), (n,), (heads, 2), (n_tp, heads), (heads, 2), (heads, 2),
        (2, 2), (2, 2), (2,), (2,), (2, 2), (2, 2), (2,), (2,), (2, 2, 2), (2, 2, 2), (2, 2), (2, 2), (n,), (n,),
    ]
    results = pl.pallas_call(
        functools.partial(mega_kernel, n, heads, n_tp, head_size),
        out_shape=(
            jax.ShapeDtypeStruct((rows, piece), bf16),
            jax.ShapeDtypeStruct((tokens, piece), bf16),
        ),
        in_specs=[any_spec] * 18,
        out_specs=(any_spec, any_spec),
        scratch_shapes=[
            pltpu.SMEM((heads,), f32), pltpu.VMEM((1, vw), f32), pltpu.VMEM((TOP_K, tokens), jnp.int32),
            pltpu.VMEM((TOP_K, tokens), f32), pltpu.VMEM((1, model), f32), pltpu.VMEM(bases.shape, f32),
            pltpu.VMEM((2, sub, piece), bf16), pltpu.VMEM((tokens, piece), bf16), dma((6,)), dma((3,)),
        ] + [
            pltpu.VMEM(shape[0], shape[1]) if isinstance(shape[0], tuple) else pltpu.VMEM(shape, bf16)
            for shape in buffers
        ] + [dma(shape) for shape in semaphores],
        compiler_params=pltpu.CompilerParams(
            collective_id=0, has_side_effects=True, vmem_limit_bytes=60 * 2**20),
        cost_estimate=pl.CostEstimate(flops=30 * 10**9, bytes_accessed=24 * 2**20, transcendentals=6 * 10**6),
        name="exchange",
    )(
        head_lambda, head_gain.reshape(1, vw), routes.T, route_weight.T, ffn_gain.reshape(1, model),
        jnp.asarray(turns), jnp.asarray(bases), query_pairs, key_pairs, value_rows, moe_input, out_weight,
        gate_weight, up_weight, down_weight, shared_gate, shared_up, shared_down)
    return pl.pallas_call(
        store_kernel,
        out_shape=tuple(jax.ShapeDtypeStruct(r.shape, r.dtype) for r in results),
        in_specs=[any_spec] * 2,
        out_specs=(any_spec, any_spec),
        scratch_shapes=[pltpu.VMEM(r.shape, r.dtype) for r in results] + [dma((2,)), dma((2,))],
        name="store",
    )(*results)


def store_kernel(attn_ref, moe_ref, attn_out, moe_out, attn_buf, moe_buf, in_sems, out_sems):
    refs = ((attn_ref, attn_buf, attn_out), (moe_ref, moe_buf, moe_out))
    ins = [pltpu.make_async_copy(source, buf, in_sems.at[i]) for i, (source, buf, _) in enumerate(refs)]
    outs = [pltpu.make_async_copy(buf, target, out_sems.at[i]) for i, (_, buf, target) in enumerate(refs)]
    for copy in ins:
        copy.start()
    for i in (1, 0):
        ins[i].wait()
        outs[i].start()
    for copy in outs:
        copy.wait()


def local(
    query_pairs,
    key_pairs,
    value_rows,
    head_lambda,
    head_gain,
    out_weight,
    moe_input,
    ffn_gain,
    routes,
    route_weight,
    gate_weight,
    up_weight,
    down_weight,
    shared_gate,
    shared_up,
    shared_down,
):
    n = lax.axis_size("ep")
    heads = head_lambda.shape[0]
    rows = query_pairs.shape[0]
    fits = n == 2 * heads and heads == 4 and lax.axis_size("tp") == 4 and (rows * heads) % (n * 64) == 0 and routes.shape[0] % 32 == 0
    if fits:
        return exchange_all(
            query_pairs, key_pairs, value_rows, head_lambda, head_gain, out_weight, moe_input, ffn_gain, routes,
            route_weight, gate_weight, up_weight, down_weight, shared_gate, shared_up, shared_down,
        )
    row_values = moe_input.astype(jnp.float32)
    inverse_norm = lax.rsqrt(jnp.mean(row_values * row_values, axis=-1, keepdims=True) + norm_eps)
    normed = (row_values * inverse_norm * ffn_gain).astype(jnp.bfloat16)
    attn_out = generic_attention(query_pairs, key_pairs, value_rows, head_lambda, head_gain, out_weight)
    token_rows = normed.shape[0]
    experts = lax.axis_size("ep")
    capacity = token_rows * TOP_K * 5 // (4 * experts)
    flat_routes = routes.reshape(-1)
    onehot = (flat_routes[:, None] == jnp.arange(experts, dtype=jnp.int32)).astype(jnp.int32)
    slot_rank = jnp.sum((jnp.cumsum(onehot, axis=0) - 1) * onehot, axis=-1)
    slot_index = flat_routes * capacity + slot_rank
    token_index = jnp.arange(token_rows * TOP_K, dtype=jnp.int32) // TOP_K
    slot_rows = (
        jnp.full((experts * capacity,), token_rows, jnp.int32).at[slot_index].set(token_index)
    )
    padded = jnp.concatenate([normed, jnp.zeros((1, normed.shape[1]), jnp.bfloat16)], axis=0)
    outgoing = padded[slot_rows]
    arrived = lax.all_to_all(outgoing, "ep", split_axis=0, concat_axis=0, tiled=True)
    gate_part = jnp.dot(arrived, gate_weight[0], preferred_element_type=jnp.float32)
    up_part = jnp.dot(arrived, up_weight[0], preferred_element_type=jnp.float32)
    hidden = (jax.nn.silu(gate_part) * up_part).astype(jnp.bfloat16)
    expert_terms = jnp.dot(hidden, down_weight[0], preferred_element_type=jnp.float32)
    shared_gated = jnp.dot(normed, shared_gate, preferred_element_type=jnp.float32)
    shared_lifted = jnp.dot(normed, shared_up, preferred_element_type=jnp.float32)
    shared_hidden = (jax.nn.silu(shared_gated) * shared_lifted).astype(jnp.bfloat16)
    shared_terms = jnp.dot(shared_hidden, shared_down, preferred_element_type=jnp.float32)
    expert_sum, shared_sum = (
        lax.psum_scatter(
            expert_terms.astype(jnp.bfloat16), "tp", scatter_dimension=1, tiled=True
        ).astype(jnp.float32),
        lax.psum_scatter(
            shared_terms.astype(jnp.bfloat16), "tp", scatter_dimension=1, tiled=True
        ).astype(jnp.float32),
    )
    returned = lax.all_to_all(
        expert_sum.astype(jnp.bfloat16), "ep", split_axis=0, concat_axis=0, tiled=True
    )
    picked = returned[slot_index.reshape(token_rows, TOP_K)]
    moe_out = (
        jnp.sum(route_weight[..., None] * picked.astype(jnp.float32), axis=1) + shared_sum
    ).astype(jnp.bfloat16)
    return (attn_out, moe_out)


def solution(mesh):
    return jax.shard_map(
        local,
        mesh=mesh,
        in_specs=(
            P("ep", "tp"),
            P("ep", "tp"),
            P("ep", "tp"),
            P("tp"),
            P(),
            P("tp", None),
            P("ep", None),
            P(),
            P("ep", None),
            P("ep", None),
            P("ep", None, "tp"),
            P("ep", None, "tp"),
            P("ep", "tp", None),
            P(None, "tp"),
            P(None, "tp"),
            P("tp", None),
        ),
        out_specs=(P("ep", "tp"), P("ep", "tp")),
        check_vma=False,
    )
```

```python
import functools

import jax
import jax.numpy as jnp
import numpy as np
from jax import lax
from jax.experimental import pallas as pl
from jax.experimental.pallas import tpu as pltpu
from jax.sharding import PartitionSpec as P

TOP_K = 2
KEY_BLOCK = 128


theta_base = 500000.0
norm_eps = 1e-06
masked_low = -1e30


def rotate(inputs, positions):
    half_size = inputs.shape[-1] // 2
    frequency = theta_base ** (-(jnp.arange(half_size, dtype=jnp.float32) * 2.0) / inputs.shape[-1])
    angles = positions.astype(jnp.float32)[:, None] * frequency[None, :]
    cosine = jnp.cos(angles)[:, None, None, :]
    sine_part = jnp.sin(angles)[:, None, None, :]
    front_half = inputs[..., :half_size]
    back_half = inputs[..., half_size:]
    return jnp.concatenate(
        [front_half * cosine - back_half * sine_part, back_half * cosine + front_half * sine_part],
        axis=-1,
    )


def generic_attention(query_pairs, key_pairs, value_rows, head_lambda, head_gain, out_weight):
    local_rows = query_pairs.shape[0]
    local_heads = head_lambda.shape[0]
    head_size = query_pairs.shape[1] // (2 * local_heads)
    value_size = value_rows.shape[1] // local_heads
    positions = lax.axis_index("ep") * local_rows + jnp.arange(local_rows, dtype=jnp.int32)
    rot_queries = rotate(
        query_pairs.astype(jnp.float32).reshape(local_rows, local_heads, 2, head_size), positions
    ).astype(jnp.bfloat16)
    rot_keys = rotate(
        key_pairs.astype(jnp.float32).reshape(local_rows, local_heads, 2, head_size), positions
    ).astype(jnp.bfloat16)
    rot_keys = rot_keys.reshape(local_rows, local_heads * 2 * head_size)
    zero_init = (
        jnp.full((local_heads, 2, local_rows), masked_low, jnp.float32),
        jnp.zeros((local_heads, 2, local_rows), jnp.float32),
        jnp.zeros((local_heads, 2, local_rows, value_size), jnp.float32),
    )
    piece_keys = lax.all_gather(rot_keys, "ep", axis=0, tiled=True)
    piece_values = lax.all_gather(value_rows, "ep", axis=0, tiled=True)
    block_count = piece_keys.shape[0] // KEY_BLOCK
    group_size = 4
    group_count = block_count // group_size
    grouped_keys = piece_keys.reshape(group_count, group_size, KEY_BLOCK, local_heads, 2, head_size)
    grouped_values = piece_values.reshape(
        group_count, group_size, KEY_BLOCK, local_heads, value_size
    )

    def one_group(current, inputs):
        block_keys, block_values, group_index = inputs
        key_positions = group_index * group_size * KEY_BLOCK + jnp.arange(
            group_size * KEY_BLOCK, dtype=jnp.int32
        ).reshape(group_size, KEY_BLOCK)
        scores = jnp.einsum(
            "qhmd,gkhmd->hmqgk", rot_queries, block_keys, preferred_element_type=jnp.float32
        ) * head_size ** (-0.5)
        allowed = key_positions[None, :, :] <= positions[:, None, None]
        scores = jnp.where(allowed, scores, masked_low)
        block_max = jnp.max(scores, axis=-1)
        weights = jnp.where(allowed, jnp.exp(scores - block_max[..., None]), 0.0)
        block_sum = jnp.sum(weights, axis=-1)
        block_out = jnp.einsum(
            "hmqgk,gkhc->hmqgc",
            weights.astype(jnp.bfloat16),
            block_values,
            preferred_element_type=jnp.float32,
        )
        run_max, run_sum, run_out = current
        new_max = jnp.maximum(run_max, jnp.max(block_max, axis=-1))
        old_scale = jnp.exp(run_max - new_max)
        new_scale = jnp.exp(block_max - new_max[..., None])
        run_sum = run_sum * old_scale + jnp.sum(new_scale * block_sum, axis=-1)
        run_out = run_out * old_scale[..., None] + jnp.sum(
            new_scale[..., None] * block_out, axis=-2
        )
        return ((new_max, run_sum, run_out), None)

    result, _ = lax.scan(
        one_group,
        zero_init,
        (grouped_keys, grouped_values, jnp.arange(group_count, dtype=jnp.int32)),
    )
    run_max, run_sum, run_out = result
    map_outputs = run_out / run_sum[..., None]
    difference = map_outputs[:, 0] - head_lambda[:, None, None] * map_outputs[:, 1]
    inverse_rms = lax.rsqrt(jnp.mean(difference * difference, axis=-1, keepdims=True) + norm_eps)
    normed_heads = (difference * inverse_rms * head_gain).astype(jnp.bfloat16)
    head_rows = normed_heads.transpose(1, 0, 2).reshape(local_rows, local_heads * value_size)
    mixer_terms = jnp.dot(head_rows, out_weight, preferred_element_type=jnp.float32)
    attn_out = lax.psum_scatter(
        mixer_terms.astype(jnp.bfloat16), "tp", scatter_dimension=1, tiled=True
    )
    return attn_out


MESH = pl.DeviceIdType.MESH
f32, bf16 = jnp.float32, jnp.bfloat16


def mega_kernel(
    n, heads, n_tp, head_size, lam_hbm, gain_hbm, routes_hbm, rw_hbm, ffn_hbm, turn_ref, base_hbm,
    q_ref, k_ref, v_ref, x_ref, w_ref, wg_ref, wu_ref, wd_ref, sg_ref, su_ref, sd_ref,
    attn_hbm, moe_hbm,
    lam_ref, gain_ref, routes_ref, rw_ref, ffn_ref, base_ref, attn_ref, moe_ref, small, out_sem,
    q_in, k_in, v_in, turn, x_in, xn, place, rq, rk, q_buf, k_buf, v_buf, vt_buf, st_buf, acc, m_buf,
    hn_send, hn_buf, w_buf, out_buf, own_buf, arr, wg, wu, wd, sg, su, sd,
    sh_send, sh_first, sh_held, sh_second, ex_send, ex_first, ex_held, ex_second, mix_send, mix_first, mix_held, mix_second, y_buf, ret, rw_pad,
    load, load_v, q_ss, q_rs, k_ss, k_rs, v_ss, v_rs, fk_ss, fk_rs, fv_ss, fv_rs, h_ss, h_rs,
    t_ss, t_rs, o_ss, o_rs, x_ss, x_rs, d_ss, d_rs, m_ss, m_rs, m2_ss, m2_rs, s_ss, s_rs, s2_ss, s2_rs, e_ss, e_rs, e2_ss, e2_rs, y_ss, y_rs,
):
    me, my_tp = lax.axis_index("ep"), lax.axis_index("tp")
    g = n // heads
    chip, core = me // g, me % g
    rows, width = k_buf.shape[1:]
    vw = v_buf.shape[2]
    sub = rows // g
    cap, piece = out_buf.shape[1:]
    tokens = xn.shape[0]
    top_k = rw_ref.shape[0]
    half = head_size // 2
    side = chip // (heads // 2)

    def mirrored(p):
        return p + side * (heads - 1 - 2 * p)

    near = mirrored(chip)

    def nearest(s):
        return mirrored(jnp.where(s <= near, near - s, s))

    barrier = pltpu.get_barrier_semaphore()
    for step in range(1, n):
        pl.semaphore_signal(barrier, inc=1, device_id={"ep": lax.rem(me + step, n)}, device_id_type=MESH)
    for step in range(1, n_tp):
        pl.semaphore_signal(barrier, inc=1, device_id={"tp": lax.rem(my_tp + step, n_tp)}, device_id_type=MESH)
    loads = [
        pltpu.make_async_copy(source, target, load.at[i])
        for i, (source, target) in enumerate((
            (x_ref, x_in), (turn_ref, turn), (k_ref, k_in), (q_ref, q_in),
            (sg_ref, sg), (su_ref, su), (sd_ref, sd),
            (wg_ref.at[0], wg), (wu_ref.at[0], wu), (wd_ref.at[0], wd), (w_ref, w_buf)))
    ]
    values = [
        pltpu.make_async_copy(v_ref.at[:, h * vw : (h + 1) * vw], v_in.at[h], load_v.at[h]) for h in range(heads)
    ]
    smalls = [
        pltpu.make_async_copy(source, target, small.at[i])
        for i, (source, target) in enumerate((
            (routes_hbm, routes_ref), (ffn_hbm, ffn_ref), (base_hbm, base_ref),
            (lam_hbm, lam_ref), (gain_hbm, gain_ref), (rw_hbm, rw_ref)))]
    for copy in (smalls[0], loads[0], *smalls[1:3], *loads[1:4], *values, *smalls[3:]):
        copy.start()

    def to_ep(source, target, send_sem, recv_sem, dest):
        return pltpu.make_async_remote_copy(
            source, target, send_sem, recv_sem, device_id={"ep": dest}, device_id_type=MESH)

    def to_tp(source, target, send_sem, recv_sem, dest):
        return pltpu.make_async_remote_copy(
            source, target, send_sem, recv_sem, device_id={"tp": dest}, device_id_type=MESH)

    def arrived(ref, sem):
        to_ep(ref, ref, sem, sem, lax.rem(me + 1, n)).wait_recv()

    across = (my_tp + 1 - 2 * (my_tp % 2), (my_tp + 2) % n_tp)
    corner = (across[0] + 2) % n_tp

    def reduction(send, first_in, held, second_in, ss, rs, ss2, rs2, pre=()):
        at = lambda ref, *index: ref.at[(*pre, *index)]

        def first_copies(h):
            return [
                to_tp(at(send, dest, h), at(first_in, h, i), at(ss, h, i), at(rs, h, i), across[h])
                for i, dest in enumerate((corner, across[h]))]

        def second_copy(h):
            return to_tp(at(held, h), at(second_in, h), at(ss2, h), at(rs2, h), across[1 - h])

        def pass_on(h):
            arrived(at(first_in, h, 0), at(rs, h, 0))
            own = send[(*pre, across[1 - h], h)].astype(f32)
            held[(*pre, h)] = (own + first_in[(*pre, h, 0)].astype(f32)).astype(bf16)
            second_copy(h).start()

        def total(h):
            arrived(at(first_in, h, 1), at(rs, h, 1))
            arrived(at(second_in, h), at(rs2, h))
            own = send[(*pre, my_tp, h)].astype(f32)
            return own + first_in[(*pre, h, 1)].astype(f32) + second_in[(*pre, h)].astype(f32)

        def sent():
            for h in range(2):
                for copy in (*first_copies(h), second_copy(h)):
                    copy.wait_send()

        return first_copies, pass_on, total, sent

    def columns(t):
        return pl.ds(pl.multiple_of(t * piece, piece), piece)

    smalls[0].wait()
    expert = lax.broadcasted_iota(jnp.int32, (n, tokens), 0)
    chosen = [(routes_ref[k : k + 1, :] == expert).astype(f32) for k in range(top_k)]
    earlier = lax.broadcasted_iota(jnp.int32, (tokens, tokens), 0) <= lax.broadcasted_iota(jnp.int32, (tokens, tokens), 1)
    ranks = jnp.dot(sum(chosen).astype(bf16), earlier.astype(bf16), preferred_element_type=f32) - 1.0
    slot = ranks + (expert * cap).astype(f32)
    slots = [jnp.sum(c * slot, axis=0, keepdims=True) for c in chosen]
    slot_row = lax.broadcasted_iota(jnp.int32, (n * cap, tokens), 0).astype(f32)
    marks = [(slot_row == s).astype(f32) for s in slots]
    for k in range(top_k):
        place[k] = marks[k].astype(bf16).reshape(n, cap, tokens)
    loads[0].wait()
    smalls[1].wait()
    x = x_in[...].astype(f32)
    inverse = lax.rsqrt(jnp.mean(x * x, axis=-1, keepdims=True) + norm_eps)
    xn[...] = (x * inverse * ffn_ref[...]).astype(bf16)
    out_buf[...] = jnp.dot(
        sum(marks).astype(bf16), xn[:, columns(my_tp)], preferred_element_type=f32).astype(bf16).reshape(n, cap, piece)

    def own_rows(dest):
        mark = place[0, dest]
        for k in range(1, top_k):
            mark = mark + place[k, dest]
        return jnp.dot(mark, xn[...], preferred_element_type=f32).astype(bf16)

    pl.semaphore_wait(barrier, n - 1 + n_tp - 1)
    for copy in loads[4:]:
        copy.start()

    def tok_copy(dest):
        return to_ep(out_buf.at[dest], arr.at[my_tp, me], t_ss.at[dest], t_rs.at[me], dest)

    def own_copy(step):
        dest = chip * g + lax.rem(core + step, g)
        return to_ep(own_buf.at[step - 1], arr.at[:, me], o_ss.at[step - 1], o_rs.at[me], dest)

    mate_chip = chip + 1 - 2 * (chip % 2)
    inner = (chip + side) % 2

    def send_tokens(first, last):
        for s in range(first, last):
            for c in range(g):
                tok_copy(nearest(s) * g + c).start()

    send_tokens(1, 2)

    @pl.when(inner == 1)
    def _():
        send_tokens(2, heads)

    for step in range(g):
        full = own_rows(chip * g + lax.rem(core + step, g))
        for t in range(n_tp):
            part = full[:, t * piece : (t + 1) * piece]
            if step == 0:
                arr[t, me] = part
            else:
                own_buf[step - 1, t] = part
        if step:
            own_copy(step).start()

    smalls[2].wait()
    base_cos, base_sin = base_ref[0, pl.ds(me, 1)], base_ref[1, pl.ds(me, 1)]
    lane = lax.broadcasted_iota(jnp.int32, (1, width), 1)
    front = lane % head_size < half
    loads[1].wait()
    cosine = turn[0] * base_cos - turn[1] * base_sin
    sine = turn[1] * base_cos + turn[0] * base_sin
    sine = jnp.where(front, -sine, sine)

    def turned(source, h):
        x = source[:, h * width : (h + 1) * width].astype(f32)
        partner = jnp.where(front, pltpu.roll(x, width - half, 1), pltpu.roll(x, half, 1))
        return (x * cosine + partner * sine).astype(bf16)

    loads[2].wait()
    for h in range(heads):
        rk[h] = turned(k_in, h)
    loads[3].wait()
    for h in range(heads):
        rq[h] = turned(q_in, h) * jnp.asarray(head_size ** -0.5, bf16)
    for copy in values:
        copy.wait()

    def q_rows(dest):
        return pl.ds(pl.multiple_of(((dest % g + me) % g) * sub, sub), sub)

    def q_copy(dest):
        return to_ep(rq.at[dest // g, q_rows(dest)], q_buf.at[me], q_ss.at[dest], q_rs.at[me], dest)

    def k_copy(dest):
        return to_ep(rk.at[dest // g], k_buf.at[me], k_ss.at[dest], k_rs.at[me], dest)

    def v_copy(dest):
        return to_ep(v_in.at[dest // g], v_buf.at[me], v_ss.at[dest], v_rs.at[me], dest)

    def send_kv(p):
        k_copy(p * g + core).start()
        v_copy(p * g + core).start()

    def send_q(p):
        for c in range(g):
            q_copy(p * g + c).start()

    for step in range(1, g):
        q_copy(chip * g + lax.rem(core + step, g)).start()
    send_kv(mate_chip)
    send_q(mate_chip)

    @pl.when(inner == 0)
    def _():
        send_tokens(2, heads)

    @pl.when(side == 0)
    def _():
        for i in (0, 1):
            send_kv(2 + (inner + i) % 2)
            send_q(2 + (inner + i) % 2)

    @pl.when(side == 1)
    def _():
        for s in range(2, heads):
            send_q(nearest(s))
        for i in (1, 0):
            send_kv((inner + i) % 2)

    q_buf[me] = rq[chip, q_rows(me)]
    k_buf[me] = rk[chip]
    v_buf[me] = v_in[chip]

    def gated(gate, up):
        return (gate / (1.0 + jnp.exp(-gate)) * up).astype(bf16)

    for i in (4, 5, 6):
        loads[i].wait()
    hidden = gated(
        jnp.dot(xn[...], sg[...], preferred_element_type=f32), jnp.dot(xn[...], su[...], preferred_element_type=f32))

    sh_copies, sh_pass, sh_total, sh_sent = reduction(
        sh_send, sh_first, sh_held, sh_second, s_ss, s_rs, s2_ss, s2_rs)
    half_tokens = tokens // 2

    def shared_down(dest, h):
        sh_send[dest, h] = jnp.dot(
            hidden[h * half_tokens : (h + 1) * half_tokens], sd[:, columns(dest)],
            preferred_element_type=f32).astype(bf16)

    for i in range(2):
        for h in range(2):
            shared_down((corner, across[h])[i], h)
            sh_copies(h)[i].start()
    for h in range(2):
        shared_down(across[1 - h], h)
        shared_down(my_tp, h)

    for copy in smalls[3:]:
        copy.wait()
    lam = lam_ref[chip]
    gain = gain_ref[...]
    vt_rows = vt_buf.shape[1]
    keys = g * rows
    lane_row = lax.broadcasted_iota(jnp.int32, (sub, width), 1)

    def forward(source, step):
        to = chip * g + lax.rem(core + step, g)
        return (
            to_ep(k_buf.at[source], k_buf.at[source], fk_ss.at[source, step], fk_rs.at[source], to),
            to_ep(v_buf.at[source], v_buf.at[source], fv_ss.at[source, step], fv_rs.at[source], to),
        )

    def prepare_kv(e):
        vt_buf[e, :vw] = v_buf[e].astype(f32).T.astype(bf16)
        vt_buf[e, vw:] = jnp.ones((vt_rows - vw, rows), bf16)

    def receive_kv(p):
        direct = p * g + core

        @pl.when(direct != me)
        def _():
            arrived(k_buf.at[direct], k_rs.at[direct])
            arrived(v_buf.at[direct], v_rs.at[direct])

        for step in range(1, g):
            for copy in forward(direct, step):
                copy.start()
        prepare_kv(direct)

    def complete_kv(p):
        for step in range(1, g):
            other = p * g + lax.rem(core + step, g)
            arrived(k_buf.at[other], fk_rs.at[other])
            arrived(v_buf.at[other], fv_rs.at[other])
            prepare_kv(other)

    def receive_q(p):
        for c in range(g):
            e = p * g + c

            @pl.when(e != me)
            def _():
                arrived(q_buf.at[e], q_rs.at[e])

            q = q_buf[e]
            zero = jnp.zeros_like(q)
            st_buf[p, 2 * c * sub : (2 * c + 1) * sub] = jnp.where(lane_row < width // 2, q, zero)
            st_buf[p, (2 * c + 1) * sub : (2 * c + 2) * sub] = jnp.where(lane_row < width // 2, zero, q)
        m_buf[p] = jnp.full((1, keys), masked_low, f32)
        acc[p] = jnp.zeros((vt_rows, keys), f32)

    def tile(p, e, first=0, diagonal=False):
        span = slice(first, keys)
        size = keys - first
        s = lax.dot_general(k_buf[e], st_buf[p, span], (((1,), (1,)), ((), ())), preferred_element_type=f32)
        if diagonal:
            key = lax.broadcasted_iota(jnp.int32, (rows, size), 0) + first
            column = lax.broadcasted_iota(jnp.int32, (rows, size), 1) + first
            block = column // rows
            query = block * rows + column % sub + (core + block) % g * sub
            s = jnp.where(key <= query, s, masked_low)
        old = m_buf[p, :, span]
        m = jnp.maximum(old, jnp.max(s, axis=0, keepdims=True))
        weights = jnp.exp(s - m).astype(bf16)
        m_buf[p, :, span] = m
        acc[p, :, span] = acc[p, :, span] * jnp.exp(old - m) + jnp.dot(
            vt_buf[e], weights, preferred_element_type=f32)

    def hn_copy(dest):
        return to_ep(hn_send.at[dest], hn_buf.at[me], h_ss.at[dest], h_rs.at[me], dest)

    def finish(p):
        a = (acc[p, :vw] / acc[p, vw : vw + 1]).T
        for c in range(g):
            e = p * g + c
            diff = a[2 * c * sub : (2 * c + 1) * sub] - lam * a[(2 * c + 1) * sub : (2 * c + 2) * sub]
            inverse = lax.rsqrt(jnp.mean(diff * diff, axis=-1, keepdims=True) + norm_eps)
            hn_send[e] = (diff * inverse * gain).astype(bf16)

            @pl.when(e != me)
            def _():
                hn_copy(e).start()

    def spread_copy(p, i):
        part = arr.at[my_tp, pl.ds(p * g, g)]
        return to_tp(part, part, x_ss.at[p, i], x_rs.at[my_tp, p], across[i])

    def relay_copy(p, c):
        part = arr.at[across[c], p * g + c]
        return to_tp(part, part, d_ss.at[p, c], d_rs.at[p, c], across[1 - c])

    def spread(s):
        p = nearest(s)
        for c in range(g):
            arrived(arr.at[my_tp, p * g + c], t_rs.at[p * g + c])
        for i in range(2):
            spread_copy(p, i).start()

    def relay(s):
        p = nearest(s)
        for c in range(2):
            arrived(arr.at[across[c], pl.ds(p * g, g)], x_rs.at[across[c], p])
            relay_copy(p, c).start()

    expert_sums = [
        reduction(ex_send, ex_first, ex_held, ex_second, e_ss, e_rs, e2_ss, e2_rs, (part,)) for part in range(2)]
    mix_copies, mix_pass, mix_total, mix_sent = reduction(
        mix_send, mix_first, mix_held, mix_second, m_ss, m_rs, m2_ss, m2_rs)
    def routed(part):
        half = n // 2
        start = half * (side if part == 0 else 1 - side)
        if part == 0:
            for step in range(1, g):
                other = chip * g + lax.rem(core + step, g)
                arrived(arr.at[:, other], o_rs.at[other])
        for s in range(1, 2) if part == 0 else range(2, heads):
            for c in range(2):
                arrived(arr.at[corner, nearest(s) * g + c], d_rs.at[nearest(s), c])
        if part == 0:
            for i in (7, 8, 9):
                loads[i].wait()
        gate = up = None
        for t in range(n_tp):
            block = arr[t, pl.ds(start, half)].reshape(half * cap, piece)
            span = slice(t * piece, (t + 1) * piece)
            gate_part = jnp.dot(block, wg[span, :], preferred_element_type=f32)
            up_part = jnp.dot(block, wu[span, :], preferred_element_type=f32)
            gate = gate_part if gate is None else gate + gate_part
            up = up_part if up is None else up + up_part
        hidden = gated(gate, up)
        quarter = half // 2 * cap

        def down(dest, h):
            ex_send[part, dest, h] = jnp.dot(
                hidden[h * quarter : (h + 1) * quarter], wd[:, columns(dest)], preferred_element_type=f32).astype(bf16)

        copies = expert_sums[part][0]
        for i in range(2):
            for h in range(2):
                down((corner, across[h])[i], h)
                copies(h)[i].start()
        for h in range(2):
            down(across[1 - h], h)
            down(my_tp, h)

    low, pair = 1 - side, 2 * side

    def phase(s, _):
        early = (5 - s) // 4
        second = (s // 2) * (1 - s // 3)
        third = (s // 3) * (1 - s // 4)
        fourth = (s // 4) * (1 - s // 5)
        fifth = s // 5
        newest = early * (chip + s * (mate_chip - chip)) + (1 - early) * (
            low * (third * 3 + (fourth + fifth) * 2) + side * (second * (1 - inner) + third * inner))
        with_q = early + side * (second + third)
        with_kv = with_q + low * (third + fifth)

        @pl.when(low * second == 1)
        def _():
            for p in (2, 3):
                receive_q(p)

        @pl.when(with_kv - low * fifth == 1)
        def _():
            receive_kv(newest)

        @pl.when(low * fourth == 1)
        def _():
            receive_kv(2)
            complete_kv(2)

        @pl.when(with_q == 1)
        def _():
            receive_q(newest)

        def diagonal(step, _):
            c = (core + step) % g

            @pl.when(step * (1 - fifth) == 1)
            def _():
                complete_kv(newest)

            for first in range(g):
                @pl.when(c == first)
                def _():
                    tile(newest, newest * g + first, first * rows, True)

            return 0

        @pl.when(with_kv == 1)
        def _():
            lax.fori_loop(0, g, diagonal, 0)

        @pl.when(side * (second * inner + third * (1 - inner)) == 1)
        def _():
            finish(newest)

        def full(i, _):
            p = early * (pair + 1) + second * (2 + low * (i // 2) + side * i) + low * fourth * 3 + side * third * (1 + i)
            j = early * pair + second * (low * (i % 2) + side * newest) + low * fourth * 2 + side * third * newest * ((i + 1) // 2)
            for c in range(g):
                tile(p, j * g + c)

            @pl.when(third * side + low * fourth == 1)
            def _():
                finish(p)

            return 0

        lax.fori_loop(0, early * s + second * (4 * low + 2 * side) + low * fourth + side * third * 3, full, 0)

        def done(p, _):
            finish(p)
            return 0

        @pl.when((early * s + fifth) * low == 1)
        def _():
            lax.fori_loop(early * pair + fifth * 2, early * (pair + 2) + fifth * 3, done, 0)

        @pl.when(s == 0)
        def _():
            spread(1)
            relay(1)

        @pl.when(s == inner)
        def _():
            for step in range(2, heads):
                spread(step)

        @pl.when(s == 1 + low * inner)
        def _():
            for step in range(2, heads):
                relay(step)
            routed(0)

        @pl.when(s == 1 + low * inner)
        def _():
            routed(1)
            for h in range(2):
                expert_sums[0][1](h)
                sh_pass(h)

        @pl.when(s == 2 + 2 * low * inner)
        def _():
            for h in range(2):
                expert_sums[1][1](h)

        return 0

    lax.fori_loop(0, heads + 2, phase, 0)

    def y_copy(dest):
        return to_ep(y_buf.at[dest], ret.at[me], y_ss.at[dest], y_rs.at[me], dest)

    def send_back():
        for part in (1, 0):
            for h in range(2):
                p = (side if part == 0 else 1 - side) * 2 + h
                y_buf[pl.ds(p * g, g)] = expert_sums[part][2](h).astype(bf16).reshape(g, cap, piece)
        for s in range(heads - 1, 0, -1):
            for c in range(g):
                y_copy(nearest(s) * g + c).start()
        for step in range(1, g):
            y_copy(chip * g + lax.rem(core + step, g)).start()
        ret[me] = y_buf[me]

    @pl.when(side == 1)
    def _():
        send_back()

    hn_buf[me] = hn_send[me]
    for step in range(1, n):
        source = lax.rem(me + step, n)
        arrived(hn_buf.at[source], h_rs.at[source])
    loads[10].wait()
    normed = [
        jnp.concatenate([hn_buf[h * g + (part + n - me) % g] for h in range(heads)], axis=1) for part in range(g)]

    def project(dest, h):
        mix_send[dest, h] = jnp.dot(normed[h], w_buf[:, columns(dest)], preferred_element_type=f32).astype(bf16)

    for i in range(2):
        for h in range(2):
            project((corner, across[h])[i], h)
            mix_copies(h)[i].start()
    for h in range(2):
        project(across[1 - h], h)
        project(my_tp, h)
    for h in range(2):
        mix_pass(h)

    @pl.when(side == 0)
    def _():
        send_back()

    out = jnp.concatenate([sh_total(h) for h in range(2)], axis=0)
    rw_pad[...] = jnp.zeros_like(rw_pad)
    rw_pad[:top_k, :tokens] = rw_ref[...]
    scale = rw_pad[...].T
    for step in range(1, n):
        source = lax.rem(me + step, n)
        arrived(ret.at[source], y_rs.at[source])
    returned = ret[...].reshape(n * cap, piece)
    for k in range(top_k):
        out = out + scale[:tokens, k : k + 1] * lax.dot_general(
            place[k].reshape(n * cap, tokens), returned, (((0,), (0,)), ((), ())), preferred_element_type=f32)
    moe_ref[...] = out.astype(bf16)
    moe_store = pltpu.make_async_copy(moe_ref, moe_hbm, out_sem.at[2])
    moe_store.start()
    for h in range(2):
        attn_ref[h] = mix_total(h).astype(bf16)
        pltpu.make_async_copy(attn_ref.at[h], attn_hbm.at[h * sub : (h + 1) * sub], out_sem.at[h]).start()
    for s in range(1, heads):
        p = nearest(s)
        k_copy(p * g + core).wait_send()
        v_copy(p * g + core).wait_send()
        for c in range(g):
            tok_copy(p * g + c).wait_send()
        for i in range(2):
            spread_copy(p, i).wait_send()
            relay_copy(p, i).wait_send()
    for step in range(1, n):
        dest = lax.rem(me + step, n)
        q_copy(dest).wait_send()
        hn_copy(dest).wait_send()
        y_copy(dest).wait_send()
    for step in range(1, g):
        own_copy(step).wait_send()
    for p in range(heads):
        for step in range(1, g):
            for copy in forward(p * g + core, step):
                copy.wait_send()
    sh_sent()
    for part in range(2):
        expert_sums[part][3]()
    mix_sent()
    moe_store.wait()
    for h in range(2):
        pltpu.make_async_copy(attn_ref.at[h], attn_hbm.at[h * sub : (h + 1) * sub], out_sem.at[h]).wait()


def turn_tables(rows, n, head_size):
    half = head_size // 2
    frequency = theta_base ** (-(np.arange(half) * 2.0) / head_size)

    def waves(positions):
        angles = np.tile(positions[:, None] * frequency[None, :], (1, 4))
        return np.stack([np.cos(angles), np.sin(angles)]).astype(np.float32)

    return waves(np.arange(rows)), waves(np.arange(n) * rows)


def exchange_all(
    query_pairs, key_pairs, value_rows, head_lambda, head_gain, out_weight, moe_input, ffn_gain, routes, route_weight,
    gate_weight, up_weight, down_weight, shared_gate, shared_up, shared_down,
):
    n, n_tp = lax.axis_size("ep"), lax.axis_size("tp")
    tokens, model = moe_input.shape
    piece = model // n_tp
    rows = query_pairs.shape[0]
    heads = head_lambda.shape[0]
    width = query_pairs.shape[1] // heads
    head_size = width // 2
    vw = value_rows.shape[1] // heads
    g = n // heads
    sub = rows // g
    keys = g * rows
    cap = -(-(tokens * TOP_K * 5 // (4 * n)) // 8) * 8
    hidden, shared = gate_weight.shape[2], shared_gate.shape[1]
    turns, bases = turn_tables(rows, n, head_size)
    any_spec = pl.BlockSpec(memory_space=pl.ANY)
    dma = pltpu.SemaphoreType.DMA
    buffers = [
        (rows, heads * width), (rows, heads * width), (heads, rows, vw), ((2, rows, width), f32),
        (tokens, model), (tokens, model), (TOP_K, n, cap, tokens), (heads, rows, width), (heads, rows, width),
        (n, sub, width), (n, rows, width), (n, rows, vw), (n, vw + 8, rows), (heads, 2 * rows, width),
        ((heads, vw + 8, keys), f32), ((heads, 1, keys), f32), (n, sub, vw), (n, sub, vw), out_weight.shape,
        (n, cap, piece), (g - 1, n_tp, cap, piece), (n_tp, n, cap, piece),
        (model, hidden), (model, hidden), (hidden, model), (model, shared), (model, shared), (shared, model),
        (n_tp, 2, tokens // 2, piece), (2, 2, tokens // 2, piece), (2, tokens // 2, piece), (2, tokens // 2, piece),
        (2, n_tp, 2, g * cap, piece), (2, 2, 2, g * cap, piece), (2, 2, g * cap, piece), (2, 2, g * cap, piece),
        (n_tp, 2, sub, piece), (2, 2, sub, piece), (2, sub, piece), (2, sub, piece), (n, cap, piece), (n, cap, piece),
        ((8, -(-tokens // 128) * 128), f32),
    ]
    semaphores = [
        (11,), (heads,), (n,), (n,), (n,), (n,), (n,), (n,), (n, g), (n,), (n, g), (n,), (n,), (n,),
        (n,), (n,), (g - 1,), (n,), (heads, 2), (n_tp, heads), (heads, 2), (heads, 2),
        (2, 2), (2, 2), (2,), (2,), (2, 2), (2, 2), (2,), (2,), (2, 2, 2), (2, 2, 2), (2, 2), (2, 2), (n,), (n,),
    ]
    results = pl.pallas_call(
        functools.partial(mega_kernel, n, heads, n_tp, head_size),
        out_shape=(
            jax.ShapeDtypeStruct((rows, piece), bf16),
            jax.ShapeDtypeStruct((tokens, piece), bf16),
        ),
        in_specs=[any_spec] * 18,
        out_specs=(any_spec, any_spec),
        scratch_shapes=[
            pltpu.SMEM((heads,), f32), pltpu.VMEM((1, vw), f32), pltpu.VMEM((TOP_K, tokens), jnp.int32),
            pltpu.VMEM((TOP_K, tokens), f32), pltpu.VMEM((1, model), f32), pltpu.VMEM(bases.shape, f32),
            pltpu.VMEM((2, sub, piece), bf16), pltpu.VMEM((tokens, piece), bf16), dma((6,)), dma((3,)),
        ] + [
            pltpu.VMEM(shape[0], shape[1]) if isinstance(shape[0], tuple) else pltpu.VMEM(shape, bf16)
            for shape in buffers
        ] + [dma(shape) for shape in semaphores],
        compiler_params=pltpu.CompilerParams(
            collective_id=0, has_side_effects=True, vmem_limit_bytes=60 * 2**20),
        cost_estimate=pl.CostEstimate(flops=30 * 10**9, bytes_accessed=24 * 2**20, transcendentals=6 * 10**6),
        name="exchange",
    )(
        head_lambda, head_gain.reshape(1, vw), routes.T, route_weight.T, ffn_gain.reshape(1, model),
        jnp.asarray(turns), jnp.asarray(bases), query_pairs, key_pairs, value_rows, moe_input, out_weight,
        gate_weight, up_weight, down_weight, shared_gate, shared_up, shared_down)
    return pl.pallas_call(
        store_kernel,
        out_shape=tuple(jax.ShapeDtypeStruct(r.shape, r.dtype) for r in results),
        in_specs=[any_spec] * 2,
        out_specs=(any_spec, any_spec),
        scratch_shapes=[pltpu.VMEM(r.shape, r.dtype) for r in results] + [dma((2,)), dma((2,))],
        name="store",
    )(*results)


def store_kernel(attn_ref, moe_ref, attn_out, moe_out, attn_buf, moe_buf, in_sems, out_sems):
    refs = ((attn_ref, attn_buf, attn_out), (moe_ref, moe_buf, moe_out))
    ins = [pltpu.make_async_copy(source, buf, in_sems.at[i]) for i, (source, buf, _) in enumerate(refs)]
    outs = [pltpu.make_async_copy(buf, target, out_sems.at[i]) for i, (_, buf, target) in enumerate(refs)]
    for copy in ins:
        copy.start()
    for i in (1, 0):
        ins[i].wait()
        outs[i].start()
    for copy in outs:
        copy.wait()


def local(
    query_pairs,
    key_pairs,
    value_rows,
    head_lambda,
    head_gain,
    out_weight,
    moe_input,
    ffn_gain,
    routes,
    route_weight,
    gate_weight,
    up_weight,
    down_weight,
    shared_gate,
    shared_up,
    shared_down,
):
    n = lax.axis_size("ep")
    heads = head_lambda.shape[0]
    rows = query_pairs.shape[0]
    fits = n == 2 * heads and heads == 4 and lax.axis_size("tp") == 4 and (rows * heads) % (n * 64) == 0 and routes.shape[0] % 32 == 0
    if fits:
        return exchange_all(
            query_pairs, key_pairs, value_rows, head_lambda, head_gain, out_weight, moe_input, ffn_gain, routes,
            route_weight, gate_weight, up_weight, down_weight, shared_gate, shared_up, shared_down,
        )
    row_values = moe_input.astype(jnp.float32)
    inverse_norm = lax.rsqrt(jnp.mean(row_values * row_values, axis=-1, keepdims=True) + norm_eps)
    normed = (row_values * inverse_norm * ffn_gain).astype(jnp.bfloat16)
    attn_out = generic_attention(query_pairs, key_pairs, value_rows, head_lambda, head_gain, out_weight)
    token_rows = normed.shape[0]
    experts = lax.axis_size("ep")
    capacity = token_rows * TOP_K * 5 // (4 * experts)
    flat_routes = routes.reshape(-1)
    onehot = (flat_routes[:, None] == jnp.arange(experts, dtype=jnp.int32)).astype(jnp.int32)
    slot_rank = jnp.sum((jnp.cumsum(onehot, axis=0) - 1) * onehot, axis=-1)
    slot_index = flat_routes * capacity + slot_rank
    token_index = jnp.arange(token_rows * TOP_K, dtype=jnp.int32) // TOP_K
    slot_rows = (
        jnp.full((experts * capacity,), token_rows, jnp.int32).at[slot_index].set(token_index)
    )
    padded = jnp.concatenate([normed, jnp.zeros((1, normed.shape[1]), jnp.bfloat16)], axis=0)
    outgoing = padded[slot_rows]
    arrived = lax.all_to_all(outgoing, "ep", split_axis=0, concat_axis=0, tiled=True)
    gate_part = jnp.dot(arrived, gate_weight[0], preferred_element_type=jnp.float32)
    up_part = jnp.dot(arrived, up_weight[0], preferred_element_type=jnp.float32)
    hidden = (jax.nn.silu(gate_part) * up_part).astype(jnp.bfloat16)
    expert_terms = jnp.dot(hidden, down_weight[0], preferred_element_type=jnp.float32)
    shared_gated = jnp.dot(normed, shared_gate, preferred_element_type=jnp.float32)
    shared_lifted = jnp.dot(normed, shared_up, preferred_element_type=jnp.float32)
    shared_hidden = (jax.nn.silu(shared_gated) * shared_lifted).astype(jnp.bfloat16)
    shared_terms = jnp.dot(shared_hidden, shared_down, preferred_element_type=jnp.float32)
    expert_sum, shared_sum = (
        lax.psum_scatter(
            expert_terms.astype(jnp.bfloat16), "tp", scatter_dimension=1, tiled=True
        ).astype(jnp.float32),
        lax.psum_scatter(
            shared_terms.astype(jnp.bfloat16), "tp", scatter_dimension=1, tiled=True
        ).astype(jnp.float32),
    )
    returned = lax.all_to_all(
        expert_sum.astype(jnp.bfloat16), "ep", split_axis=0, concat_axis=0, tiled=True
    )
    picked = returned[slot_index.reshape(token_rows, TOP_K)]
    moe_out = (
        jnp.sum(route_weight[..., None] * picked.astype(jnp.float32), axis=1) + shared_sum
    ).astype(jnp.bfloat16)
    return (attn_out, moe_out)


def solution(mesh):
    return jax.shard_map(
        local,
        mesh=mesh,
        in_specs=(
            P("ep", "tp"),
            P("ep", "tp"),
            P("ep", "tp"),
            P("tp"),
            P(),
            P("tp", None),
            P("ep", None),
            P(),
            P("ep", None),
            P("ep", None),
            P("ep", None, "tp"),
            P("ep", None, "tp"),
            P("ep", "tp", None),
            P(None, "tp"),
            P(None, "tp"),
            P("tp", None),
        ),
        out_specs=(P("ep", "tp"), P("ep", "tp")),
        check_vma=False,
    )
```

```python
import functools

import jax
import jax.numpy as jnp
import numpy as np
from jax import lax
from jax.experimental import pallas as pl
from jax.experimental.pallas import tpu as pltpu
from jax.sharding import PartitionSpec as P

TOP_K = 2
KEY_BLOCK = 128


theta_base = 500000.0
norm_eps = 1e-06
masked_low = -1e30


def rotate(inputs, positions):
    half_size = inputs.shape[-1] // 2
    frequency = theta_base ** (-(jnp.arange(half_size, dtype=jnp.float32) * 2.0) / inputs.shape[-1])
    angles = positions.astype(jnp.float32)[:, None] * frequency[None, :]
    cosine = jnp.cos(angles)[:, None, None, :]
    sine_part = jnp.sin(angles)[:, None, None, :]
    front_half = inputs[..., :half_size]
    back_half = inputs[..., half_size:]
    return jnp.concatenate(
        [front_half * cosine - back_half * sine_part, back_half * cosine + front_half * sine_part],
        axis=-1,
    )


def generic_attention(query_pairs, key_pairs, value_rows, head_lambda, head_gain, out_weight):
    local_rows = query_pairs.shape[0]
    local_heads = head_lambda.shape[0]
    head_size = query_pairs.shape[1] // (2 * local_heads)
    value_size = value_rows.shape[1] // local_heads
    positions = lax.axis_index("ep") * local_rows + jnp.arange(local_rows, dtype=jnp.int32)
    rot_queries = rotate(
        query_pairs.astype(jnp.float32).reshape(local_rows, local_heads, 2, head_size), positions
    ).astype(jnp.bfloat16)
    rot_keys = rotate(
        key_pairs.astype(jnp.float32).reshape(local_rows, local_heads, 2, head_size), positions
    ).astype(jnp.bfloat16)
    rot_keys = rot_keys.reshape(local_rows, local_heads * 2 * head_size)
    zero_init = (
        jnp.full((local_heads, 2, local_rows), masked_low, jnp.float32),
        jnp.zeros((local_heads, 2, local_rows), jnp.float32),
        jnp.zeros((local_heads, 2, local_rows, value_size), jnp.float32),
    )
    piece_keys = lax.all_gather(rot_keys, "ep", axis=0, tiled=True)
    piece_values = lax.all_gather(value_rows, "ep", axis=0, tiled=True)
    block_count = piece_keys.shape[0] // KEY_BLOCK
    group_size = 4
    group_count = block_count // group_size
    grouped_keys = piece_keys.reshape(group_count, group_size, KEY_BLOCK, local_heads, 2, head_size)
    grouped_values = piece_values.reshape(
        group_count, group_size, KEY_BLOCK, local_heads, value_size
    )

    def one_group(current, inputs):
        block_keys, block_values, group_index = inputs
        key_positions = group_index * group_size * KEY_BLOCK + jnp.arange(
            group_size * KEY_BLOCK, dtype=jnp.int32
        ).reshape(group_size, KEY_BLOCK)
        scores = jnp.einsum(
            "qhmd,gkhmd->hmqgk", rot_queries, block_keys, preferred_element_type=jnp.float32
        ) * head_size ** (-0.5)
        allowed = key_positions[None, :, :] <= positions[:, None, None]
        scores = jnp.where(allowed, scores, masked_low)
        block_max = jnp.max(scores, axis=-1)
        weights = jnp.where(allowed, jnp.exp(scores - block_max[..., None]), 0.0)
        block_sum = jnp.sum(weights, axis=-1)
        block_out = jnp.einsum(
            "hmqgk,gkhc->hmqgc",
            weights.astype(jnp.bfloat16),
            block_values,
            preferred_element_type=jnp.float32,
        )
        run_max, run_sum, run_out = current
        new_max = jnp.maximum(run_max, jnp.max(block_max, axis=-1))
        old_scale = jnp.exp(run_max - new_max)
        new_scale = jnp.exp(block_max - new_max[..., None])
        run_sum = run_sum * old_scale + jnp.sum(new_scale * block_sum, axis=-1)
        run_out = run_out * old_scale[..., None] + jnp.sum(
            new_scale[..., None] * block_out, axis=-2
        )
        return ((new_max, run_sum, run_out), None)

    result, _ = lax.scan(
        one_group,
        zero_init,
        (grouped_keys, grouped_values, jnp.arange(group_count, dtype=jnp.int32)),
    )
    run_max, run_sum, run_out = result
    map_outputs = run_out / run_sum[..., None]
    difference = map_outputs[:, 0] - head_lambda[:, None, None] * map_outputs[:, 1]
    inverse_rms = lax.rsqrt(jnp.mean(difference * difference, axis=-1, keepdims=True) + norm_eps)
    normed_heads = (difference * inverse_rms * head_gain).astype(jnp.bfloat16)
    head_rows = normed_heads.transpose(1, 0, 2).reshape(local_rows, local_heads * value_size)
    mixer_terms = jnp.dot(head_rows, out_weight, preferred_element_type=jnp.float32)
    attn_out = lax.psum_scatter(
        mixer_terms.astype(jnp.bfloat16), "tp", scatter_dimension=1, tiled=True
    )
    return attn_out


MESH = pl.DeviceIdType.MESH
f32, bf16 = jnp.float32, jnp.bfloat16


def mega_kernel(
    n, heads, n_tp, head_size, lam_hbm, gain_hbm, routes_hbm, rw_hbm, ffn_hbm, turn_ref, base_hbm,
    q_ref, k_ref, v_ref, x_ref, w_ref, wg_ref, wu_ref, wd_ref, sg_ref, su_ref, sd_ref,
    attn_hbm, moe_hbm,
    lam_ref, gain_ref, routes_ref, rw_ref, ffn_ref, base_ref, attn_ref, moe_ref, small, out_sem,
    q_in, k_in, v_in, turn, x_in, xn, place, rq, rk, q_buf, k_buf, v_buf, vt_buf, st_buf, acc, m_buf,
    hn_send, hn_buf, w_buf, out_buf, own_buf, arr, wg, wu, wd, sg, su, sd,
    sh_send, sh_first, sh_held, sh_second, ex_send, ex_first, ex_held, ex_second, mix_send, mix_first, mix_held, mix_second, y_buf, ret, rw_pad,
    load, load_v, q_ss, q_rs, k_ss, k_rs, v_ss, v_rs, fk_ss, fk_rs, fv_ss, fv_rs, h_ss, h_rs,
    t_ss, t_rs, o_ss, o_rs, x_ss, x_rs, d_ss, d_rs, m_ss, m_rs, m2_ss, m2_rs, s_ss, s_rs, s2_ss, s2_rs, e_ss, e_rs, e2_ss, e2_rs, y_ss, y_rs,
):
    me, my_tp = lax.axis_index("ep"), lax.axis_index("tp")
    g = n // heads
    chip, core = me // g, me % g
    rows, width = k_buf.shape[1:]
    vw = v_buf.shape[2]
    sub = rows // g
    cap, piece = out_buf.shape[1:]
    tokens = xn.shape[0]
    top_k = rw_ref.shape[0]
    half = head_size // 2
    side = chip // (heads // 2)

    def mirrored(p):
        return p + side * (heads - 1 - 2 * p)

    near = mirrored(chip)

    def nearest(s):
        return mirrored(jnp.where(s <= near, near - s, s))

    barrier = pltpu.get_barrier_semaphore()
    for step in range(1, n):
        pl.semaphore_signal(barrier, inc=1, device_id={"ep": lax.rem(me + step, n)}, device_id_type=MESH)
    for step in range(1, n_tp):
        pl.semaphore_signal(barrier, inc=1, device_id={"tp": lax.rem(my_tp + step, n_tp)}, device_id_type=MESH)
    loads = [
        pltpu.make_async_copy(source, target, load.at[i])
        for i, (source, target) in enumerate((
            (x_ref, x_in), (turn_ref, turn), (k_ref, k_in), (q_ref, q_in),
            (sg_ref, sg), (su_ref, su), (sd_ref, sd),
            (wg_ref.at[0], wg), (wu_ref.at[0], wu), (wd_ref.at[0], wd), (w_ref, w_buf)))
    ]
    values = [
        pltpu.make_async_copy(v_ref.at[:, h * vw : (h + 1) * vw], v_in.at[h], load_v.at[h]) for h in range(heads)
    ]
    smalls = [
        pltpu.make_async_copy(source, target, small.at[i])
        for i, (source, target) in enumerate((
            (routes_hbm, routes_ref), (ffn_hbm, ffn_ref), (base_hbm, base_ref),
            (lam_hbm, lam_ref), (gain_hbm, gain_ref), (rw_hbm, rw_ref)))]
    for copy in (smalls[0], loads[0], *smalls[1:3], *loads[1:4], *values, *smalls[3:]):
        copy.start()

    def to_ep(source, target, send_sem, recv_sem, dest):
        return pltpu.make_async_remote_copy(
            source, target, send_sem, recv_sem, device_id={"ep": dest}, device_id_type=MESH)

    def to_tp(source, target, send_sem, recv_sem, dest):
        return pltpu.make_async_remote_copy(
            source, target, send_sem, recv_sem, device_id={"tp": dest}, device_id_type=MESH)

    def arrived(ref, sem):
        to_ep(ref, ref, sem, sem, lax.rem(me + 1, n)).wait_recv()

    across = (my_tp + 1 - 2 * (my_tp % 2), (my_tp + 2) % n_tp)
    corner = (across[0] + 2) % n_tp

    def reduction(send, first_in, held, second_in, ss, rs, ss2, rs2, pre=()):
        at = lambda ref, *index: ref.at[(*pre, *index)]

        def first_copies(h):
            return [
                to_tp(at(send, dest, h), at(first_in, h, i), at(ss, h, i), at(rs, h, i), across[h])
                for i, dest in enumerate((corner, across[h]))]

        def second_copy(h):
            return to_tp(at(held, h), at(second_in, h), at(ss2, h), at(rs2, h), across[1 - h])

        def pass_on(h):
            arrived(at(first_in, h, 0), at(rs, h, 0))
            own = send[(*pre, across[1 - h], h)].astype(f32)
            held[(*pre, h)] = (own + first_in[(*pre, h, 0)].astype(f32)).astype(bf16)
            second_copy(h).start()

        def total(h):
            arrived(at(first_in, h, 1), at(rs, h, 1))
            arrived(at(second_in, h), at(rs2, h))
            own = send[(*pre, my_tp, h)].astype(f32)
            return own + first_in[(*pre, h, 1)].astype(f32) + second_in[(*pre, h)].astype(f32)

        def sent():
            for h in range(2):
                for copy in (*first_copies(h), second_copy(h)):
                    copy.wait_send()

        return first_copies, pass_on, total, sent

    def columns(t):
        return pl.ds(pl.multiple_of(t * piece, piece), piece)

    smalls[0].wait()
    expert = lax.broadcasted_iota(jnp.int32, (n, tokens), 0)
    chosen = [(routes_ref[k : k + 1, :] == expert).astype(f32) for k in range(top_k)]
    earlier = lax.broadcasted_iota(jnp.int32, (tokens, tokens), 0) <= lax.broadcasted_iota(jnp.int32, (tokens, tokens), 1)
    ranks = jnp.dot(sum(chosen).astype(bf16), earlier.astype(bf16), preferred_element_type=f32) - 1.0
    slot = ranks + (expert * cap).astype(f32)
    slots = [jnp.sum(c * slot, axis=0, keepdims=True) for c in chosen]
    slot_row = lax.broadcasted_iota(jnp.int32, (n * cap, tokens), 0).astype(f32)
    marks = [(slot_row == s).astype(f32) for s in slots]
    for k in range(top_k):
        place[k] = marks[k].astype(bf16).reshape(n, cap, tokens)
    loads[0].wait()
    smalls[1].wait()
    x = x_in[...].astype(f32)
    inverse = lax.rsqrt(jnp.mean(x * x, axis=-1, keepdims=True) + norm_eps)
    xn[...] = (x * inverse * ffn_ref[...]).astype(bf16)
    out_buf[...] = jnp.dot(
        sum(marks).astype(bf16), xn[:, columns(my_tp)], preferred_element_type=f32).astype(bf16).reshape(n, cap, piece)

    def own_rows(dest):
        mark = place[0, dest]
        for k in range(1, top_k):
            mark = mark + place[k, dest]
        return jnp.dot(mark, xn[...], preferred_element_type=f32).astype(bf16)

    pl.semaphore_wait(barrier, n - 1 + n_tp - 1)
    for copy in loads[4:]:
        copy.start()

    def tok_copy(dest):
        return to_ep(out_buf.at[dest], arr.at[my_tp, me], t_ss.at[dest], t_rs.at[me], dest)

    def own_copy(step):
        dest = chip * g + lax.rem(core + step, g)
        return to_ep(own_buf.at[step - 1], arr.at[:, me], o_ss.at[step - 1], o_rs.at[me], dest)

    mate_chip = chip + 1 - 2 * (chip % 2)
    inner = (chip + side) % 2

    def send_tokens(first, last):
        for s in range(first, last):
            for c in range(g):
                tok_copy(nearest(s) * g + c).start()

    send_tokens(1, 2)

    @pl.when(inner == 1)
    def _():
        send_tokens(2, heads)

    for step in range(g):
        full = own_rows(chip * g + lax.rem(core + step, g))
        for t in range(n_tp):
            part = full[:, t * piece : (t + 1) * piece]
            if step == 0:
                arr[t, me] = part
            else:
                own_buf[step - 1, t] = part
        if step:
            own_copy(step).start()

    smalls[2].wait()
    base_cos, base_sin = base_ref[0, pl.ds(me, 1)], base_ref[1, pl.ds(me, 1)]
    lane = lax.broadcasted_iota(jnp.int32, (1, width), 1)
    front = lane % head_size < half
    loads[1].wait()
    cosine = turn[0] * base_cos - turn[1] * base_sin
    sine = turn[1] * base_cos + turn[0] * base_sin
    sine = jnp.where(front, -sine, sine)

    def turned(source, h):
        x = source[:, h * width : (h + 1) * width].astype(f32)
        partner = jnp.where(front, pltpu.roll(x, width - half, 1), pltpu.roll(x, half, 1))
        return (x * cosine + partner * sine).astype(bf16)

    loads[2].wait()
    for h in range(heads):
        rk[h] = turned(k_in, h)
    loads[3].wait()
    for h in range(heads):
        rq[h] = turned(q_in, h) * jnp.asarray(head_size ** -0.5, bf16)
    for copy in values:
        copy.wait()

    def q_rows(dest):
        return pl.ds(pl.multiple_of(((dest % g + me) % g) * sub, sub), sub)

    def q_copy(dest):
        return to_ep(rq.at[dest // g, q_rows(dest)], q_buf.at[me], q_ss.at[dest], q_rs.at[me], dest)

    def k_copy(dest):
        return to_ep(rk.at[dest // g], k_buf.at[me], k_ss.at[dest], k_rs.at[me], dest)

    def v_copy(dest):
        return to_ep(v_in.at[dest // g], v_buf.at[me], v_ss.at[dest], v_rs.at[me], dest)

    def send_kv(p):
        k_copy(p * g + core).start()
        v_copy(p * g + core).start()

    def send_q(p):
        for c in range(g):
            q_copy(p * g + c).start()

    for step in range(1, g):
        q_copy(chip * g + lax.rem(core + step, g)).start()
    send_kv(mate_chip)
    send_q(mate_chip)

    @pl.when(inner == 0)
    def _():
        send_tokens(2, heads)

    @pl.when(side == 0)
    def _():
        for i in (0, 1):
            send_kv(2 + (inner + i) % 2)
            send_q(2 + (inner + i) % 2)

    @pl.when(side == 1)
    def _():
        for s in range(2, heads):
            send_q(nearest(s))
        for i in (1, 0):
            send_kv((inner + i) % 2)

    q_buf[me] = rq[chip, q_rows(me)]
    k_buf[me] = rk[chip]
    v_buf[me] = v_in[chip]

    def gated(gate, up):
        return (gate / (1.0 + jnp.exp(-gate)) * up).astype(bf16)

    for i in (4, 5, 6):
        loads[i].wait()
    hidden = gated(
        jnp.dot(xn[...], sg[...], preferred_element_type=f32), jnp.dot(xn[...], su[...], preferred_element_type=f32))

    sh_copies, sh_pass, sh_total, sh_sent = reduction(
        sh_send, sh_first, sh_held, sh_second, s_ss, s_rs, s2_ss, s2_rs)
    half_tokens = tokens // 2

    def shared_down(dest, h):
        sh_send[dest, h] = jnp.dot(
            hidden[h * half_tokens : (h + 1) * half_tokens], sd[:, columns(dest)],
            preferred_element_type=f32).astype(bf16)

    for i in range(2):
        for h in range(2):
            shared_down((corner, across[h])[i], h)
            sh_copies(h)[i].start()
    for h in range(2):
        shared_down(across[1 - h], h)
        shared_down(my_tp, h)

    for copy in smalls[3:]:
        copy.wait()
    lam = lam_ref[chip]
    gain = gain_ref[...]
    vt_rows = vt_buf.shape[1]
    keys = g * rows
    lane_row = lax.broadcasted_iota(jnp.int32, (sub, width), 1)

    def forward(source, step):
        to = chip * g + lax.rem(core + step, g)
        return (
            to_ep(k_buf.at[source], k_buf.at[source], fk_ss.at[source, step], fk_rs.at[source], to),
            to_ep(v_buf.at[source], v_buf.at[source], fv_ss.at[source, step], fv_rs.at[source], to),
        )

    def prepare_kv(e):
        vt_buf[e, :vw] = v_buf[e].astype(f32).T.astype(bf16)
        vt_buf[e, vw:] = jnp.ones((vt_rows - vw, rows), bf16)

    def receive_kv(p):
        direct = p * g + core

        @pl.when(direct != me)
        def _():
            arrived(k_buf.at[direct], k_rs.at[direct])
            arrived(v_buf.at[direct], v_rs.at[direct])

        for step in range(1, g):
            for copy in forward(direct, step):
                copy.start()
        prepare_kv(direct)

    def complete_kv(p):
        for step in range(1, g):
            other = p * g + lax.rem(core + step, g)
            arrived(k_buf.at[other], fk_rs.at[other])
            arrived(v_buf.at[other], fv_rs.at[other])
            prepare_kv(other)

    def receive_q(p):
        for c in range(g):
            e = p * g + c

            @pl.when(e != me)
            def _():
                arrived(q_buf.at[e], q_rs.at[e])

            q = q_buf[e]
            zero = jnp.zeros_like(q)
            st_buf[p, 2 * c * sub : (2 * c + 1) * sub] = jnp.where(lane_row < width // 2, q, zero)
            st_buf[p, (2 * c + 1) * sub : (2 * c + 2) * sub] = jnp.where(lane_row < width // 2, zero, q)
        m_buf[p] = jnp.full((1, keys), masked_low, f32)
        acc[p] = jnp.zeros((vt_rows, keys), f32)

    def tile(p, e, first=0, diagonal=False):
        span = slice(first, keys)
        size = keys - first
        s = lax.dot_general(k_buf[e], st_buf[p, span], (((1,), (1,)), ((), ())), preferred_element_type=f32)
        if diagonal:
            key = lax.broadcasted_iota(jnp.int32, (rows, size), 0) + first
            column = lax.broadcasted_iota(jnp.int32, (rows, size), 1) + first
            block = column // rows
            query = block * rows + column % sub + (core + block) % g * sub
            s = jnp.where(key <= query, s, masked_low)
        old = m_buf[p, :, span]
        m = jnp.maximum(old, jnp.max(s, axis=0, keepdims=True))
        weights = jnp.exp(s - m).astype(bf16)
        m_buf[p, :, span] = m
        acc[p, :, span] = acc[p, :, span] * jnp.exp(old - m) + jnp.dot(
            vt_buf[e], weights, preferred_element_type=f32)

    def hn_copy(dest):
        return to_ep(hn_send.at[dest], hn_buf.at[me], h_ss.at[dest], h_rs.at[me], dest)

    def finish(p):
        a = (acc[p, :vw] / acc[p, vw : vw + 1]).T
        for c in range(g):
            e = p * g + c
            diff = a[2 * c * sub : (2 * c + 1) * sub] - lam * a[(2 * c + 1) * sub : (2 * c + 2) * sub]
            inverse = lax.rsqrt(jnp.mean(diff * diff, axis=-1, keepdims=True) + norm_eps)
            hn_send[e] = (diff * inverse * gain).astype(bf16)

            @pl.when(e != me)
            def _():
                hn_copy(e).start()

    def spread_copy(p, i):
        part = arr.at[my_tp, pl.ds(p * g, g)]
        return to_tp(part, part, x_ss.at[p, i], x_rs.at[my_tp, p], across[i])

    def relay_copy(p, c):
        part = arr.at[across[c], p * g + c]
        return to_tp(part, part, d_ss.at[p, c], d_rs.at[p, c], across[1 - c])

    def spread(s):
        p = nearest(s)
        for c in range(g):
            arrived(arr.at[my_tp, p * g + c], t_rs.at[p * g + c])
        for i in range(2):
            spread_copy(p, i).start()

    def relay(s):
        p = nearest(s)
        for c in range(2):
            arrived(arr.at[across[c], pl.ds(p * g, g)], x_rs.at[across[c], p])
            relay_copy(p, c).start()

    expert_sums = [
        reduction(ex_send, ex_first, ex_held, ex_second, e_ss, e_rs, e2_ss, e2_rs, (part,)) for part in range(2)]
    mix_copies, mix_pass, mix_total, mix_sent = reduction(
        mix_send, mix_first, mix_held, mix_second, m_ss, m_rs, m2_ss, m2_rs)
    def routed(part):
        half = n // 2
        start = half * (side if part == 0 else 1 - side)
        if part == 0:
            for step in range(1, g):
                other = chip * g + lax.rem(core + step, g)
                arrived(arr.at[:, other], o_rs.at[other])
        for s in range(1, 2) if part == 0 else range(2, heads):
            for c in range(2):
                arrived(arr.at[corner, nearest(s) * g + c], d_rs.at[nearest(s), c])
        if part == 0:
            for i in (7, 8, 9):
                loads[i].wait()
        gate = up = None
        for t in range(n_tp):
            block = arr[t, pl.ds(start, half)].reshape(half * cap, piece)
            span = slice(t * piece, (t + 1) * piece)
            gate_part = jnp.dot(block, wg[span, :], preferred_element_type=f32)
            up_part = jnp.dot(block, wu[span, :], preferred_element_type=f32)
            gate = gate_part if gate is None else gate + gate_part
            up = up_part if up is None else up + up_part
        hidden = gated(gate, up)
        quarter = half // 2 * cap

        def down(dest, h):
            ex_send[part, dest, h] = jnp.dot(
                hidden[h * quarter : (h + 1) * quarter], wd[:, columns(dest)], preferred_element_type=f32).astype(bf16)

        copies = expert_sums[part][0]
        for i in range(2):
            for h in range(2):
                down((corner, across[h])[i], h)
                copies(h)[i].start()
        for h in range(2):
            down(across[1 - h], h)
            down(my_tp, h)

    low, pair = 1 - side, 2 * side

    def phase(s, _):
        early = (5 - s) // 4
        second = (s // 2) * (1 - s // 3)
        third = (s // 3) * (1 - s // 4)
        fourth = (s // 4) * (1 - s // 5)
        fifth = s // 5
        newest = early * (chip + s * (mate_chip - chip)) + (1 - early) * (
            low * (third * 3 + (fourth + fifth) * 2) + side * (second * (1 - inner) + third * inner))
        with_q = early + side * (second + third)
        with_kv = with_q + low * (third + fifth)

        @pl.when(low * second == 1)
        def _():
            for p in (2, 3):
                receive_q(p)

        @pl.when(with_kv - low * fifth == 1)
        def _():
            receive_kv(newest)

        @pl.when(low * fourth == 1)
        def _():
            receive_kv(2)
            complete_kv(2)

        @pl.when(with_q == 1)
        def _():
            receive_q(newest)

        def diagonal(step, _):
            c = (core + step) % g

            @pl.when(step * (1 - fifth) == 1)
            def _():
                complete_kv(newest)

            for first in range(g):
                @pl.when(c == first)
                def _():
                    tile(newest, newest * g + first, first * rows, True)

            return 0

        @pl.when(with_kv == 1)
        def _():
            lax.fori_loop(0, g, diagonal, 0)

        @pl.when(side * (second * inner + third * (1 - inner)) == 1)
        def _():
            finish(newest)

        def full(i, _):
            p = early * (pair + 1) + second * (2 + low * (i // 2) + side * i) + low * fourth * 3 + side * third * (1 + i)
            j = early * pair + second * (low * (i % 2) + side * newest) + low * fourth * 2 + side * third * newest * ((i + 1) // 2)
            for c in range(g):
                tile(p, j * g + c)

            @pl.when(third * side + low * fourth == 1)
            def _():
                finish(p)

            return 0

        lax.fori_loop(0, early * s + second * (4 * low + 2 * side) + low * fourth + side * third * 3, full, 0)

        def done(p, _):
            finish(p)
            return 0

        @pl.when((early * s + fifth) * low == 1)
        def _():
            lax.fori_loop(early * pair + fifth * 2, early * (pair + 2) + fifth * 3, done, 0)

        @pl.when(s == 0)
        def _():
            spread(1)
            relay(1)

        @pl.when(s == inner)
        def _():
            for step in range(2, heads):
                spread(step)

        @pl.when(s == 1 + low * inner)
        def _():
            for step in range(2, heads):
                relay(step)
            routed(0)

        @pl.when(s == 1 + low * inner)
        def _():
            routed(1)
            for h in range(2):
                expert_sums[0][1](h)
                sh_pass(h)

        @pl.when(s == 2 + 2 * low * inner)
        def _():
            for h in range(2):
                expert_sums[1][1](h)

        return 0

    lax.fori_loop(0, heads + 2, phase, 0)

    def y_copy(dest):
        return to_ep(y_buf.at[dest], ret.at[me], y_ss.at[dest], y_rs.at[me], dest)

    def send_back():
        for part in (1, 0):
            for h in range(2):
                p = (side if part == 0 else 1 - side) * 2 + h
                y_buf[pl.ds(p * g, g)] = expert_sums[part][2](h).astype(bf16).reshape(g, cap, piece)
        for s in range(heads - 1, 0, -1):
            for c in range(g):
                y_copy(nearest(s) * g + c).start()
        for step in range(1, g):
            y_copy(chip * g + lax.rem(core + step, g)).start()
        ret[me] = y_buf[me]

    @pl.when(side == 1)
    def _():
        send_back()

    hn_buf[me] = hn_send[me]
    for step in range(1, n):
        source = lax.rem(me + step, n)
        arrived(hn_buf.at[source], h_rs.at[source])
    loads[10].wait()
    normed = [
        jnp.concatenate([hn_buf[h * g + (part + n - me) % g] for h in range(heads)], axis=1) for part in range(g)]

    def project(dest, h):
        mix_send[dest, h] = jnp.dot(normed[h], w_buf[:, columns(dest)], preferred_element_type=f32).astype(bf16)

    for i in range(2):
        for h in range(2):
            project((corner, across[h])[i], h)
            mix_copies(h)[i].start()
    for h in range(2):
        project(across[1 - h], h)
        project(my_tp, h)
    @pl.when(low * inner == 1)
    def _():
        send_back()

    for h in range(2):
        mix_pass(h)

    @pl.when(low * (1 - inner) == 1)
    def _():
        send_back()

    out = jnp.concatenate([sh_total(h) for h in range(2)], axis=0)
    rw_pad[...] = jnp.zeros_like(rw_pad)
    rw_pad[:top_k, :tokens] = rw_ref[...]
    scale = rw_pad[...].T
    for step in range(1, n):
        source = lax.rem(me + step, n)
        arrived(ret.at[source], y_rs.at[source])
    returned = ret[...].reshape(n * cap, piece)
    for k in range(top_k):
        out = out + scale[:tokens, k : k + 1] * lax.dot_general(
            place[k].reshape(n * cap, tokens), returned, (((0,), (0,)), ((), ())), preferred_element_type=f32)
    moe_ref[...] = out.astype(bf16)
    moe_store = pltpu.make_async_copy(moe_ref, moe_hbm, out_sem.at[2])
    moe_store.start()
    for h in range(2):
        attn_ref[h] = mix_total(h).astype(bf16)
        pltpu.make_async_copy(attn_ref.at[h], attn_hbm.at[h * sub : (h + 1) * sub], out_sem.at[h]).start()
    for s in range(1, heads):
        p = nearest(s)
        k_copy(p * g + core).wait_send()
        v_copy(p * g + core).wait_send()
        for c in range(g):
            tok_copy(p * g + c).wait_send()
        for i in range(2):
            spread_copy(p, i).wait_send()
            relay_copy(p, i).wait_send()
    for step in range(1, n):
        dest = lax.rem(me + step, n)
        q_copy(dest).wait_send()
        hn_copy(dest).wait_send()
        y_copy(dest).wait_send()
    for step in range(1, g):
        own_copy(step).wait_send()
    for p in range(heads):
        for step in range(1, g):
            for copy in forward(p * g + core, step):
                copy.wait_send()
    sh_sent()
    for part in range(2):
        expert_sums[part][3]()
    mix_sent()
    moe_store.wait()
    for h in range(2):
        pltpu.make_async_copy(attn_ref.at[h], attn_hbm.at[h * sub : (h + 1) * sub], out_sem.at[h]).wait()


def turn_tables(rows, n, head_size):
    half = head_size // 2
    frequency = theta_base ** (-(np.arange(half) * 2.0) / head_size)

    def waves(positions):
        angles = np.tile(positions[:, None] * frequency[None, :], (1, 4))
        return np.stack([np.cos(angles), np.sin(angles)]).astype(np.float32)

    return waves(np.arange(rows)), waves(np.arange(n) * rows)


def exchange_all(
    query_pairs, key_pairs, value_rows, head_lambda, head_gain, out_weight, moe_input, ffn_gain, routes, route_weight,
    gate_weight, up_weight, down_weight, shared_gate, shared_up, shared_down,
):
    n, n_tp = lax.axis_size("ep"), lax.axis_size("tp")
    tokens, model = moe_input.shape
    piece = model // n_tp
    rows = query_pairs.shape[0]
    heads = head_lambda.shape[0]
    width = query_pairs.shape[1] // heads
    head_size = width // 2
    vw = value_rows.shape[1] // heads
    g = n // heads
    sub = rows // g
    keys = g * rows
    cap = -(-(tokens * TOP_K * 5 // (4 * n)) // 8) * 8
    hidden, shared = gate_weight.shape[2], shared_gate.shape[1]
    turns, bases = turn_tables(rows, n, head_size)
    any_spec = pl.BlockSpec(memory_space=pl.ANY)
    dma = pltpu.SemaphoreType.DMA
    buffers = [
        (rows, heads * width), (rows, heads * width), (heads, rows, vw), ((2, rows, width), f32),
        (tokens, model), (tokens, model), (TOP_K, n, cap, tokens), (heads, rows, width), (heads, rows, width),
        (n, sub, width), (n, rows, width), (n, rows, vw), (n, vw + 8, rows), (heads, 2 * rows, width),
        ((heads, vw + 8, keys), f32), ((heads, 1, keys), f32), (n, sub, vw), (n, sub, vw), out_weight.shape,
        (n, cap, piece), (g - 1, n_tp, cap, piece), (n_tp, n, cap, piece),
        (model, hidden), (model, hidden), (hidden, model), (model, shared), (model, shared), (shared, model),
        (n_tp, 2, tokens // 2, piece), (2, 2, tokens // 2, piece), (2, tokens // 2, piece), (2, tokens // 2, piece),
        (2, n_tp, 2, g * cap, piece), (2, 2, 2, g * cap, piece), (2, 2, g * cap, piece), (2, 2, g * cap, piece),
        (n_tp, 2, sub, piece), (2, 2, sub, piece), (2, sub, piece), (2, sub, piece), (n, cap, piece), (n, cap, piece),
        ((8, -(-tokens // 128) * 128), f32),
    ]
    semaphores = [
        (11,), (heads,), (n,), (n,), (n,), (n,), (n,), (n,), (n, g), (n,), (n, g), (n,), (n,), (n,),
        (n,), (n,), (g - 1,), (n,), (heads, 2), (n_tp, heads), (heads, 2), (heads, 2),
        (2, 2), (2, 2), (2,), (2,), (2, 2), (2, 2), (2,), (2,), (2, 2, 2), (2, 2, 2), (2, 2), (2, 2), (n,), (n,),
    ]
    results = pl.pallas_call(
        functools.partial(mega_kernel, n, heads, n_tp, head_size),
        out_shape=(
            jax.ShapeDtypeStruct((rows, piece), bf16),
            jax.ShapeDtypeStruct((tokens, piece), bf16),
        ),
        in_specs=[any_spec] * 18,
        out_specs=(any_spec, any_spec),
        scratch_shapes=[
            pltpu.SMEM((heads,), f32), pltpu.VMEM((1, vw), f32), pltpu.VMEM((TOP_K, tokens), jnp.int32),
            pltpu.VMEM((TOP_K, tokens), f32), pltpu.VMEM((1, model), f32), pltpu.VMEM(bases.shape, f32),
            pltpu.VMEM((2, sub, piece), bf16), pltpu.VMEM((tokens, piece), bf16), dma((6,)), dma((3,)),
        ] + [
            pltpu.VMEM(shape[0], shape[1]) if isinstance(shape[0], tuple) else pltpu.VMEM(shape, bf16)
            for shape in buffers
        ] + [dma(shape) for shape in semaphores],
        compiler_params=pltpu.CompilerParams(
            collective_id=0, has_side_effects=True, vmem_limit_bytes=60 * 2**20),
        cost_estimate=pl.CostEstimate(flops=30 * 10**9, bytes_accessed=24 * 2**20, transcendentals=6 * 10**6),
        name="exchange",
    )(
        head_lambda, head_gain.reshape(1, vw), routes.T, route_weight.T, ffn_gain.reshape(1, model),
        jnp.asarray(turns), jnp.asarray(bases), query_pairs, key_pairs, value_rows, moe_input, out_weight,
        gate_weight, up_weight, down_weight, shared_gate, shared_up, shared_down)
    return pl.pallas_call(
        store_kernel,
        out_shape=tuple(jax.ShapeDtypeStruct(r.shape, r.dtype) for r in results),
        in_specs=[any_spec] * 2,
        out_specs=(any_spec, any_spec),
        scratch_shapes=[pltpu.VMEM(r.shape, r.dtype) for r in results] + [dma((2,)), dma((2,))],
        name="store",
    )(*results)


def store_kernel(attn_ref, moe_ref, attn_out, moe_out, attn_buf, moe_buf, in_sems, out_sems):
    refs = ((attn_ref, attn_buf, attn_out), (moe_ref, moe_buf, moe_out))
    ins = [pltpu.make_async_copy(source, buf, in_sems.at[i]) for i, (source, buf, _) in enumerate(refs)]
    outs = [pltpu.make_async_copy(buf, target, out_sems.at[i]) for i, (_, buf, target) in enumerate(refs)]
    for copy in ins:
        copy.start()
    for i in (1, 0):
        ins[i].wait()
        outs[i].start()
    for copy in outs:
        copy.wait()


def local(
    query_pairs,
    key_pairs,
    value_rows,
    head_lambda,
    head_gain,
    out_weight,
    moe_input,
    ffn_gain,
    routes,
    route_weight,
    gate_weight,
    up_weight,
    down_weight,
    shared_gate,
    shared_up,
    shared_down,
):
    n = lax.axis_size("ep")
    heads = head_lambda.shape[0]
    rows = query_pairs.shape[0]
    fits = n == 2 * heads and heads == 4 and lax.axis_size("tp") == 4 and (rows * heads) % (n * 64) == 0 and routes.shape[0] % 32 == 0
    if fits:
        return exchange_all(
            query_pairs, key_pairs, value_rows, head_lambda, head_gain, out_weight, moe_input, ffn_gain, routes,
            route_weight, gate_weight, up_weight, down_weight, shared_gate, shared_up, shared_down,
        )
    row_values = moe_input.astype(jnp.float32)
    inverse_norm = lax.rsqrt(jnp.mean(row_values * row_values, axis=-1, keepdims=True) + norm_eps)
    normed = (row_values * inverse_norm * ffn_gain).astype(jnp.bfloat16)
    attn_out = generic_attention(query_pairs, key_pairs, value_rows, head_lambda, head_gain, out_weight)
    token_rows = normed.shape[0]
    experts = lax.axis_size("ep")
    capacity = token_rows * TOP_K * 5 // (4 * experts)
    flat_routes = routes.reshape(-1)
    onehot = (flat_routes[:, None] == jnp.arange(experts, dtype=jnp.int32)).astype(jnp.int32)
    slot_rank = jnp.sum((jnp.cumsum(onehot, axis=0) - 1) * onehot, axis=-1)
    slot_index = flat_routes * capacity + slot_rank
    token_index = jnp.arange(token_rows * TOP_K, dtype=jnp.int32) // TOP_K
    slot_rows = (
        jnp.full((experts * capacity,), token_rows, jnp.int32).at[slot_index].set(token_index)
    )
    padded = jnp.concatenate([normed, jnp.zeros((1, normed.shape[1]), jnp.bfloat16)], axis=0)
    outgoing = padded[slot_rows]
    arrived = lax.all_to_all(outgoing, "ep", split_axis=0, concat_axis=0, tiled=True)
    gate_part = jnp.dot(arrived, gate_weight[0], preferred_element_type=jnp.float32)
    up_part = jnp.dot(arrived, up_weight[0], preferred_element_type=jnp.float32)
    hidden = (jax.nn.silu(gate_part) * up_part).astype(jnp.bfloat16)
    expert_terms = jnp.dot(hidden, down_weight[0], preferred_element_type=jnp.float32)
    shared_gated = jnp.dot(normed, shared_gate, preferred_element_type=jnp.float32)
    shared_lifted = jnp.dot(normed, shared_up, preferred_element_type=jnp.float32)
    shared_hidden = (jax.nn.silu(shared_gated) * shared_lifted).astype(jnp.bfloat16)
    shared_terms = jnp.dot(shared_hidden, shared_down, preferred_element_type=jnp.float32)
    expert_sum, shared_sum = (
        lax.psum_scatter(
            expert_terms.astype(jnp.bfloat16), "tp", scatter_dimension=1, tiled=True
        ).astype(jnp.float32),
        lax.psum_scatter(
            shared_terms.astype(jnp.bfloat16), "tp", scatter_dimension=1, tiled=True
        ).astype(jnp.float32),
    )
    returned = lax.all_to_all(
        expert_sum.astype(jnp.bfloat16), "ep", split_axis=0, concat_axis=0, tiled=True
    )
    picked = returned[slot_index.reshape(token_rows, TOP_K)]
    moe_out = (
        jnp.sum(route_weight[..., None] * picked.astype(jnp.float32), axis=1) + shared_sum
    ).astype(jnp.bfloat16)
    return (attn_out, moe_out)


def solution(mesh):
    return jax.shard_map(
        local,
        mesh=mesh,
        in_specs=(
            P("ep", "tp"),
            P("ep", "tp"),
            P("ep", "tp"),
            P("tp"),
            P(),
            P("tp", None),
            P("ep", None),
            P(),
            P("ep", None),
            P("ep", None),
            P("ep", None, "tp"),
            P("ep", None, "tp"),
            P("ep", "tp", None),
            P(None, "tp"),
            P(None, "tp"),
            P("tp", None),
        ),
        out_specs=(P("ep", "tp"), P("ep", "tp")),
        check_vma=False,
    )
```
